32 devices in a mesh: sp: 4 (over z), dp: 8 (over y, x, core).
Axes of the slice: x: 2, y: 2, z: 4, core: 2. Of those that a mesh axis runs over, the one named last changes fastest.
Arguments:
- tokens: bfloat16 [8, 512, 2048], P('dp', 'sp'), may hold values from -6 to 6
- receptance_weight: bfloat16 [2048, 1024], P('dp'), may hold values from -0.125 to 0.125
- key_projection_weight: bfloat16 [2048, 1024], P('dp'), may hold values from -0.125 to 0.125
- value_projection_weight: bfloat16 [2048, 1024], P('dp'), may hold values from -0.125 to 0.125
- decay_down_weight: bfloat16 [2048, 256], P('dp'), may hold values from -0.125 to 0.125
- decay_up_weight: bfloat16 [2, 128, 1024], replicated, may hold values from -0.71875 to 0.71875
- decay_floor_level: float32 [2, 1024], replicated, may hold values from -10 to -2.25
- correction_rate_logit: float32 [2, 1024], P(None, 'sp'), may hold values from -4 to 4
- diagonal_address_factor: float32 [2, 1024], P(None, 'sp'), may hold values from -1 to 1
- head_norm_gain: float32 [1024], P('sp'), may hold values from 0.1 to 1.9
Outputs:
- mixed: bfloat16 [8, 512, 1024], P('dp', 'sp')
The draws below stay inside these ranges and needn't reach their ends.
All inputs are finite; a program needn't handle non-finite values.
Results may differ from the reference program's by a relative error of at most 0.0056.
The reference program's roundings to bfloat16 on the way (of `lowered` and `pre`) count: a program that leaves them out, or rounds other values in their place, can miss the bound.
Values may be sent and summed in bfloat16 or wider, within the bound.
A program may use at most 128 MiB of HBM per device.

```python
import math
import jax
import jax.numpy as jnp
from jax import lax

D = 2048
ATTENTION_SPLITS = 16
SUBSPACE_SIZE = 64
RANK = 128
CHANNEL_COUNT = 1024
LENGTH = 512
SEQS = 8


def draw_decay_floor_level(key, part):
    first, second, third, fourth = jax.random.split(key, 4)
    keep = 5
    slow = jax.random.randint(first, (2, ATTENTION_SPLITS, 1), 0, 10) < keep
    slow_level = jax.random.uniform(second, (2, ATTENTION_SPLITS, 1), jnp.float32, -9.5, -8.5)
    fast_level = jax.random.uniform(third, (2, ATTENTION_SPLITS, 1), jnp.float32, -3.25, -2.75)
    jitter = jax.random.uniform(fourth, (2, ATTENTION_SPLITS, SUBSPACE_SIZE), jnp.float32, -0.5, 0.5)
    return (jnp.where(slow, slow_level, fast_level) + jitter).reshape(2, ATTENTION_SPLITS * SUBSPACE_SIZE)


def level_of(stream_key, shape, cuts, low, high):
    loudness = 1.0
    for axis_at, parts in cuts:
        heights = jax.random.uniform(jax.random.fold_in(jax.random.fold_in(stream_key, 6), axis_at), (parts,), jnp.float32, low / len(cuts), high / len(cuts))
        loudness = loudness * jnp.repeat(jnp.exp(heights), shape[axis_at] // parts).reshape((-1,) + (1,) * (len(shape) - 1 - axis_at))
    return loudness


def gaussian(own_key, dims, scale, limit, cuts=(), dtype=jnp.bfloat16):
    entries = scale * jax.random.normal(own_key, dims, jnp.float32)
    if cuts:
        entries = entries * level_of(own_key, dims, cuts, -0.22, 0.18)
    return jnp.clip(entries, -limit, limit).astype(dtype)


def setup_inputs(seed: int = 0) -> dict:
    splits = jax.random.split(jax.random.key(seed), 11)
    tokens = gaussian(splits[0], (SEQS, LENGTH, D), 1.0, 6.0, ((0, 8), (1, 4)))
    receptance_weight = gaussian(splits[1], (D, CHANNEL_COUNT), D ** -0.5, 0.125, ((0, 8),))
    key_projection_weight = gaussian(splits[2], (D, CHANNEL_COUNT), D ** -0.5, 0.125, ((0, 8),))
    value_projection_weight = gaussian(splits[3], (D, CHANNEL_COUNT), D ** -0.5, 0.125, ((0, 8),))
    decay_down_weight = gaussian(splits[4], (D, 2 * RANK), D ** -0.5, 0.125, ((0, 8),))
    decay_up_weight = gaussian(splits[5], (2, RANK, CHANNEL_COUNT), 0.12, 0.71875)
    decay_floor_level = draw_decay_floor_level(jax.random.fold_in(splits[10], 71), 0)
    correction_rate_logit = gaussian(splits[7], (2, CHANNEL_COUNT), 1.0, 4.0, ((1, 4),), jnp.float32)
    diagonal_address_factor = gaussian(splits[8], (2, CHANNEL_COUNT), 0.2, 1.0, ((1, 4),), jnp.float32)
    head_norm_gain = jnp.clip(1.0 + 0.18 * jax.random.normal(splits[9], (CHANNEL_COUNT,), jnp.float32), 0.1, 1.9)
    return {"tokens": tokens, "receptance_weight": receptance_weight, "key_projection_weight": key_projection_weight, "value_projection_weight": value_projection_weight, "decay_down_weight": decay_down_weight, "decay_up_weight": decay_up_weight, "decay_floor_level": decay_floor_level, "correction_rate_logit": correction_rate_logit, "diagonal_address_factor": diagonal_address_factor, "head_norm_gain": head_norm_gain}


def contract(pattern, former, latter):
    return jnp.einsum(pattern, former, latter, precision=lax.Precision.HIGHEST)

def recur(state, inputs):
    query, rated_key, value, eraser, writer, decay = inputs
    pulled = contract('hij,hj->hi', state, eraser)
    state = state * decay[:, None, :] + pulled[:, :, None] * writer[:, None, :] + value[:, :, None] * rated_key[:, None, :]
    return (state, contract('hij,hj->hi', state, query))

def reference(tokens, receptance_weight, key_projection_weight, value_projection_weight, decay_down_weight, decay_up_weight, decay_floor_level, correction_rate_logit, diagonal_address_factor, head_norm_gain):
    flat = tokens.reshape(SEQS * LENGTH, D)
    receive = jnp.dot(flat, receptance_weight, preferred_element_type=jnp.float32).astype(jnp.bfloat16)
    key_rows = jnp.dot(flat, key_projection_weight, preferred_element_type=jnp.float32).astype(jnp.bfloat16)
    value_rows = jnp.dot(flat, value_projection_weight, preferred_element_type=jnp.float32).astype(jnp.bfloat16)
    lowered = jnp.tanh(jnp.dot(flat, decay_down_weight, preferred_element_type=jnp.float32)).astype(jnp.bfloat16)
    forward_pre = (jnp.dot(lowered[:, :RANK], decay_up_weight[0], preferred_element_type=jnp.float32) + decay_floor_level[0]).astype(jnp.bfloat16)
    backward_pre = (jnp.dot(lowered[:, RANK:], decay_up_weight[1], preferred_element_type=jnp.float32) + decay_floor_level[1]).astype(jnp.bfloat16)
    amend_strength = jax.nn.sigmoid(correction_rate_logit).reshape(2, ATTENTION_SPLITS, SUBSPACE_SIZE)
    diagonal_extra = diagonal_address_factor.reshape(2, ATTENTION_SPLITS, SUBSPACE_SIZE)
    gain = head_norm_gain.reshape(ATTENTION_SPLITS, SUBSPACE_SIZE)

    def to_sequences(content_matrix_full):
        return content_matrix_full.reshape(SEQS, LENGTH, ATTENTION_SPLITS, SUBSPACE_SIZE)

    def one_sequence(items):
        probe_matrix_full, keys, content_matrix_full, fore, backs = [piece.astype(jnp.float32) for piece in items]
        normed = keys / jnp.sqrt(lax.optimization_barrier(jnp.sum(keys * keys, -1, keepdims=True)) + 1.0)
        total = jnp.zeros((LENGTH, ATTENTION_SPLITS, SUBSPACE_SIZE), jnp.float32)
        for sweep_orientation, pre in ((0, fore), (1, backs)):
            decay = jnp.exp(-math.exp(-0.5) * jax.nn.sigmoid(pre))
            strength_multiplied = keys * amend_strength[sweep_orientation]
            inputs = (probe_matrix_full, strength_multiplied, content_matrix_full, -normed, normed * amend_strength[sweep_orientation], decay)
            if sweep_orientation == 1:
                inputs = tuple((jnp.flip(piece, 0) for piece in inputs))
            state = jnp.zeros((ATTENTION_SPLITS, SUBSPACE_SIZE, SUBSPACE_SIZE), jnp.float32)
            _, readout = lax.scan(recur, state, inputs)
            if sweep_orientation == 1:
                readout = jnp.flip(readout, 0)
            centred = readout - lax.optimization_barrier(jnp.mean(readout, -1, keepdims=True))
            variance = lax.optimization_barrier(jnp.mean(centred * centred, -1, keepdims=True))
            diagonal_contribution = lax.optimization_barrier(jnp.sum(probe_matrix_full * strength_multiplied * diagonal_extra[sweep_orientation], -1, keepdims=True)) * content_matrix_full
            total = total + (centred * lax.rsqrt(variance + 0.00064) * gain + diagonal_contribution)
        return total.reshape(LENGTH, ATTENTION_SPLITS * SUBSPACE_SIZE).astype(jnp.bfloat16)
    return lax.map(one_sequence, (to_sequences(receive), to_sequences(key_rows), to_sequences(value_rows), to_sequences(forward_pre), to_sequences(backward_pre)))
```

```python
import functools, math
import jax, jax.numpy as jnp
from jax import lax
from jax.experimental import pallas as pl
from jax.experimental.pallas import tpu as pltpu
from jax.sharding import PartitionSpec as P
HEAD = 64
SPAN = 64
BF = jnp.bfloat16
F32 = jnp.float32
NT = (((1,), (1,)), ((), ()))
TN = (((0,), (0,)), ((), ()))


def mm(a, b):
    return jnp.dot(a, b, preferred_element_type=F32)


def dot(a, b, dims):
    return lax.dot_general(a, b, dims, preferred_element_type=F32)


def split(x):
    hi = x.astype(BF)
    return hi, (x - hi.astype(F32)).astype(BF)


def iota(shape, axis):
    return lax.broadcasted_iota(jnp.int32, shape, axis)


def head_ones(chans):
    return (iota((chans, chans), 0) // HEAD == iota((chans, chans), 1) // HEAD).astype(BF)


def head_sum(x, ones):
    hi, lo = split(x)
    return mm(hi, ones) + mm(lo, ones)


def spread(x, mask):
    x = x.astype(BF)
    heads = mask.shape[0] // HEAD
    if heads > 1:
        x = jnp.concatenate([x] * heads, axis=0)
    return x * mask


def at_row(start, size):
    return pl.ds(pl.multiple_of(start, size), size)


class Core:
    def __init__(self, tok, wk, wd, wv, wr, up, floor, rate, diag, gain, out, scratch):
        self.tok, self.wk, self.wd, self.wv, self.wr = tok, wk, wd, wv, wr
        self.up, self.floor, self.rate, self.diag, self.gain, self.out = up, floor, rate, diag, gain, out
        (self.pk_s, self.pv_s, self.inv_s, self.grow_s, self.g_s, self.wp_s, self.kend_s,
         self.t_s, self.teg_s, self.step_s, self.tcv_s, self.put_s, self.state_s) = scratch
        self.length, self.chans = out.shape
        self.heads = self.chans // HEAD
        self.rank = up.shape[1]
        self.blocks = self.length // SPAN
        self.half = self.length // 2

    def unit(self, block):
        return at_row(block * SPAN, SPAN)

    def keys(self, start):
        chans, rank, tile = self.chans, self.rank, self.half
        many = tile // SPAN
        ones = head_ones(chans)
        at = at_row(start, tile)
        source = self.tok[at, :]
        pk = mm(source, self.wk[...]).astype(BF)
        self.pk_s[at, :] = pk
        pk = pk.astype(F32)
        lowered = jnp.tanh(mm(source, self.wd[...])).astype(BF)
        inv = lax.rsqrt(head_sum(pk * pk, ones) + 1.0)
        self.inv_s[at, :] = inv
        normed = pk * inv
        rates = jax.nn.sigmoid(self.rate[...])
        ri = iota((tile, tile), 0)
        ci = iota((tile, tile), 1)
        same = ri // SPAN == ci // SPAN
        first = start // SPAN
        units = []
        for d in range(2):
            pre = (
                mm(lowered[:, d * rank : (d + 1) * rank], self.up[d]) + self.floor[d : d + 1, :]
            ).astype(BF).astype(F32)
            fall = -math.exp(-0.5) * jax.nn.sigmoid(pre)
            tri = jnp.logical_and(same, (ci <= ri) if d == 0 else (ci >= ri)).astype(BF)
            hi, lo = split(fall)
            inclusive = mm(tri, hi) + mm(tri, lo)
            rated = normed * rates[d : d + 1, :]
            for s in range(many):
                cut = slice(s * SPAN, (s + 1) * SPAN)
                inside = inclusive[cut]
                end = inside[SPAN - 1 :] if d == 0 else inside[:1]
                mid = 0.5 * end
                inside = inside - mid
                g = jnp.exp(mid)
                grow = jnp.exp(inside)
                e = -normed[cut] * jnp.exp(inside - fall[cut])
                w = rated[cut] * jnp.exp(-inside)
                here = self.unit(first + s)
                self.grow_s[d, here, :] = grow
                self.g_s[d, pl.ds(pl.multiple_of((first + s) * 8, 8), 8), :] = jnp.broadcast_to(g, (8, chans))
                w = w.astype(BF)
                kend = (w.astype(F32) * g).astype(BF)
                self.wp_s[d, here, :] = w
                self.kend_s[d, here, :] = kend
                units.append((d, first + s, e.astype(BF), w, kend, (e * g).astype(BF)))
        return units

    def strict(self, d):
        ti = iota((SPAN, self.chans), 0)
        ji = iota((SPAN, self.chans), 1) % HEAD
        return (ti > ji) if d == 0 else (ti < ji)

    def invert(self, units):
        chans = self.chans
        mask = head_ones(chans)
        ti = iota((SPAN, chans), 0)
        ji = iota((SPAN, chans), 1) % HEAD
        eye = (ti == ji).astype(F32)
        full = [
            jnp.where(self.strict(d), dot(e, spread(w, mask), NT), 0.0) for d, _, e, w, _, _ in units
        ]
        near = ti // 4 == ji // 4
        base = [jnp.where(near, a, 0.0) for a in full]
        square = [mm(a.astype(BF), spread(a, mask)) for a in base]
        inverse = [eye + a for a in base]
        inverse = [t + mm(t.astype(BF), spread(a2, mask)) for t, a2 in zip(inverse, square)]
        size = 4
        while size < SPAN:
            far = jnp.logical_and(ti // (2 * size) == ji // (2 * size), ti // size != ji // size)
            first = [
                mm(t.astype(BF), spread(jnp.where(far, a, 0.0), mask))
                for t, a in zip(inverse, full)
            ]
            inverse = [t + mm(f.astype(BF), spread(t, mask)) for t, f in zip(inverse, first)]
            size *= 2
        for (d, block, _, _, kend, eg), t in zip(units, inverse):
            here = self.unit(block)
            t = (t - eye).astype(BF)
            self.t_s[d, here, :] = t
            teg = (eg.astype(F32) + mm(t, spread(eg, mask))).astype(BF)
            self.teg_s[d, here, :] = teg
            self.step_s[d, at_row(block * chans, chans), :] = dot(teg, kend, TN).astype(BF) * mask

    def values(self):
        chans = self.chans
        mask = head_ones(chans)
        pv = mm(self.tok[...], self.wv[...]).astype(BF)
        self.pv_s[...] = pv
        cv = pv.astype(F32) / self.inv_s[...]
        for block in range(self.blocks):
            cut = slice(block * SPAN, (block + 1) * SPAN)
            x = cv[cut]
            for d in range(2):
                tcv = x + mm(self.t_s[d, cut, :], spread(x, mask))
                self.tcv_s[d, cut, :] = tcv
                put = dot(tcv.astype(BF), self.kend_s[d, cut, :], TN) * mask.astype(F32)
                self.put_s[d, cut, :] = sum(put[h * HEAD : (h + 1) * HEAD] for h in range(self.heads))

    def scan(self):
        states = [jnp.zeros((HEAD, self.chans), F32) for _ in range(2)]
        for step in range(self.blocks):
            for d in range(2):
                block = step if d == 0 else self.blocks - 1 - step
                cut = slice(block * SPAN, (block + 1) * SPAN)
                state = states[d]
                low = state.astype(BF)
                self.state_s[d, cut, :] = low
                if step < self.blocks - 1:
                    g = self.g_s[d, block * 8 : block * 8 + 1, :]
                    step_w = self.step_s[d, block * self.chans : (block + 1) * self.chans, :]
                    states[d] = state * (g * g) + mm(low, step_w) + self.put_s[d, cut, :]

    def outputs(self, start, tile):
        chans = self.chans
        mask = head_ones(chans)
        at = at_row(start, tile)
        first = start // SPAN
        pr = mm(self.tok[at, :], self.wr[...]).astype(BF).astype(F32)
        pp = pr * self.pk_s[at, :].astype(F32)
        rates = jax.nn.sigmoid(self.rate[...])
        both = jnp.sum(rates * self.diag[...], axis=0, keepdims=True)
        total = head_sum(pp * both, mask) * self.pv_s[at, :].astype(F32)
        inv = self.inv_s[at, :]
        for d in range(2):
            ys = []
            diag = head_sum(pp * rates[d : d + 1, :], mask) * inv
            for s in range(tile // SPAN):
                cut = slice(s * SPAN, (s + 1) * SPAN)
                here = self.unit(first + s)
                g = self.g_s[d, pl.ds(pl.multiple_of((first + s) * 8, 8), 8), :][:1]
                q = pr[cut] * self.grow_s[d, here, :]
                qb = q.astype(BF)
                qg = (q * g).astype(BF)
                b = jnp.where(self.strict(d), dot(qb, spread(self.wp_s[d, here, :], mask), NT), 0.0)
                read = dot(
                    jnp.concatenate([self.teg_s[d, here, :], qg], axis=0),
                    spread(self.state_s[d, here, :], mask), NT,
                )
                exact = self.tcv_s[d, here, :] + read[:SPAN]
                ys.append(read[SPAN:] + mm(b.astype(BF), spread(exact, mask)) + diag[cut] * exact)
            y = jnp.concatenate(ys, axis=0)
            centred = y - head_sum(y, mask) * (1.0 / HEAD)
            variance = head_sum(centred * centred, mask) * (1.0 / HEAD)
            total = total + centred * lax.rsqrt(variance + 0.00064) * self.gain[...]
        self.out[at, :] = total.astype(BF)


def core_scratch(length, chans):
    vm = pltpu.VMEM
    both = lambda n, dt: vm((2, n, chans), dt)
    blocks = length // SPAN
    return [
        vm((length, chans), BF), vm((length, chans), BF), vm((length, chans), F32),
        both(length, F32), both(blocks * 8, F32), both(length, BF), both(length, BF),
        both(length, BF), both(length, BF), both(blocks * chans, BF), both(length, F32),
        both(length, F32), both(length, BF),
    ]


def core_kernel(
    tok_ref, w_ref, up_ref, floor_ref, rate_ref, diag_ref, gain_ref, out_ref,
    eq_s, wp_s, qe_s, kend_s, cv_s, own_s, decay_s, diag_s, t_s, b_s, state_s, y_s,
    arrivals=(),
):
    length, chans = out_ref.shape
    heads = chans // HEAD
    rank = up_ref.shape[1]
    rows = min(256, length)
    blocks = length // SPAN

    def head_ones():
        return (iota((chans, chans), 0) // HEAD == iota((chans, chans), 1) // HEAD).astype(BF)

    def head_sum(x, ones):
        hi, lo = split(x)
        return mm(hi, ones) + mm(lo, ones)

    def at_block(block):
        return pl.ds(pl.multiple_of(block * SPAN, SPAN), SPAN)

    def project(ready):
        tile = SPAN * len(ready)

        def put(ref, x, *lead):
            for s, block in enumerate(ready):
                ref[(*lead, at_block(block), slice(None))] = x[s * SPAN : (s + 1) * SPAN]

        source = jnp.concatenate([tok_ref[at_block(block), :] for block in ready], axis=0)
        pr = mm(source, w_ref[:, :chans]).astype(BF).astype(F32)
        pk = mm(source, w_ref[:, chans : 2 * chans]).astype(BF).astype(F32)
        pv = mm(source, w_ref[:, 2 * chans : 3 * chans]).astype(BF).astype(F32)
        lowered = jnp.tanh(mm(source, w_ref[:, 3 * chans :])).astype(BF)
        ones = head_ones()
        norm2 = head_sum(pk * pk, ones) + 1.0
        inv = lax.rsqrt(norm2)
        scale = norm2 * inv
        normed = pk * inv
        put(cv_s, scale * pv)
        rates = jax.nn.sigmoid(rate_ref[...])
        both = jnp.sum(rates * diag_ref[...], axis=0, keepdims=True)
        put(own_s, head_sum(pr * pk * both, ones) * pv)
        ri = iota((tile, tile), 0)
        ci = iota((tile, tile), 1)
        same = ri // SPAN == ci // SPAN
        whole = same.astype(BF)
        for d in range(2):
            pre = (
                mm(lowered[:, d * rank : (d + 1) * rank], up_ref[d]) + floor_ref[d : d + 1, :]
            ).astype(BF).astype(F32)
            fall = -math.exp(-0.5) * jax.nn.sigmoid(pre)
            tri = jnp.logical_and(same, (ci <= ri) if d == 0 else (ci >= ri)).astype(BF)
            hi, lo = split(fall)
            inclusive = mm(tri, hi) + mm(tri, lo)
            final = mm(whole, hi) + mm(whole, lo)
            half = 0.5 * final
            grow = jnp.exp(inclusive - half)
            shrink = jnp.exp(half - inclusive)
            g = jnp.exp(half)
            e = -normed * (grow * jnp.exp(-fall))
            q = pr * grow
            w = normed * rates[d : d + 1, :] * shrink
            put(wp_s, w.astype(BF), d)
            put(kend_s, (w * g).astype(BF), d)
            eb, qb = e.astype(BF), q.astype(BF)
            eg, qg = (e * g).astype(BF), (q * g).astype(BF)
            g2 = g * g
            put(diag_s, head_sum(pr * normed * rates[d : d + 1, :], ones), d)
            for s, block in enumerate(ready):
                cut = slice(s * SPAN, (s + 1) * SPAN)
                base = pl.multiple_of(block * 2 * SPAN, 2 * SPAN)
                eq_s[d, pl.ds(base, SPAN), :] = eb[cut]
                eq_s[d, pl.ds(base + SPAN, SPAN), :] = qb[cut]
                qe_s[d, pl.ds(base, SPAN), :] = eg[cut]
                qe_s[d, pl.ds(base + SPAN, SPAN), :] = qg[cut]
                decay_s[d, pl.ds(pl.multiple_of(block * 8, 8), 8), :] = g2[
                    s * SPAN : s * SPAN + 8
                ]

    def spread(x, mask):
        x = x.astype(BF)
        if heads > 1:
            x = jnp.concatenate([x] * heads, axis=0)
        return x * mask

    def invert(ready):
        mask = head_ones()
        ti = iota((SPAN, chans), 0)
        ji = iota((SPAN, chans), 1) % HEAD
        eye = (ti == ji).astype(F32)
        work = []
        for block in ready:
            for d in range(2):
                two = pl.ds(pl.multiple_of(block * 2 * SPAN, 2 * SPAN), 2 * SPAN)
                at = pl.ds(pl.multiple_of(block * SPAN, SPAN), SPAN)
                ab = lax.dot_general(
                    eq_s[d, two, :], spread(wp_s[d, at, :], mask), NT, preferred_element_type=F32
                )
                strict = (ti > ji) if d == 0 else (ti < ji)
                b_s[d, at, :] = jnp.where(strict, ab[SPAN:], 0.0).astype(BF)
                work.append((d, at, jnp.where(strict, ab[:SPAN], 0.0)))
        near = ti // 4 == ji // 4
        full = [a for _, _, a in work]
        base = [jnp.where(near, a, 0.0) for a in full]
        square = [mm(a.astype(BF), spread(a, mask)) for a in base]
        inverse = [eye + a for a in base]
        inverse = [t + mm(t.astype(BF), spread(a2, mask)) for t, a2 in zip(inverse, square)]
        size = 4
        while size < SPAN:
            far = jnp.logical_and(ti // (2 * size) == ji // (2 * size), ti // size != ji // size)
            first = [
                mm(t.astype(BF), spread(jnp.where(far, a, 0.0), mask))
                for t, a in zip(inverse, full)
            ]
            inverse = [t + mm(f.astype(BF), spread(t, mask)) for t, f in zip(inverse, first)]
            size *= 2
        for (d, at, _), t in zip(work, inverse):
            t_s[d, at, :] = (t - eye).astype(BF)

    for settle, ready in arrivals:
        settle()
        project(ready)
        invert(ready)

    state_s[...] = jnp.zeros_like(state_s)

    @pl.loop(0, blocks)
    def _(step):
        mask = head_ones()
        for d in range(2):
            block = step if d == 0 else blocks - 1 - step
            two = pl.ds(pl.multiple_of(block * 2 * SPAN, 2 * SPAN), 2 * SPAN)
            at = pl.ds(pl.multiple_of(block * SPAN, SPAN), SPAN)
            state = state_s[d]
            read = lax.dot_general(
                qe_s[d, two, :], state.astype(BF), NT, preferred_element_type=F32
            )
            x = cv_s[at, :] + read[:SPAN]
            exact = x + mm(t_s[d, at, :], spread(x, mask))
            a = exact.astype(BF)
            y_s[d, at, :] = read[SPAN:] + mm(b_s[d, at, :], spread(a, mask)) + diag_s[d, at, :] * exact
            decay = decay_s[d, pl.ds(pl.multiple_of(block * 8, 8), 8), :][:1]
            put = lax.dot_general(a, kend_s[d, at, :], TN, preferred_element_type=F32)
            state_s[d] = state * decay + put * mask.astype(F32)

    @pl.loop(0, length // rows)
    def _(step):
        at = pl.ds(pl.multiple_of(step * rows, rows), rows)
        ones = head_ones()
        total = own_s[at, :]
        for d in range(2):
            y = y_s[d, at, :]
            centred = y - head_sum(y, ones) * (1.0 / HEAD)
            variance = head_sum(centred * centred, ones) * (1.0 / HEAD)
            total = total + centred * lax.rsqrt(variance + 0.00064) * gain_ref[...]
        out_ref[at, :] = total.astype(BF)


MESH = pl.DeviceIdType.MESH


def whole_kernel(
    sp, dp, tok_ref, w_ref, up_ref, floor_ref, rate_ref, diag_ref, gain_ref, out_ref,
    tok_all, w_all, out_all, slots,
    ring_out, ring_in, far_out, far_in, pass_out, pass_in, back_out, back_in, *scratch,
):
    rows = tok_ref.shape[0]
    half_rows = rows // 2
    depth = w_ref.shape[0]
    chans = out_all.shape[1]
    chips = dp // 2
    z = lax.axis_index("sp")
    me = lax.axis_index("dp")
    chip = me // 2
    core = me % 2
    partner = chip * 2 + 1 - core

    def peer(k):
        return lax.rem(chip + k, chips) * 2 + core

    def z_peer(k):
        return lax.rem(z + k, sp)

    barrier = pltpu.get_barrier_semaphore()
    for target in [(z, partner)] + [(z, peer(k)) for k in range(1, chips)] + [
        (z_peer(k), me) for k in range(1, sp)
    ]:
        pl.semaphore_signal(barrier, inc=1, device_id=target, device_id_type=MESH)
    pl.semaphore_wait(barrier, chips + sp - 1)

    def remote(src, dst, out_sem, in_sem, target):
        copy = pltpu.make_async_remote_copy(
            src_ref=src, dst_ref=dst, send_sem=out_sem, recv_sem=in_sem,
            device_id=target, device_id_type=MESH,
        )
        copy.start()
        return copy

    def w_at(device):
        return pl.ds(pl.multiple_of(device * depth, depth), depth)

    def ring_step(s):
        copies = []
        for way in range(2):
            owner = z_peer(sp - s) if way == 0 else z_peer(s)
            at = pl.ds(
                pl.multiple_of(owner * rows + way * half_rows, half_rows), half_rows
            )
            first = tok_ref.at[pl.ds(way * half_rows, half_rows), :]
            copies.append(
                remote(
                    first if s == 0 else tok_all.at[at, :], tok_all.at[at, :],
                    ring_out.at[way, s], ring_in.at[way, s],
                    (z_peer(1) if way == 0 else z_peer(sp - 1), me),
                )
            )
        return copies

    ring = [ring_step(0)] if sp > 1 else []
    far = [
        remote(w_ref, w_all.at[w_at(me), :], far_out.at[k], far_in.at[k], (z, peer(k)))
        for k in range(1, chips)
    ]
    passed = [remote(w_ref, w_all.at[w_at(me), :], pass_out.at[0], pass_in.at[0], (z, partner))]
    w_all[w_at(me), :] = w_ref[...]
    tok_all[pl.ds(pl.multiple_of(z * rows, rows), rows), :] = tok_ref[...]
    for s in range(max(sp, chips) - 1):
        if s < sp - 2:
            for copy in ring[s]:
                copy.wait_recv()
            ring.append(ring_step(s + 1))
        if s < chips - 1:
            far[s].wait_recv()
            block = w_at(peer(chips - 1 - s))
            passed.append(
                remote(
                    w_all.at[block, :], w_all.at[block, :],
                    pass_out.at[s + 1], pass_in.at[s + 1], (z, partner),
                )
            )
    for copy in passed:
        copy.wait_recv()

    def last_ring():
        for copy in ring[-1]:
            copy.wait_recv()

    per = rows // SPAN
    arrivals = [(lambda: None, [z * per + b for b in range(per)])]
    for s in range(sp - 1):
        before, after = z_peer(sp - 1 - s), z_peer(s + 1)
        ready = [before * per + b for b in range(per // 2)]
        ready += [after * per + b for b in range(per // 2, per)]
        arrivals.append((last_ring if s == sp - 2 else lambda: None, ready))

    core_kernel(
        tok_all, w_all, up_ref, floor_ref, rate_ref, diag_ref, gain_ref, out_all, *scratch,
        arrivals=arrivals,
    )
    for copy in far + passed + [c for pair in ring for c in pair]:
        copy.wait_send()

    def out_at(owner):
        return pl.ds(pl.multiple_of(owner * rows, rows), rows)

    back = [
        remote(
            out_all.at[out_at(z_peer(k)), :], slots.at[z], back_out.at[k], back_in.at[k],
            (z_peer(k), me),
        )
        for k in range(1, sp)
    ]
    slots[z] = out_all[out_at(z), :]
    for copy in back:
        copy.wait()
    for s in range(sp):
        out_ref[:, s * chans : (s + 1) * chans] = slots[s]


def whole_call(sp, dp, rows, depth, chans, width):
    vm = pltpu.VMEM
    dma = pltpu.SemaphoreType.DMA
    length = rows * sp
    both = lambda n, dt: vm((2, n, chans), dt)
    return pl.pallas_call(
        functools.partial(whole_kernel, sp, dp),
        out_shape=jax.ShapeDtypeStruct((rows, chans * sp), BF),
        in_specs=[pl.BlockSpec(memory_space=vm)] * 7,
        out_specs=pl.BlockSpec(memory_space=vm),
        scratch_shapes=[
            vm((length, depth), BF), vm((depth, width), BF), vm((length, chans), BF),
            vm((sp, rows, chans), BF),
            dma((2, sp)), dma((2, sp)), dma((dp,)), dma((dp,)), dma((dp,)), dma((dp,)),
            dma((sp,)), dma((sp,)),
            both(2 * length, BF), both(length, BF), both(2 * length, BF), both(length, BF),
            vm((length, chans), F32), vm((length, chans), F32),
            both(length // SPAN * 8, F32), both(length, F32), both(length, BF), both(length, BF),
            vm((2, chans, chans), F32), both(length, F32),
        ],
        compiler_params=pltpu.CompilerParams(
            vmem_limit_bytes=58 * 1024 * 1024, collective_id=0, has_side_effects=True
        ),
        name="whole",
    )


def halves_kernel(
    sp, side, other, tok_ref, wr_ref, wk_ref, wv_ref, wd_ref, up_ref, floor_ref, rate_ref, diag_ref, gain_ref,
    out_ref, tok_all, wk_all, wv_all, wr_all, wd_all, up_s, floor_s, rate_s, diag_s, gain_s, out_all,
    w_in, w_out, relay_out, d_in, d_pass, t_in, t_pass, t_out, t_fwd, p_in, p_out, o_in, o_out, here, *scratch,
):
    rows = tok_ref.shape[0]
    depth = wk_ref.shape[0]
    chans = wk_all.shape[1]
    half = sp // 2
    part = rows // 2
    z = lax.axis_index("sp")
    me = lax.axis_index("dp")
    core = me % 2
    chip = me // 2
    cy, cx = chip // side, chip % side
    h = z // half
    j = z % half
    u = jnp.where(h == 1, j, half - 1 - j)
    slot = u * 2 + core
    partner = chip * 2 + 1 - core

    def layer(hh, uu):
        return half - 1 - uu + hh * (2 * uu + 1)

    def x_peer(k):
        return cy * side + lax.rem(cx + k, side)

    def y_peer(k):
        return lax.rem(cy + k, other) * side + cx

    x_peers = [x_peer(k) for k in range(1, side)]
    y_peers = [y_peer(k) for k in range(1, other)]

    def local(src, dst, n):
        copy = pltpu.make_async_copy(src, dst, here.at[n])
        copy.start()
        return copy

    def cols(who):
        return pl.ds(pl.multiple_of(who * chans, chans), chans)

    mine = at_row(me * depth, depth)
    own = [
        local(wd_ref, wd_all.at[mine, :], 0),
        local(wk_ref.at[:, cols(slot)], wk_all.at[mine, :], 1),
        local(up_ref.at[:, :, cols(slot)], up_s, 2),
        local(floor_ref.at[:, cols(slot)], floor_s, 3),
        local(wv_ref.at[:, cols(slot)], wv_all.at[mine, :], 4),
        local(wr_ref.at[:, cols(slot)], wr_all.at[mine, :], 5),
    ]

    @pl.when(core == h)
    def _():
        local(tok_ref, tok_all.at[at_row(z * rows, rows), :], 6)

    barrier = pltpu.get_barrier_semaphore()
    greet = [(z, p * 2 + k) for p in x_peers + y_peers for k in range(2)]
    greet += [(lax.rem(z + n, sp), chip * 2 + k) for n in range(1, sp) for k in range(2)]
    greet.append((z, partner))
    for target in greet:
        pl.semaphore_signal(barrier, inc=1, device_id=target, device_id_type=MESH)
    pl.semaphore_wait(barrier, len(greet))

    def remote(src, dst, out_sem, in_sem, target):
        return pltpu.make_async_remote_copy(
            src_ref=src, dst_ref=dst, send_sem=out_sem, recv_sem=in_sem,
            device_id=target, device_id_type=MESH,
        )

    def go(copy):
        copy.start()
        return copy

    sent = []
    pieces = [(wk_ref, wk_all), (wv_ref, wv_all), (wr_ref, wr_all)]

    def direct(n):
        src, dst = pieces[n]
        for i, p in enumerate(x_peers + y_peers):
            for k in range(2):
                sent.append(go(remote(
                    src.at[:, cols(u * 2 + k)], dst.at[mine, :],
                    w_out.at[n, i * 2 + k], w_in.at[n, me], (z, p * 2 + k),
                )))
        last = 2 * len(x_peers + y_peers)
        sent.append(go(remote(
            src.at[:, cols(u * 2 + 1 - core)], dst.at[mine, :],
            w_out.at[n, last], w_in.at[n, me], (z, partner),
        )))

    def arrived(sem, dst, block):
        remote(dst.at[block, :], dst.at[block, :], sem, sem, (z, partner)).wait_recv()

    def w_rows(p, c):
        return at_row((p * 2 + c) * depth, depth)

    def relay(n):
        dst = pieces[n][1]
        count = 0
        for c, froms, tos in ((0, x_peers, y_peers), (1, y_peers, x_peers)):
            for p in froms:
                block = w_rows(p, c)
                arrived(w_in.at[n, p * 2 + c], dst, block)
                for q in tos:
                    sent.append(go(remote(
                        dst.at[block, :], dst.at[block, :],
                        relay_out.at[n, count], w_in.at[n, p * 2 + c], (z, q * 2 + core),
                    )))
                    count += 1

    def finish(n):
        dst = pieces[n][1]
        for c, others in ((1, x_peers), (0, y_peers)):
            for p in others:
                arrived(w_in.at[n, p * 2 + c], dst, w_rows(p, c))
        for ky in range(1, other):
            for kx in range(1, side):
                p = lax.rem(cy + ky, other) * side + lax.rem(cx + kx, side)
                for c in range(2):
                    arrived(w_in.at[n, p * 2 + c], dst, w_rows(p, c))
        arrived(w_in.at[n, partner], dst, w_rows(chip, 1 - core))

    def decay_direct():
        for i, p in enumerate(x_peers + y_peers):
            sent.append(go(remote(
                wd_ref, wd_all.at[mine, :], w_out.at[3, i], d_in.at[me], (z, p * 2 + core))))
        sent.append(go(remote(
            wd_ref, wd_all.at[mine, :], w_out.at[3, len(x_peers + y_peers)], d_in.at[me], (z, partner))))

    def decay_pass(p, n):
        block = w_rows(p, core)
        sent.append(go(remote(
            wd_all.at[block, :], wd_all.at[block, :], d_pass.at[n], d_in.at[p * 2 + core], (z, partner))))

    late = []

    def decay_relay():
        for c, froms, tos in ((0, x_peers, y_peers), (1, y_peers, x_peers)):
            @pl.when(core == c)
            def _():
                count = 0
                for p in froms:
                    block = w_rows(p, c)
                    arrived(d_in.at[p * 2 + c], wd_all, block)
                    for q in tos:
                        go(remote(
                            wd_all.at[block, :], wd_all.at[block, :],
                            relay_out.at[3, count], d_in.at[p * 2 + c], (z, q * 2 + c)))
                        count += 1
                for p in tos:
                    arrived(d_in.at[p * 2 + c], wd_all, w_rows(p, c))

            def close(c=c, froms=froms, tos=tos):
                @pl.when(core == c)
                def _():
                    count = 0
                    for p in froms:
                        block = w_rows(p, c)
                        for q in tos:
                            remote(
                                wd_all.at[block, :], wd_all.at[block, :],
                                relay_out.at[3, count], d_in.at[p * 2 + c], (z, q * 2 + c)).wait_send()
                            count += 1

            late.append(close)
        for n, p in enumerate(x_peers + y_peers):
            decay_pass(p, n)

    def decay_finish():
        n = len(x_peers + y_peers)
        corners = [
            lax.rem(cy + ky, other) * side + lax.rem(cx + kx, side)
            for ky in range(1, other) for kx in range(1, side)
        ]
        for p in corners:
            arrived(d_in.at[p * 2 + core], wd_all, w_rows(p, core))
            decay_pass(p, n)
            n += 1
        arrived(d_in.at[partner], wd_all, w_rows(chip, 1 - core))
        for p in x_peers + y_peers + corners:
            arrived(d_in.at[p * 2 + 1 - core], wd_all, w_rows(p, 1 - core))

    def t_rows(s, i):
        return at_row(s * rows + i * part, part)

    def block_sends(act):
        def both_parts(target_layer, first):
            for i in range(2):
                act(remote(
                    tok_ref.at[pl.ds(i * part, part), :], tok_all.at[t_rows(z, i), :],
                    t_out.at[first + i], t_in.at[z], (target_layer, chip * 2 + i)))

        @pl.when(core != h)
        def _():
            both_parts(layer(core, 0), 0)

        @pl.when(jnp.logical_and(core == h, u + 1 < half))
        def _():
            both_parts(layer(h, u + 1), 0)

        @pl.when(jnp.logical_and(core == h, u > 0))
        def _():
            both_parts(layer(h, u - 1), 2)

        @pl.when(core == h)
        def _():
            act(remote(
                tok_ref, tok_all.at[at_row(z * rows, rows), :], t_out.at[4], t_pass.at[z], (z, partner)))

    def forward(s, outward, inward, n, act):
        block = t_rows(s, core)
        for cond, step in ((outward, 1), (inward, -1)):
            if cond is not None:
                @pl.when(cond)
                def _():
                    act(remote(
                        tok_all.at[block, :], tok_all.at[block, :], t_fwd.at[n], t_in.at[s],
                        (layer(h, u + step), me)))
        act(remote(
            tok_all.at[block, :], tok_all.at[block, :], t_fwd.at[sp + n], t_pass.at[s], (z, partner)))

    near = [lax.rem(u + k, half) for k in range(1, half)]
    sources = [
        (layer(h, v), jnp.logical_and(u > v, u + 1 < half), jnp.logical_and(u < v, u > 0)) for v in near
    ]
    sources += [(layer(1 - h, v), u + 1 < half, None) for v in range(half)]

    def take_tokens(n):
        s, outward, inward = sources[n]
        arrived(t_in.at[s], tok_all, t_rows(s, core))
        forward(s, outward, inward, n, go)

    def own_tokens():
        block = at_row(z * rows, rows)

        @pl.when(core == h)
        def _():
            pltpu.make_async_copy(tok_ref, tok_all.at[block, :], here.at[6]).wait()

        @pl.when(core != h)
        def _():
            arrived(t_pass.at[z], tok_all, block)

    def passed_tokens(n):
        s = sources[n][0]
        arrived(t_pass.at[s], tok_all, t_rows(s, 1 - core))

    goal = (layer(core, z // 2), chip * 2 + z % 2)
    stay = jnp.logical_and(goal[0] == z, z % 2 == core)
    smalls = [(rate_ref, rate_s), (diag_ref, diag_s), (gain_ref, gain_s)]

    @pl.when(jnp.logical_not(stay))
    def _():
        for n, (src, dst) in enumerate(smalls):
            go(remote(src, dst, p_out.at[n], p_in.at[n], goal))

    @pl.when(stay)
    def _():
        for n, (src, dst) in enumerate(smalls):
            pltpu.make_async_copy(src, dst, p_in.at[n]).start()

    decay_direct()
    block_sends(go)
    direct(0)
    decay_relay()
    relay(0)
    direct(1)
    direct(2)
    for n in range(len(sources)):
        take_tokens(n)
    decay_finish()
    finish(0)
    for copy in own[:4]:
        copy.wait()
    own_tokens()
    for n in range(half - 1):
        passed_tokens(n)

    @pl.when(jnp.logical_not(stay))
    def _():
        for n, (src, dst) in enumerate(smalls):
            remote(src, dst, p_out.at[n], p_in.at[n], goal).wait_send()
    for n, (src, dst) in enumerate(smalls):
        remote(dst, dst, p_in.at[n], p_in.at[n], (z, partner)).wait_recv()

    work = Core(
        tok_all, wk_all, wd_all, wv_all, wr_all, up_s, floor_s, rate_s, diag_s, gain_s, out_all, scratch)
    near_rows = h * half * rows
    far_rows = (1 - h) * half * rows
    units = work.keys(near_rows)
    relay(1)
    work.invert(units)
    for n in range(half - 1, len(sources)):
        passed_tokens(n)
    units = work.keys(far_rows)
    relay(2)
    work.invert(units)
    finish(1)
    own[4].wait()
    work.values()
    work.scan()
    finish(2)
    own[5].wait()

    def give(s, n, act):
        block = at_row(s * rows, rows)
        act(remote(
            out_all.at[block, :], out_ref.at[:, cols(slot)], o_out.at[n], o_in.at[slot],
            (s, chip * 2 + h)))

    work.outputs(far_rows, half * rows)
    for v in range(half):
        give(layer(1 - h, v), v, go)
    work.outputs(near_rows, half * rows)
    for n in range(half - 1):
        give(sources[n][0], half + n, go)

    @pl.when(core != h)
    def _():
        give(z, sp - 1, go)

    @pl.when(core == h)
    def _():
        out_ref[:, cols(slot)] = out_all[at_row(z * rows, rows), :]

    def stop(copy):
        copy.wait_send()

    block_sends(stop)
    for n, (s, outward, inward) in enumerate(sources):
        forward(s, outward, inward, n, stop)
    for copy in sent:
        copy.wait_send()
    for close in late:
        close()
    for v in range(half):
        give(layer(1 - h, v), v, stop)
    for n in range(half - 1):
        give(sources[n][0], half + n, stop)

    @pl.when(core != h)
    def _():
        give(z, sp - 1, stop)

    for g in range(sp):
        @pl.when(jnp.logical_not(jnp.logical_and(core == h, slot == g)))
        def _():
            remote(
                out_all.at[pl.ds(0, rows), :], out_ref.at[:, g * chans : (g + 1) * chans],
                o_in.at[g], o_in.at[g], (z, partner)).wait_recv()


def halves_call(sp, dp, side, rows, width, depth, chans, rank):
    vm = pltpu.VMEM
    dma = pltpu.SemaphoreType.DMA
    chips = dp // 2
    other = chips // side
    peers = side + other - 2
    corners = (side - 1) * (other - 1)
    length = rows * sp
    return pl.pallas_call(
        functools.partial(halves_kernel, sp, side, other),
        out_shape=jax.ShapeDtypeStruct((rows, chans * sp), BF),
        in_specs=[pl.BlockSpec(memory_space=pl.ANY)] * 10,
        out_specs=pl.BlockSpec(memory_space=vm),
        scratch_shapes=[
            vm((length, width), BF), vm((width, chans), BF), vm((width, chans), BF), vm((width, chans), BF),
            vm((width, 2 * rank), BF), vm((2, rank, chans), BF), vm((2, chans), F32), vm((2, chans), F32),
            vm((2, chans), F32), vm((1, chans), F32), vm((length, chans), BF),
            dma((3, dp)), dma((4, 2 * peers + 1)), dma((4, 2 * corners)), dma((dp,)), dma((peers + corners,)),
            dma((sp,)), dma((sp,)), dma((5,)), dma((2 * sp,)), dma((3,)), dma((3,)), dma((sp,)), dma((sp,)),
            dma((7,)),
        ] + core_scratch(length, chans),
        compiler_params=pltpu.CompilerParams(
            vmem_limit_bytes=58 * 1024 * 1024, collective_id=0, has_side_effects=True
        ),
        name="halves",
    )


def per_device(
    sp, dp,
    tokens, receptance_weight, key_projection_weight, value_projection_weight,
    decay_down_weight, decay_up_weight, decay_floor_level, correction_rate_logit,
    diagonal_address_factor, head_norm_gain,
):
    rows, width = tokens.shape[1:]
    depth, channels = receptance_weight.shape
    chans = channels // sp
    side = math.isqrt(dp // 2)
    gain = head_norm_gain[None, :]
    if chans % 128 == 0 and sp % 2 == 0 and dp == 2 * side * side and rows % (2 * SPAN) == 0:
        mixed = halves_call(sp, dp, side, rows, width, depth, chans, decay_up_weight.shape[1])(
            tokens[0], receptance_weight, key_projection_weight, value_projection_weight, decay_down_weight,
            decay_up_weight, decay_floor_level, correction_rate_logit, diagonal_address_factor, gain)
        return mixed[None]
    start = lax.axis_index("sp") * chans

    def mine(x):
        return lax.dynamic_slice_in_dim(x, start, chans, axis=x.ndim - 1)

    packed = jnp.concatenate(
        [mine(receptance_weight), mine(key_projection_weight), mine(value_projection_weight),
         decay_down_weight], axis=1)
    mixed = whole_call(sp, dp, rows, width, chans, packed.shape[1])(
        tokens[0], packed, mine(decay_up_weight), mine(decay_floor_level),
        correction_rate_logit, diagonal_address_factor, gain)
    return mixed[None]


def solution(mesh):
    in_specs = (
        P("dp", "sp", None), P("dp", None), P("dp", None), P("dp", None), P("dp", None),
        P(), P(), P(None, "sp"), P(None, "sp"), P("sp"),
    )
    return jax.shard_map(
        functools.partial(per_device, mesh.shape["sp"], mesh.shape["dp"]), mesh=mesh, in_specs=in_specs,
        out_specs=P("dp", "sp", None), check_vma=False,
    )
```

```python
import functools, math
import jax, jax.numpy as jnp
from jax import lax
from jax.experimental import pallas as pl
from jax.experimental.pallas import tpu as pltpu
from jax.sharding import PartitionSpec as P
HEAD = 64
SPAN = 64
BF = jnp.bfloat16
F32 = jnp.float32
NT = (((1,), (1,)), ((), ()))
TN = (((0,), (0,)), ((), ()))


def mm(a, b):
    return jnp.dot(a, b, preferred_element_type=F32)


def dot(a, b, dims):
    return lax.dot_general(a, b, dims, preferred_element_type=F32)


def split(x):
    hi = x.astype(BF)
    return hi, (x - hi.astype(F32)).astype(BF)


def iota(shape, axis):
    return lax.broadcasted_iota(jnp.int32, shape, axis)


def head_ones(chans):
    return (iota((chans, chans), 0) // HEAD == iota((chans, chans), 1) // HEAD).astype(BF)


def head_sum(x, ones):
    hi, lo = split(x)
    return mm(hi, ones) + mm(lo, ones)


def spread(x, mask):
    x = x.astype(BF)
    heads = mask.shape[0] // HEAD
    if heads > 1:
        x = jnp.concatenate([x] * heads, axis=0)
    return x * mask


WIDE = 128


def lanes(x, p):
    return x[:, p * WIDE : (p + 1) * WIDE]


def by_head(x, y, mask, dims=None):
    parts = []
    for p in range(x.shape[1] // WIDE):
        block = spread(lanes(y, p), mask)
        a = lanes(x, p).astype(BF)
        parts.append(mm(a, block) if dims is None else dot(a, block, dims))
    return jnp.concatenate(parts, axis=1)


def at_row(start, size):
    return pl.ds(pl.multiple_of(start, size), size)


class Core:
    def __init__(self, tok, wk, wd, wv, wr, up, floor, rate, diag, gain, out, scratch):
        self.tok, self.wk, self.wd, self.wv, self.wr = tok, wk, wd, wv, wr
        self.up, self.floor, self.rate, self.diag, self.gain, self.out = up, floor, rate, diag, gain, out
        (self.pk_s, self.pv_s, self.inv_s, self.grow_s, self.past_s, self.shrink_s, self.g_s, self.wp_s, self.kend_s,
         self.t_s, self.teg_s, self.step_s, self.tcv_s, self.put_s, self.state_s) = scratch
        self.length, self.chans = out.shape
        self.heads = self.chans // HEAD
        self.rank = up.shape[1]
        self.blocks = self.length // SPAN
        self.half = self.length // 2

    def unit(self, block):
        return at_row(block * SPAN, SPAN)

    def decays(self, start):
        chans, rank, tile = self.chans, self.rank, self.half
        lowered = jnp.tanh(mm(self.tok[at_row(start, tile), :], self.wd[...])).astype(BF)
        ri = iota((SPAN, SPAN), 0)
        ci = iota((SPAN, SPAN), 1)
        first = start // SPAN
        pres = [
            (mm(lowered[:, d * rank : (d + 1) * rank], self.up[d]) + self.floor[d : d + 1, :])
            .astype(BF).astype(F32) for d in range(2)
        ]
        for s in range(tile // SPAN):
            falls = [
                -math.exp(-0.5) * jax.nn.sigmoid(pre[s * SPAN : (s + 1) * SPAN]) for pre in pres
            ]
            here = self.unit(first + s)
            for d, fall in enumerate(falls):
                tri = ((ci <= ri) if d == 0 else (ci >= ri)).astype(BF)
                hi, lo = split(fall)
                inside = mm(tri, hi) + mm(tri, lo)
                mid = 0.5 * (inside[SPAN - 1 :] if d == 0 else inside[:1])
                inside = inside - mid
                self.grow_s[d, here, :] = jnp.exp(inside)
                self.past_s[d, here, :] = jnp.exp(inside - fall)
                self.shrink_s[d, here, :] = jnp.exp(-inside)
                self.g_s[d, pl.ds(pl.multiple_of((first + s) * 8, 8), 8), :] = jnp.broadcast_to(
                    jnp.exp(mid), (8, chans))

    def g_of(self, d, block):
        return self.g_s[d, pl.ds(pl.multiple_of(block * 8, 8), 8), :][:1]

    def keys(self, start):
        chans, tile = self.chans, self.half
        at = at_row(start, tile)
        first = start // SPAN
        pk = mm(self.tok[at, :], self.wk[...]).astype(BF)
        self.pk_s[at, :] = pk
        pk = pk.astype(F32)
        inv = lax.rsqrt(head_sum(pk * pk, head_ones(chans)) + 1.0)
        self.inv_s[at, :] = inv
        normed = pk * inv
        rates = jax.nn.sigmoid(self.rate[...])
        units = []
        for s in range(tile // SPAN):
            cut = slice(s * SPAN, (s + 1) * SPAN)
            here = self.unit(first + s)
            for d in range(2):
                g = self.g_of(d, first + s)
                e = -normed[cut] * self.past_s[d, here, :]
                w = normed[cut] * rates[d : d + 1, :] * self.shrink_s[d, here, :]
                self.wp_s[d, here, :] = w.astype(BF)
                self.kend_s[d, here, :] = (w * g).astype(BF)
                units.append((d, first + s, e.astype(BF), (e * g).astype(BF)))
        return units

    def strict(self, d):
        ti = iota((SPAN, self.chans), 0)
        ji = iota((SPAN, self.chans), 1) % HEAD
        return (ti > ji) if d == 0 else (ti < ji)

    def invert(self, units):
        chans = self.chans
        mask = head_ones(WIDE)
        ti = iota((SPAN, chans), 0)
        ji = iota((SPAN, chans), 1) % HEAD
        eye = (ti == ji).astype(F32)
        full = [
            jnp.where(self.strict(d), by_head(e, self.wp_s[d, self.unit(block), :], mask, NT), 0.0)
            for d, block, e, _ in units
        ]
        near = ti // 4 == ji // 4
        base = [jnp.where(near, a, 0.0) for a in full]
        square = [by_head(a, a, mask) for a in base]
        inverse = [eye + a for a in base]
        inverse = [t + by_head(t, a2, mask) for t, a2 in zip(inverse, square)]
        size = 4
        while size < SPAN:
            far = jnp.logical_and(ti // (2 * size) == ji // (2 * size), ti // size != ji // size)
            first = [by_head(t, jnp.where(far, a, 0.0), mask) for t, a in zip(inverse, full)]
            inverse = [t + by_head(f, t, mask) for t, f in zip(inverse, first)]
            size *= 2
        tegs = []
        for (d, block, _, eg), t in zip(units, inverse):
            t = (t - eye).astype(BF)
            self.t_s[d, self.unit(block), :] = t
            tegs.append((eg.astype(F32) + by_head(t, eg, mask)).astype(BF))
        ones = head_ones(chans)
        for (d, block, _, _), teg in zip(units, tegs):
            self.teg_s[d, self.unit(block), :] = teg
            self.step_s[d, at_row(block * chans, chans), :] = (
                dot(teg, self.kend_s[d, self.unit(block), :], TN).astype(BF) * ones)

    def values(self):
        chans = self.chans
        small = head_ones(WIDE)
        mask = head_ones(chans).astype(F32)
        pv = mm(self.tok[...], self.wv[...]).astype(BF)
        self.pv_s[...] = pv
        cv = pv.astype(F32) / self.inv_s[...]
        each = 4
        for group in range(0, self.blocks, each):
            work = []
            for block in range(group, min(group + each, self.blocks)):
                cut = slice(block * SPAN, (block + 1) * SPAN)
                for d in range(2):
                    tcv = cv[cut] + by_head(self.t_s[d, cut, :], cv[cut], small)
                    self.tcv_s[d, cut, :] = tcv
                    work.append((d, cut, tcv.astype(BF)))
            puts = [dot(tcv, self.kend_s[d, cut, :], TN) for d, cut, tcv in work]
            for (d, cut, _), put in zip(work, puts):
                put = put * mask
                self.put_s[d, cut, :] = sum(put[h * HEAD : (h + 1) * HEAD] for h in range(self.heads))

    def scan(self):
        states = [jnp.zeros((HEAD, self.chans), F32) for _ in range(2)]
        for step in range(self.blocks):
            for d in range(2):
                block = step if d == 0 else self.blocks - 1 - step
                cut = slice(block * SPAN, (block + 1) * SPAN)
                state = states[d]
                low = state.astype(BF)
                self.state_s[d, cut, :] = low
                if step < self.blocks - 1:
                    g = self.g_s[d, block * 8 : block * 8 + 1, :]
                    step_w = self.step_s[d, block * self.chans : (block + 1) * self.chans, :]
                    states[d] = state * (g * g) + mm(low, step_w) + self.put_s[d, cut, :]

    def outputs(self, start, tile, p):
        mask = head_ones(WIDE)
        at = at_row(start, tile)
        cols = slice(p * WIDE, (p + 1) * WIDE)
        first = start // SPAN
        pr = mm(self.tok[at, :], self.wr[:, cols]).astype(BF).astype(F32)
        pp = pr * self.pk_s[at, cols].astype(F32)
        rates = jax.nn.sigmoid(self.rate[:, cols])
        both = jnp.sum(rates * self.diag[:, cols], axis=0, keepdims=True)
        inv = self.inv_s[at, cols]
        total = head_sum(pp * both, mask) * self.pv_s[at, cols].astype(F32)
        diags = [head_sum(pp * rates[d : d + 1, :], mask) * inv for d in range(2)]
        ti = iota((SPAN, WIDE), 0)
        ji = iota((SPAN, WIDE), 1) % HEAD
        units = [(d, s) for s in range(tile // SPAN) for d in range(2)]
        bs, reads = [], []
        for d, s in units:
            here = self.unit(first + s)
            q = pr[s * SPAN : (s + 1) * SPAN] * self.grow_s[d, here, cols]
            bs.append(by_head(q, self.wp_s[d, here, cols], mask, NT))
            g = self.g_s[d, pl.ds(pl.multiple_of((first + s) * 8, 8), 8), cols][:1]
            lhs = jnp.concatenate([self.teg_s[d, here, cols], (q * g).astype(BF)], axis=0)
            reads.append(by_head(lhs, self.state_s[d, here, cols], mask, NT))
        ys = [[], []]
        for (d, s), b, read in zip(units, bs, reads):
            exact = self.tcv_s[d, self.unit(first + s), cols] + read[:SPAN]
            b = jnp.where((ti > ji) if d == 0 else (ti < ji), b, 0.0)
            ys[d].append(
                read[SPAN:] + by_head(b, exact, mask) + diags[d][s * SPAN : (s + 1) * SPAN] * exact)
        ys = [jnp.concatenate(y, axis=0) for y in ys]
        means = [head_sum(y, mask) * (1.0 / HEAD) for y in ys]
        centred = [y - mean for y, mean in zip(ys, means)]
        variances = [head_sum(c * c, mask) * (1.0 / HEAD) for c in centred]
        for c, variance in zip(centred, variances):
            total = total + c * lax.rsqrt(variance + 0.00064) * self.gain[:, cols]
        self.out[at, cols] = total.astype(BF)


def core_scratch(length, chans):
    vm = pltpu.VMEM
    both = lambda n, dt: vm((2, n, chans), dt)
    blocks = length // SPAN
    return [
        vm((length, chans), BF), vm((length, chans), BF), vm((length, chans), F32),
        both(length, F32), both(length, F32), both(length, F32), both(blocks * 8, F32),
        both(length, BF), both(length, BF),
        both(length, BF), both(length, BF), both(blocks * chans, BF), both(length, F32),
        both(length, F32), both(length, BF),
    ]


def core_kernel(
    tok_ref, w_ref, up_ref, floor_ref, rate_ref, diag_ref, gain_ref, out_ref,
    eq_s, wp_s, qe_s, kend_s, cv_s, own_s, decay_s, diag_s, t_s, b_s, state_s, y_s,
    arrivals=(),
):
    length, chans = out_ref.shape
    heads = chans // HEAD
    rank = up_ref.shape[1]
    rows = min(256, length)
    blocks = length // SPAN

    def head_ones():
        return (iota((chans, chans), 0) // HEAD == iota((chans, chans), 1) // HEAD).astype(BF)

    def head_sum(x, ones):
        hi, lo = split(x)
        return mm(hi, ones) + mm(lo, ones)

    def at_block(block):
        return pl.ds(pl.multiple_of(block * SPAN, SPAN), SPAN)

    def project(ready):
        tile = SPAN * len(ready)

        def put(ref, x, *lead):
            for s, block in enumerate(ready):
                ref[(*lead, at_block(block), slice(None))] = x[s * SPAN : (s + 1) * SPAN]

        source = jnp.concatenate([tok_ref[at_block(block), :] for block in ready], axis=0)
        pr = mm(source, w_ref[:, :chans]).astype(BF).astype(F32)
        pk = mm(source, w_ref[:, chans : 2 * chans]).astype(BF).astype(F32)
        pv = mm(source, w_ref[:, 2 * chans : 3 * chans]).astype(BF).astype(F32)
        lowered = jnp.tanh(mm(source, w_ref[:, 3 * chans :])).astype(BF)
        ones = head_ones()
        norm2 = head_sum(pk * pk, ones) + 1.0
        inv = lax.rsqrt(norm2)
        scale = norm2 * inv
        normed = pk * inv
        put(cv_s, scale * pv)
        rates = jax.nn.sigmoid(rate_ref[...])
        both = jnp.sum(rates * diag_ref[...], axis=0, keepdims=True)
        put(own_s, head_sum(pr * pk * both, ones) * pv)
        ri = iota((tile, tile), 0)
        ci = iota((tile, tile), 1)
        same = ri // SPAN == ci // SPAN
        whole = same.astype(BF)
        for d in range(2):
            pre = (
                mm(lowered[:, d * rank : (d + 1) * rank], up_ref[d]) + floor_ref[d : d + 1, :]
            ).astype(BF).astype(F32)
            fall = -math.exp(-0.5) * jax.nn.sigmoid(pre)
            tri = jnp.logical_and(same, (ci <= ri) if d == 0 else (ci >= ri)).astype(BF)
            hi, lo = split(fall)
            inclusive = mm(tri, hi) + mm(tri, lo)
            final = mm(whole, hi) + mm(whole, lo)
            half = 0.5 * final
            grow = jnp.exp(inclusive - half)
            shrink = jnp.exp(half - inclusive)
            g = jnp.exp(half)
            e = -normed * (grow * jnp.exp(-fall))
            q = pr * grow
            w = normed * rates[d : d + 1, :] * shrink
            put(wp_s, w.astype(BF), d)
            put(kend_s, (w * g).astype(BF), d)
            eb, qb = e.astype(BF), q.astype(BF)
            eg, qg = (e * g).astype(BF), (q * g).astype(BF)
            g2 = g * g
            put(diag_s, head_sum(pr * normed * rates[d : d + 1, :], ones), d)
            for s, block in enumerate(ready):
                cut = slice(s * SPAN, (s + 1) * SPAN)
                base = pl.multiple_of(block * 2 * SPAN, 2 * SPAN)
                eq_s[d, pl.ds(base, SPAN), :] = eb[cut]
                eq_s[d, pl.ds(base + SPAN, SPAN), :] = qb[cut]
                qe_s[d, pl.ds(base, SPAN), :] = eg[cut]
                qe_s[d, pl.ds(base + SPAN, SPAN), :] = qg[cut]
                decay_s[d, pl.ds(pl.multiple_of(block * 8, 8), 8), :] = g2[
                    s * SPAN : s * SPAN + 8
                ]

    def spread(x, mask):
        x = x.astype(BF)
        if heads > 1:
            x = jnp.concatenate([x] * heads, axis=0)
        return x * mask

    def invert(ready):
        mask = head_ones()
        ti = iota((SPAN, chans), 0)
        ji = iota((SPAN, chans), 1) % HEAD
        eye = (ti == ji).astype(F32)
        work = []
        for block in ready:
            for d in range(2):
                two = pl.ds(pl.multiple_of(block * 2 * SPAN, 2 * SPAN), 2 * SPAN)
                at = pl.ds(pl.multiple_of(block * SPAN, SPAN), SPAN)
                ab = lax.dot_general(
                    eq_s[d, two, :], spread(wp_s[d, at, :], mask), NT, preferred_element_type=F32
                )
                strict = (ti > ji) if d == 0 else (ti < ji)
                b_s[d, at, :] = jnp.where(strict, ab[SPAN:], 0.0).astype(BF)
                work.append((d, at, jnp.where(strict, ab[:SPAN], 0.0)))
        near = ti // 4 == ji // 4
        full = [a for _, _, a in work]
        base = [jnp.where(near, a, 0.0) for a in full]
        square = [mm(a.astype(BF), spread(a, mask)) for a in base]
        inverse = [eye + a for a in base]
        inverse = [t + mm(t.astype(BF), spread(a2, mask)) for t, a2 in zip(inverse, square)]
        size = 4
        while size < SPAN:
            far = jnp.logical_and(ti // (2 * size) == ji // (2 * size), ti // size != ji // size)
            first = [
                mm(t.astype(BF), spread(jnp.where(far, a, 0.0), mask))
                for t, a in zip(inverse, full)
            ]
            inverse = [t + mm(f.astype(BF), spread(t, mask)) for t, f in zip(inverse, first)]
            size *= 2
        for (d, at, _), t in zip(work, inverse):
            t_s[d, at, :] = (t - eye).astype(BF)

    for settle, ready in arrivals:
        settle()
        project(ready)
        invert(ready)

    state_s[...] = jnp.zeros_like(state_s)

    @pl.loop(0, blocks)
    def _(step):
        mask = head_ones()
        for d in range(2):
            block = step if d == 0 else blocks - 1 - step
            two = pl.ds(pl.multiple_of(block * 2 * SPAN, 2 * SPAN), 2 * SPAN)
            at = pl.ds(pl.multiple_of(block * SPAN, SPAN), SPAN)
            state = state_s[d]
            read = lax.dot_general(
                qe_s[d, two, :], state.astype(BF), NT, preferred_element_type=F32
            )
            x = cv_s[at, :] + read[:SPAN]
            exact = x + mm(t_s[d, at, :], spread(x, mask))
            a = exact.astype(BF)
            y_s[d, at, :] = read[SPAN:] + mm(b_s[d, at, :], spread(a, mask)) + diag_s[d, at, :] * exact
            decay = decay_s[d, pl.ds(pl.multiple_of(block * 8, 8), 8), :][:1]
            put = lax.dot_general(a, kend_s[d, at, :], TN, preferred_element_type=F32)
            state_s[d] = state * decay + put * mask.astype(F32)

    @pl.loop(0, length // rows)
    def _(step):
        at = pl.ds(pl.multiple_of(step * rows, rows), rows)
        ones = head_ones()
        total = own_s[at, :]
        for d in range(2):
            y = y_s[d, at, :]
            centred = y - head_sum(y, ones) * (1.0 / HEAD)
            variance = head_sum(centred * centred, ones) * (1.0 / HEAD)
            total = total + centred * lax.rsqrt(variance + 0.00064) * gain_ref[...]
        out_ref[at, :] = total.astype(BF)


MESH = pl.DeviceIdType.MESH


def whole_kernel(
    sp, dp, tok_ref, w_ref, up_ref, floor_ref, rate_ref, diag_ref, gain_ref, out_ref,
    tok_all, w_all, out_all, slots,
    ring_out, ring_in, far_out, far_in, pass_out, pass_in, back_out, back_in, *scratch,
):
    rows = tok_ref.shape[0]
    half_rows = rows // 2
    depth = w_ref.shape[0]
    chans = out_all.shape[1]
    chips = dp // 2
    z = lax.axis_index("sp")
    me = lax.axis_index("dp")
    chip = me // 2
    core = me % 2
    partner = chip * 2 + 1 - core

    def peer(k):
        return lax.rem(chip + k, chips) * 2 + core

    def z_peer(k):
        return lax.rem(z + k, sp)

    barrier = pltpu.get_barrier_semaphore()
    for target in [(z, partner)] + [(z, peer(k)) for k in range(1, chips)] + [
        (z_peer(k), me) for k in range(1, sp)
    ]:
        pl.semaphore_signal(barrier, inc=1, device_id=target, device_id_type=MESH)
    pl.semaphore_wait(barrier, chips + sp - 1)

    def remote(src, dst, out_sem, in_sem, target):
        copy = pltpu.make_async_remote_copy(
            src_ref=src, dst_ref=dst, send_sem=out_sem, recv_sem=in_sem,
            device_id=target, device_id_type=MESH,
        )
        copy.start()
        return copy

    def w_at(device):
        return pl.ds(pl.multiple_of(device * depth, depth), depth)

    def ring_step(s):
        copies = []
        for way in range(2):
            owner = z_peer(sp - s) if way == 0 else z_peer(s)
            at = pl.ds(
                pl.multiple_of(owner * rows + way * half_rows, half_rows), half_rows
            )
            first = tok_ref.at[pl.ds(way * half_rows, half_rows), :]
            copies.append(
                remote(
                    first if s == 0 else tok_all.at[at, :], tok_all.at[at, :],
                    ring_out.at[way, s], ring_in.at[way, s],
                    (z_peer(1) if way == 0 else z_peer(sp - 1), me),
                )
            )
        return copies

    ring = [ring_step(0)] if sp > 1 else []
    far = [
        remote(w_ref, w_all.at[w_at(me), :], far_out.at[k], far_in.at[k], (z, peer(k)))
        for k in range(1, chips)
    ]
    passed = [remote(w_ref, w_all.at[w_at(me), :], pass_out.at[0], pass_in.at[0], (z, partner))]
    w_all[w_at(me), :] = w_ref[...]
    tok_all[pl.ds(pl.multiple_of(z * rows, rows), rows), :] = tok_ref[...]
    for s in range(max(sp, chips) - 1):
        if s < sp - 2:
            for copy in ring[s]:
                copy.wait_recv()
            ring.append(ring_step(s + 1))
        if s < chips - 1:
            far[s].wait_recv()
            block = w_at(peer(chips - 1 - s))
            passed.append(
                remote(
                    w_all.at[block, :], w_all.at[block, :],
                    pass_out.at[s + 1], pass_in.at[s + 1], (z, partner),
                )
            )
    for copy in passed:
        copy.wait_recv()

    def last_ring():
        for copy in ring[-1]:
            copy.wait_recv()

    per = rows // SPAN
    arrivals = [(lambda: None, [z * per + b for b in range(per)])]
    for s in range(sp - 1):
        before, after = z_peer(sp - 1 - s), z_peer(s + 1)
        ready = [before * per + b for b in range(per // 2)]
        ready += [after * per + b for b in range(per // 2, per)]
        arrivals.append((last_ring if s == sp - 2 else lambda: None, ready))

    core_kernel(
        tok_all, w_all, up_ref, floor_ref, rate_ref, diag_ref, gain_ref, out_all, *scratch,
        arrivals=arrivals,
    )
    for copy in far + passed + [c for pair in ring for c in pair]:
        copy.wait_send()

    def out_at(owner):
        return pl.ds(pl.multiple_of(owner * rows, rows), rows)

    back = [
        remote(
            out_all.at[out_at(z_peer(k)), :], slots.at[z], back_out.at[k], back_in.at[k],
            (z_peer(k), me),
        )
        for k in range(1, sp)
    ]
    slots[z] = out_all[out_at(z), :]
    for copy in back:
        copy.wait()
    for s in range(sp):
        out_ref[:, s * chans : (s + 1) * chans] = slots[s]


def whole_call(sp, dp, rows, depth, chans, width):
    vm = pltpu.VMEM
    dma = pltpu.SemaphoreType.DMA
    length = rows * sp
    both = lambda n, dt: vm((2, n, chans), dt)
    return pl.pallas_call(
        functools.partial(whole_kernel, sp, dp),
        out_shape=jax.ShapeDtypeStruct((rows, chans * sp), BF),
        in_specs=[pl.BlockSpec(memory_space=vm)] * 7,
        out_specs=pl.BlockSpec(memory_space=vm),
        scratch_shapes=[
            vm((length, depth), BF), vm((depth, width), BF), vm((length, chans), BF),
            vm((sp, rows, chans), BF),
            dma((2, sp)), dma((2, sp)), dma((dp,)), dma((dp,)), dma((dp,)), dma((dp,)),
            dma((sp,)), dma((sp,)),
            both(2 * length, BF), both(length, BF), both(2 * length, BF), both(length, BF),
            vm((length, chans), F32), vm((length, chans), F32),
            both(length // SPAN * 8, F32), both(length, F32), both(length, BF), both(length, BF),
            vm((2, chans, chans), F32), both(length, F32),
        ],
        compiler_params=pltpu.CompilerParams(
            vmem_limit_bytes=58 * 1024 * 1024, collective_id=0, has_side_effects=True
        ),
        name="whole",
    )


def halves_kernel(
    sp, side, other, tok_ref, wr_ref, wk_ref, wv_ref, wd_ref, up_ref, floor_ref, rate_ref, diag_ref, gain_ref,
    out_ref, tok_all, wk_all, wv_all, wr_all, wd_all, up_s, floor_s, rate_s, diag_s, gain_s, out_all,
    w_in, w_out, relay_out, d_in, d_pass, t_in, t_pass, t_out, t_fwd, p_in, p_out, o_in, o_out, here, *scratch,
):
    rows = tok_ref.shape[0]
    depth = wk_ref.shape[0]
    chans = wk_all.shape[1]
    half = sp // 2
    part = rows // 2
    z = lax.axis_index("sp")
    me = lax.axis_index("dp")
    core = me % 2
    chip = me // 2
    cy, cx = chip // side, chip % side
    h = z // half
    j = z % half
    u = jnp.where(h == 1, j, half - 1 - j)
    slot = u * 2 + core
    partner = chip * 2 + 1 - core

    def layer(hh, uu):
        return half - 1 - uu + hh * (2 * uu + 1)

    def x_peer(k):
        return cy * side + lax.rem(cx + k, side)

    def y_peer(k):
        return lax.rem(cy + k, other) * side + cx

    x_peers = [x_peer(k) for k in range(1, side)]
    y_peers = [y_peer(k) for k in range(1, other)]

    def local(src, dst, n):
        copy = pltpu.make_async_copy(src, dst, here.at[n])
        copy.start()
        return copy

    def cols(who):
        return pl.ds(pl.multiple_of(who * chans, chans), chans)

    mine = at_row(me * depth, depth)
    own = [
        local(wd_ref, wd_all.at[mine, :], 0),
        local(wk_ref.at[:, cols(slot)], wk_all.at[mine, :], 1),
        local(up_ref.at[:, :, cols(slot)], up_s, 2),
        local(floor_ref.at[:, cols(slot)], floor_s, 3),
        local(wv_ref.at[:, cols(slot)], wv_all.at[mine, :], 4),
        local(wr_ref.at[:, cols(slot)], wr_all.at[mine, :], 5),
    ]

    @pl.when(core == h)
    def _():
        local(tok_ref, tok_all.at[at_row(z * rows, rows), :], 6)

    barrier = pltpu.get_barrier_semaphore()
    greet = [(z, p * 2 + k) for p in x_peers + y_peers for k in range(2)]
    greet += [(lax.rem(z + n, sp), chip * 2 + k) for n in range(1, sp) for k in range(2)]
    greet.append((z, partner))
    for target in greet:
        pl.semaphore_signal(barrier, inc=1, device_id=target, device_id_type=MESH)
    pl.semaphore_wait(barrier, len(greet))

    def remote(src, dst, out_sem, in_sem, target):
        return pltpu.make_async_remote_copy(
            src_ref=src, dst_ref=dst, send_sem=out_sem, recv_sem=in_sem,
            device_id=target, device_id_type=MESH,
        )

    def go(copy):
        copy.start()
        return copy

    sent = []
    wide = chans // WIDE
    pieces = [(wk_ref, wk_all, 0, chans), (wv_ref, wv_all, 0, chans)]
    pieces += [(wr_ref, wr_all, p * WIDE, WIDE) for p in range(wide)]
    decay = len(pieces)

    def take(n, who):
        src, _, low, size = pieces[n]
        return src.at[:, pl.ds(pl.multiple_of(who * chans + low, WIDE), size)]

    def landing(n, block):
        _, dst, low, size = pieces[n]
        return dst.at[block, low : low + size]

    def direct(n):
        for i, p in enumerate(x_peers + y_peers):
            for k in range(2):
                sent.append(go(remote(
                    take(n, u * 2 + k), landing(n, mine),
                    w_out.at[n, i * 2 + k], w_in.at[n, me], (z, p * 2 + k),
                )))
        last = 2 * len(x_peers + y_peers)
        sent.append(go(remote(
            take(n, u * 2 + 1 - core), landing(n, mine),
            w_out.at[n, last], w_in.at[n, me], (z, partner),
        )))

    def wait_for(sem, dst):
        remote(dst, dst, sem, sem, (z, partner)).wait_recv()

    def arrived(sem, dst, block):
        wait_for(sem, dst.at[block, :])

    def w_rows(p, c):
        return at_row((p * 2 + c) * depth, depth)

    def relay(n):
        count = 0
        for c, froms, tos in ((0, x_peers, y_peers), (1, y_peers, x_peers)):
            for p in froms:
                block = w_rows(p, c)
                wait_for(w_in.at[n, p * 2 + c], landing(n, block))
                for q in tos:
                    sent.append(go(remote(
                        landing(n, block), landing(n, block),
                        relay_out.at[n, count], w_in.at[n, p * 2 + c], (z, q * 2 + core),
                    )))
                    count += 1

    def finish(n):
        for c, others in ((1, x_peers), (0, y_peers)):
            for p in others:
                wait_for(w_in.at[n, p * 2 + c], landing(n, w_rows(p, c)))
        for ky in range(1, other):
            for kx in range(1, side):
                p = lax.rem(cy + ky, other) * side + lax.rem(cx + kx, side)
                for c in range(2):
                    wait_for(w_in.at[n, p * 2 + c], landing(n, w_rows(p, c)))
        wait_for(w_in.at[n, partner], landing(n, w_rows(chip, 1 - core)))

    def decay_direct():
        for i, p in enumerate(x_peers + y_peers):
            sent.append(go(remote(
                wd_ref, wd_all.at[mine, :], w_out.at[decay, i], d_in.at[me], (z, p * 2 + core))))
        sent.append(go(remote(
            wd_ref, wd_all.at[mine, :], w_out.at[decay, len(x_peers + y_peers)], d_in.at[me], (z, partner))))

    def decay_pass(p, n):
        block = w_rows(p, core)
        sent.append(go(remote(
            wd_all.at[block, :], wd_all.at[block, :], d_pass.at[n], d_in.at[p * 2 + core], (z, partner))))

    late = []

    def decay_relay():
        for c, froms, tos in ((0, x_peers, y_peers), (1, y_peers, x_peers)):
            @pl.when(core == c)
            def _():
                count = 0
                for p in froms:
                    block = w_rows(p, c)
                    arrived(d_in.at[p * 2 + c], wd_all, block)
                    for q in tos:
                        go(remote(
                            wd_all.at[block, :], wd_all.at[block, :],
                            relay_out.at[decay, count], d_in.at[p * 2 + c], (z, q * 2 + c)))
                        count += 1
                for p in tos:
                    arrived(d_in.at[p * 2 + c], wd_all, w_rows(p, c))

            def close(c=c, froms=froms, tos=tos):
                @pl.when(core == c)
                def _():
                    count = 0
                    for p in froms:
                        block = w_rows(p, c)
                        for q in tos:
                            remote(
                                wd_all.at[block, :], wd_all.at[block, :],
                                relay_out.at[decay, count], d_in.at[p * 2 + c], (z, q * 2 + c)).wait_send()
                            count += 1

            late.append(close)
        for n, p in enumerate(x_peers + y_peers):
            decay_pass(p, n)

    def decay_finish():
        n = len(x_peers + y_peers)
        corners = [
            lax.rem(cy + ky, other) * side + lax.rem(cx + kx, side)
            for ky in range(1, other) for kx in range(1, side)
        ]
        for p in corners:
            arrived(d_in.at[p * 2 + core], wd_all, w_rows(p, core))
            decay_pass(p, n)
            n += 1
        arrived(d_in.at[partner], wd_all, w_rows(chip, 1 - core))
        for p in x_peers + y_peers + corners:
            arrived(d_in.at[p * 2 + 1 - core], wd_all, w_rows(p, 1 - core))

    def t_rows(s, i):
        return at_row(s * rows + i * part, part)

    def block_sends(act):
        def both_parts(target_layer, first):
            for i in range(2):
                act(remote(
                    tok_ref.at[pl.ds(i * part, part), :], tok_all.at[t_rows(z, i), :],
                    t_out.at[first + i], t_in.at[z], (target_layer, chip * 2 + i)))

        @pl.when(core != h)
        def _():
            both_parts(layer(core, 0), 0)

        @pl.when(jnp.logical_and(core == h, u + 1 < half))
        def _():
            both_parts(layer(h, u + 1), 0)

        @pl.when(jnp.logical_and(core == h, u > 0))
        def _():
            both_parts(layer(h, u - 1), 2)

        @pl.when(core == h)
        def _():
            act(remote(
                tok_ref, tok_all.at[at_row(z * rows, rows), :], t_out.at[4], t_pass.at[z], (z, partner)))

    def forward(s, outward, inward, n, act):
        block = t_rows(s, core)
        for cond, step in ((outward, 1), (inward, -1)):
            if cond is not None:
                @pl.when(cond)
                def _():
                    act(remote(
                        tok_all.at[block, :], tok_all.at[block, :], t_fwd.at[n], t_in.at[s],
                        (layer(h, u + step), me)))
        act(remote(
            tok_all.at[block, :], tok_all.at[block, :], t_fwd.at[sp + n], t_pass.at[s], (z, partner)))

    near = [lax.rem(u + k, half) for k in range(1, half)]
    sources = [
        (layer(h, v), jnp.logical_and(u > v, u + 1 < half), jnp.logical_and(u < v, u > 0)) for v in near
    ]
    sources += [(layer(1 - h, v), u + 1 < half, None) for v in range(half)]

    def take_tokens(n):
        s, outward, inward = sources[n]
        arrived(t_in.at[s], tok_all, t_rows(s, core))
        forward(s, outward, inward, n, go)

    def own_tokens():
        block = at_row(z * rows, rows)

        @pl.when(core == h)
        def _():
            pltpu.make_async_copy(tok_ref, tok_all.at[block, :], here.at[6]).wait()

        @pl.when(core != h)
        def _():
            arrived(t_pass.at[z], tok_all, block)

    def passed_tokens(n):
        s = sources[n][0]
        arrived(t_pass.at[s], tok_all, t_rows(s, 1 - core))

    goal = (layer(core, z // 2), chip * 2 + z % 2)
    stay = jnp.logical_and(goal[0] == z, z % 2 == core)
    smalls = [(rate_ref, rate_s), (diag_ref, diag_s), (gain_ref, gain_s)]

    @pl.when(jnp.logical_not(stay))
    def _():
        for n, (src, dst) in enumerate(smalls):
            go(remote(src, dst, p_out.at[n], p_in.at[n], goal))

    @pl.when(stay)
    def _():
        for n, (src, dst) in enumerate(smalls):
            pltpu.make_async_copy(src, dst, p_in.at[n]).start()

    decay_direct()
    block_sends(go)
    direct(0)
    decay_relay()
    relay(0)
    direct(1)
    direct(2)
    for n in range(len(sources)):
        take_tokens(n)
    decay_finish()
    for n in (0, 2, 3):
        own[n].wait()
    own_tokens()
    for n in range(half - 1):
        passed_tokens(n)
    work = Core(
        tok_all, wk_all, wd_all, wv_all, wr_all, up_s, floor_s, rate_s, diag_s, gain_s, out_all, scratch)
    near_rows = h * half * rows
    far_rows = (1 - h) * half * rows
    work.decays(near_rows)
    finish(0)
    own[1].wait()

    @pl.when(jnp.logical_not(stay))
    def _():
        for n, (src, dst) in enumerate(smalls):
            remote(src, dst, p_out.at[n], p_in.at[n], goal).wait_send()
    for n, (src, dst) in enumerate(smalls):
        remote(dst, dst, p_in.at[n], p_in.at[n], (z, partner)).wait_recv()

    units = work.keys(near_rows)
    work.invert(units)
    for n in range(half - 1, len(sources)):
        passed_tokens(n)
    work.decays(far_rows)
    units = work.keys(far_rows)
    relay(1)
    for p in range(1, wide):
        direct(2 + p)
    work.invert(units)
    relay(2)
    finish(1)
    own[4].wait()
    work.values()
    work.scan()

    def give(s, p, n, act):
        block = at_row(s * rows, rows)
        low = p * WIDE
        act(remote(
            out_all.at[block, low : low + WIDE],
            out_ref.at[:, pl.ds(pl.multiple_of(slot * chans + low, WIDE), WIDE)],
            o_out.at[p, n], o_in.at[p, slot], (s, chip * 2 + h)))

    def give_far(p, act):
        for v in range(half):
            give(layer(1 - h, v), p, v, act)

    def give_near(p, act):
        for n in range(half - 1):
            give(sources[n][0], p, half + n, act)

        @pl.when(core != h)
        def _():
            give(z, p, sp - 1, act)

    own[5].wait()
    for p in range(wide):
        if p + 1 < wide:
            relay(3 + p)
        finish(2 + p)
        work.outputs(far_rows, half * rows, p)
        give_far(p, go)
        work.outputs(near_rows, half * rows, p)
        give_near(p, go)

    @pl.when(core == h)
    def _():
        out_ref[:, cols(slot)] = out_all[at_row(z * rows, rows), :]

    def stop(copy):
        copy.wait_send()

    block_sends(stop)
    for n, (s, outward, inward) in enumerate(sources):
        forward(s, outward, inward, n, stop)
    for copy in sent:
        copy.wait_send()
    for close in late:
        close()
    for p in range(wide):
        give_far(p, stop)
        give_near(p, stop)
        for g in range(sp):
            low = g * chans + p * WIDE

            @pl.when(jnp.logical_not(jnp.logical_and(core == h, slot == g)))
            def _():
                wait_for(o_in.at[p, g], out_ref.at[:, low : low + WIDE])


def halves_call(sp, dp, side, rows, width, depth, chans, rank):
    vm = pltpu.VMEM
    dma = pltpu.SemaphoreType.DMA
    chips = dp // 2
    other = chips // side
    peers = side + other - 2
    corners = (side - 1) * (other - 1)
    length = rows * sp
    wide = chans // WIDE
    return pl.pallas_call(
        functools.partial(halves_kernel, sp, side, other),
        out_shape=jax.ShapeDtypeStruct((rows, chans * sp), BF),
        in_specs=[pl.BlockSpec(memory_space=pl.ANY)] * 10,
        out_specs=pl.BlockSpec(memory_space=vm),
        scratch_shapes=[
            vm((length, width), BF), vm((width, chans), BF), vm((width, chans), BF), vm((width, chans), BF),
            vm((width, 2 * rank), BF), vm((2, rank, chans), BF), vm((2, chans), F32), vm((2, chans), F32),
            vm((2, chans), F32), vm((1, chans), F32), vm((length, chans), BF),
            dma((2 + wide, dp)), dma((3 + wide, 2 * peers + 1)), dma((3 + wide, 2 * corners)), dma((dp,)), dma((peers + corners,)),
            dma((sp,)), dma((sp,)), dma((5,)), dma((2 * sp,)), dma((3,)), dma((3,)), dma((wide, sp)), dma((wide, sp)),
            dma((7,)),
        ] + core_scratch(length, chans),
        compiler_params=pltpu.CompilerParams(
            vmem_limit_bytes=58 * 1024 * 1024, collective_id=0, has_side_effects=True
        ),
        name="halves",
    )


def per_device(
    sp, dp,
    tokens, receptance_weight, key_projection_weight, value_projection_weight,
    decay_down_weight, decay_up_weight, decay_floor_level, correction_rate_logit,
    diagonal_address_factor, head_norm_gain,
):
    rows, width = tokens.shape[1:]
    depth, channels = receptance_weight.shape
    chans = channels // sp
    side = math.isqrt(dp // 2)
    gain = head_norm_gain[None, :]
    if chans % 128 == 0 and sp % 2 == 0 and dp == 2 * side * side and rows % (2 * SPAN) == 0:
        mixed = halves_call(sp, dp, side, rows, width, depth, chans, decay_up_weight.shape[1])(
            tokens[0], receptance_weight, key_projection_weight, value_projection_weight, decay_down_weight,
            decay_up_weight, decay_floor_level, correction_rate_logit, diagonal_address_factor, gain)
        return mixed[None]
    start = lax.axis_index("sp") * chans

    def mine(x):
        return lax.dynamic_slice_in_dim(x, start, chans, axis=x.ndim - 1)

    packed = jnp.concatenate(
        [mine(receptance_weight), mine(key_projection_weight), mine(value_projection_weight),
         decay_down_weight], axis=1)
    mixed = whole_call(sp, dp, rows, width, chans, packed.shape[1])(
        tokens[0], packed, mine(decay_up_weight), mine(decay_floor_level),
        correction_rate_logit, diagonal_address_factor, gain)
    return mixed[None]


def solution(mesh):
    in_specs = (
        P("dp", "sp", None), P("dp", None), P("dp", None), P("dp", None), P("dp", None),
        P(), P(), P(None, "sp"), P(None, "sp"), P("sp"),
    )
    return jax.shard_map(
        functools.partial(per_device, mesh.shape["sp"], mesh.shape["dp"]), mesh=mesh, in_specs=in_specs,
        out_specs=P("dp", "sp", None), check_vma=False,
    )
```

```python
import functools, math
import jax, jax.numpy as jnp
from jax import lax
from jax.experimental import pallas as pl
from jax.experimental.pallas import tpu as pltpu
from jax.sharding import PartitionSpec as P
HEAD = 64
SPAN = 64
BF = jnp.bfloat16
F32 = jnp.float32
NT = (((1,), (1,)), ((), ()))
TN = (((0,), (0,)), ((), ()))


def mm(a, b):
    return jnp.dot(a, b, preferred_element_type=F32)


def dot(a, b, dims):
    return lax.dot_general(a, b, dims, preferred_element_type=F32)


def split(x):
    hi = x.astype(BF)
    return hi, (x - hi.astype(F32)).astype(BF)


def iota(shape, axis):
    return lax.broadcasted_iota(jnp.int32, shape, axis)


def head_ones(chans):
    return (iota((chans, chans), 0) // HEAD == iota((chans, chans), 1) // HEAD).astype(BF)


def head_sum(x, ones):
    hi, lo = split(x)
    if ones.shape[0] > WIDE:
        return mm(hi, ones) + mm(lo, ones)
    return mm(jnp.concatenate([hi, lo], axis=1), jnp.concatenate([ones, ones], axis=0))


def spread(x, mask):
    x = x.astype(BF)
    heads = mask.shape[0] // HEAD
    if heads > 1:
        x = jnp.concatenate([x] * heads, axis=0)
    return x * mask


WIDE = 128


def lanes(x, p):
    return x[:, p * WIDE : (p + 1) * WIDE]


def by_head(x, y, mask, dims=None):
    parts = []
    for p in range(x.shape[1] // WIDE):
        block = spread(lanes(y, p), mask)
        a = lanes(x, p).astype(BF)
        parts.append(mm(a, block) if dims is None else dot(a, block, dims))
    return jnp.concatenate(parts, axis=1)


def at_row(start, size):
    return pl.ds(pl.multiple_of(start, size), size)


class Core:
    def __init__(self, tok, wk, wd, wv, wr, up, floor, rate, diag, gain, out, scratch):
        self.tok, self.wk, self.wd, self.wv, self.wr = tok, wk, wd, wv, wr
        self.up, self.floor, self.rate, self.diag, self.gain, self.out = up, floor, rate, diag, gain, out
        (self.pk_s, self.pv_s, self.inv_s, self.grow_s, self.past_s, self.shrink_s, self.g_s, self.wp_s, self.kend_s,
         self.t_s, self.teg_s, self.step_s, self.tcv_s, self.put_s, self.state_s) = scratch
        self.length, self.chans = out.shape
        self.heads = self.chans // HEAD
        self.rank = up.shape[1]
        self.blocks = self.length // SPAN
        self.half = self.length // 2

    def unit(self, block):
        return at_row(block * SPAN, SPAN)

    def decays(self, start):
        chans, rank, tile = self.chans, self.rank, self.half
        lowered = jnp.tanh(mm(self.tok[at_row(start, tile), :], self.wd[...])).astype(BF)
        ri = iota((SPAN, SPAN), 0)
        ci = iota((SPAN, SPAN), 1)
        first = start // SPAN
        pres = [
            (mm(lowered[:, d * rank : (d + 1) * rank], self.up[d]) + self.floor[d : d + 1, :])
            .astype(BF).astype(F32) for d in range(2)
        ]
        for s in range(tile // SPAN):
            falls = [
                -math.exp(-0.5) * jax.nn.sigmoid(pre[s * SPAN : (s + 1) * SPAN]) for pre in pres
            ]
            here = self.unit(first + s)
            for d, fall in enumerate(falls):
                tri = ((ci <= ri) if d == 0 else (ci >= ri)).astype(BF)
                hi, lo = split(fall)
                inside = mm(tri, hi) + mm(tri, lo)
                mid = 0.5 * (inside[SPAN - 1 :] if d == 0 else inside[:1])
                inside = inside - mid
                self.grow_s[d, here, :] = jnp.exp(inside)
                self.past_s[d, here, :] = jnp.exp(inside - fall)
                self.shrink_s[d, here, :] = jnp.exp(-inside)
                self.g_s[d, pl.ds(pl.multiple_of((first + s) * 8, 8), 8), :] = jnp.broadcast_to(
                    jnp.exp(mid), (8, chans))

    def g_of(self, d, block):
        return self.g_s[d, pl.ds(pl.multiple_of(block * 8, 8), 8), :][:1]

    def keys(self, start):
        chans, tile = self.chans, self.half
        at = at_row(start, tile)
        first = start // SPAN
        pk = mm(self.tok[at, :], self.wk[...]).astype(BF)
        self.pk_s[at, :] = pk
        pk = pk.astype(F32)
        inv = lax.rsqrt(head_sum(pk * pk, head_ones(chans)) + 1.0)
        self.inv_s[at, :] = inv
        normed = pk * inv
        rates = jax.nn.sigmoid(self.rate[...])
        units = []
        for s in range(tile // SPAN):
            cut = slice(s * SPAN, (s + 1) * SPAN)
            here = self.unit(first + s)
            for d in range(2):
                g = self.g_of(d, first + s)
                e = -normed[cut] * self.past_s[d, here, :]
                w = normed[cut] * rates[d : d + 1, :] * self.shrink_s[d, here, :]
                self.wp_s[d, here, :] = w.astype(BF)
                self.kend_s[d, here, :] = (w * g).astype(BF)
                units.append((d, first + s, e.astype(BF), (e * g).astype(BF)))
        return units

    def strict(self, d):
        ti = iota((SPAN, self.chans), 0)
        ji = iota((SPAN, self.chans), 1) % HEAD
        return (ti > ji) if d == 0 else (ti < ji)

    def invert(self, units):
        chans = self.chans
        mask = head_ones(WIDE)
        ti = iota((SPAN, chans), 0)
        ji = iota((SPAN, chans), 1) % HEAD
        eye = (ti == ji).astype(F32)
        full = [
            jnp.where(self.strict(d), by_head(e, self.wp_s[d, self.unit(block), :], mask, NT), 0.0)
            for d, block, e, _ in units
        ]
        near = ti // 4 == ji // 4
        base = [jnp.where(near, a, 0.0) for a in full]
        square = [by_head(a, a, mask) for a in base]
        inverse = [eye + a for a in base]
        inverse = [t + by_head(t, a2, mask) for t, a2 in zip(inverse, square)]
        size = 4
        while size < SPAN:
            far = jnp.logical_and(ti // (2 * size) == ji // (2 * size), ti // size != ji // size)
            first = [by_head(t, jnp.where(far, a, 0.0), mask) for t, a in zip(inverse, full)]
            inverse = [t + by_head(f, t, mask) for t, f in zip(inverse, first)]
            size *= 2
        tegs = []
        for (d, block, _, eg), t in zip(units, inverse):
            t = (t - eye).astype(BF)
            self.t_s[d, self.unit(block), :] = t
            tegs.append((eg.astype(F32) + by_head(t, eg, mask)).astype(BF))
        ones = head_ones(chans)
        for (d, block, _, _), teg in zip(units, tegs):
            self.teg_s[d, self.unit(block), :] = teg
            self.step_s[d, at_row(block * chans, chans), :] = (
                dot(teg, self.kend_s[d, self.unit(block), :], TN).astype(BF) * ones)

    def values(self):
        chans = self.chans
        small = head_ones(WIDE)
        mask = head_ones(chans).astype(F32)
        pv = mm(self.tok[...], self.wv[...]).astype(BF)
        self.pv_s[...] = pv
        cv = pv.astype(F32) / self.inv_s[...]
        each = 4
        for group in range(0, self.blocks, each):
            work = []
            for block in range(group, min(group + each, self.blocks)):
                cut = slice(block * SPAN, (block + 1) * SPAN)
                for d in range(2):
                    tcv = cv[cut] + by_head(self.t_s[d, cut, :], cv[cut], small)
                    self.tcv_s[d, cut, :] = tcv
                    work.append((d, cut, tcv.astype(BF)))
            puts = [dot(tcv, self.kend_s[d, cut, :], TN) for d, cut, tcv in work]
            for (d, cut, _), put in zip(work, puts):
                put = put * mask
                self.put_s[d, cut, :] = sum(put[h * HEAD : (h + 1) * HEAD] for h in range(self.heads))

    def scan(self):
        states = [jnp.zeros((HEAD, self.chans), F32) for _ in range(2)]
        for step in range(self.blocks):
            for d in range(2):
                block = step if d == 0 else self.blocks - 1 - step
                cut = slice(block * SPAN, (block + 1) * SPAN)
                state = states[d]
                low = state.astype(BF)
                self.state_s[d, cut, :] = low
                if step < self.blocks - 1:
                    g = self.g_s[d, block * 8 : block * 8 + 1, :]
                    step_w = self.step_s[d, block * self.chans : (block + 1) * self.chans, :]
                    states[d] = state * (g * g) + mm(low, step_w) + self.put_s[d, cut, :]

    def outputs(self, start, tile, p):
        mask = head_ones(WIDE)
        at = at_row(start, tile)
        cols = slice(p * WIDE, (p + 1) * WIDE)
        first = start // SPAN
        pr = mm(self.tok[at, :], self.wr[:, cols]).astype(BF).astype(F32)
        pp = pr * self.pk_s[at, cols].astype(F32)
        rates = jax.nn.sigmoid(self.rate[:, cols])
        both = jnp.sum(rates * self.diag[:, cols], axis=0, keepdims=True)
        inv = self.inv_s[at, cols]
        total = head_sum(pp * both, mask) * self.pv_s[at, cols].astype(F32)
        diags = [head_sum(pp * rates[d : d + 1, :], mask) * inv for d in range(2)]
        ti = iota((SPAN, WIDE), 0)
        ji = iota((SPAN, WIDE), 1) % HEAD
        units = [(d, s) for s in range(tile // SPAN) for d in range(2)]
        bs, reads = [], []
        for d, s in units:
            here = self.unit(first + s)
            q = pr[s * SPAN : (s + 1) * SPAN] * self.grow_s[d, here, cols]
            bs.append(by_head(q, self.wp_s[d, here, cols], mask, NT))
            g = self.g_s[d, pl.ds(pl.multiple_of((first + s) * 8, 8), 8), cols][:1]
            lhs = jnp.concatenate([self.teg_s[d, here, cols], (q * g).astype(BF)], axis=0)
            reads.append(by_head(lhs, self.state_s[d, here, cols], mask, NT))
        ys = [[], []]
        for (d, s), b, read in zip(units, bs, reads):
            exact = self.tcv_s[d, self.unit(first + s), cols] + read[:SPAN]
            b = jnp.where((ti > ji) if d == 0 else (ti < ji), b, 0.0)
            ys[d].append(
                read[SPAN:] + by_head(b, exact, mask) + diags[d][s * SPAN : (s + 1) * SPAN] * exact)
        ys = [jnp.concatenate(y, axis=0) for y in ys]
        means = [head_sum(y, mask) * (1.0 / HEAD) for y in ys]
        centred = [y - mean for y, mean in zip(ys, means)]
        variances = [head_sum(c * c, mask) * (1.0 / HEAD) for c in centred]
        for c, variance in zip(centred, variances):
            total = total + c * lax.rsqrt(variance + 0.00064) * self.gain[:, cols]
        self.out[at, cols] = total.astype(BF)


def core_scratch(length, chans):
    vm = pltpu.VMEM
    both = lambda n, dt: vm((2, n, chans), dt)
    blocks = length // SPAN
    return [
        vm((length, chans), BF), vm((length, chans), BF), vm((length, chans), F32),
        both(length, F32), both(length, F32), both(length, F32), both(blocks * 8, F32),
        both(length, BF), both(length, BF),
        both(length, BF), both(length, BF), both(blocks * chans, BF), both(length, F32),
        both(length, F32), both(length, BF),
    ]


def core_kernel(
    tok_ref, w_ref, up_ref, floor_ref, rate_ref, diag_ref, gain_ref, out_ref,
    eq_s, wp_s, qe_s, kend_s, cv_s, own_s, decay_s, diag_s, t_s, b_s, state_s, y_s,
    arrivals=(),
):
    length, chans = out_ref.shape
    heads = chans // HEAD
    rank = up_ref.shape[1]
    rows = min(256, length)
    blocks = length // SPAN

    def head_ones():
        return (iota((chans, chans), 0) // HEAD == iota((chans, chans), 1) // HEAD).astype(BF)

    def head_sum(x, ones):
        hi, lo = split(x)
        return mm(hi, ones) + mm(lo, ones)

    def at_block(block):
        return pl.ds(pl.multiple_of(block * SPAN, SPAN), SPAN)

    def project(ready):
        tile = SPAN * len(ready)

        def put(ref, x, *lead):
            for s, block in enumerate(ready):
                ref[(*lead, at_block(block), slice(None))] = x[s * SPAN : (s + 1) * SPAN]

        source = jnp.concatenate([tok_ref[at_block(block), :] for block in ready], axis=0)
        pr = mm(source, w_ref[:, :chans]).astype(BF).astype(F32)
        pk = mm(source, w_ref[:, chans : 2 * chans]).astype(BF).astype(F32)
        pv = mm(source, w_ref[:, 2 * chans : 3 * chans]).astype(BF).astype(F32)
        lowered = jnp.tanh(mm(source, w_ref[:, 3 * chans :])).astype(BF)
        ones = head_ones()
        norm2 = head_sum(pk * pk, ones) + 1.0
        inv = lax.rsqrt(norm2)
        scale = norm2 * inv
        normed = pk * inv
        put(cv_s, scale * pv)
        rates = jax.nn.sigmoid(rate_ref[...])
        both = jnp.sum(rates * diag_ref[...], axis=0, keepdims=True)
        put(own_s, head_sum(pr * pk * both, ones) * pv)
        ri = iota((tile, tile), 0)
        ci = iota((tile, tile), 1)
        same = ri // SPAN == ci // SPAN
        whole = same.astype(BF)
        for d in range(2):
            pre = (
                mm(lowered[:, d * rank : (d + 1) * rank], up_ref[d]) + floor_ref[d : d + 1, :]
            ).astype(BF).astype(F32)
            fall = -math.exp(-0.5) * jax.nn.sigmoid(pre)
            tri = jnp.logical_and(same, (ci <= ri) if d == 0 else (ci >= ri)).astype(BF)
            hi, lo = split(fall)
            inclusive = mm(tri, hi) + mm(tri, lo)
            final = mm(whole, hi) + mm(whole, lo)
            half = 0.5 * final
            grow = jnp.exp(inclusive - half)
            shrink = jnp.exp(half - inclusive)
            g = jnp.exp(half)
            e = -normed * (grow * jnp.exp(-fall))
            q = pr * grow
            w = normed * rates[d : d + 1, :] * shrink
            put(wp_s, w.astype(BF), d)
            put(kend_s, (w * g).astype(BF), d)
            eb, qb = e.astype(BF), q.astype(BF)
            eg, qg = (e * g).astype(BF), (q * g).astype(BF)
            g2 = g * g
            put(diag_s, head_sum(pr * normed * rates[d : d + 1, :], ones), d)
            for s, block in enumerate(ready):
                cut = slice(s * SPAN, (s + 1) * SPAN)
                base = pl.multiple_of(block * 2 * SPAN, 2 * SPAN)
                eq_s[d, pl.ds(base, SPAN), :] = eb[cut]
                eq_s[d, pl.ds(base + SPAN, SPAN), :] = qb[cut]
                qe_s[d, pl.ds(base, SPAN), :] = eg[cut]
                qe_s[d, pl.ds(base + SPAN, SPAN), :] = qg[cut]
                decay_s[d, pl.ds(pl.multiple_of(block * 8, 8), 8), :] = g2[
                    s * SPAN : s * SPAN + 8
                ]

    def spread(x, mask):
        x = x.astype(BF)
        if heads > 1:
            x = jnp.concatenate([x] * heads, axis=0)
        return x * mask

    def invert(ready):
        mask = head_ones()
        ti = iota((SPAN, chans), 0)
        ji = iota((SPAN, chans), 1) % HEAD
        eye = (ti == ji).astype(F32)
        work = []
        for block in ready:
            for d in range(2):
                two = pl.ds(pl.multiple_of(block * 2 * SPAN, 2 * SPAN), 2 * SPAN)
                at = pl.ds(pl.multiple_of(block * SPAN, SPAN), SPAN)
                ab = lax.dot_general(
                    eq_s[d, two, :], spread(wp_s[d, at, :], mask), NT, preferred_element_type=F32
                )
                strict = (ti > ji) if d == 0 else (ti < ji)
                b_s[d, at, :] = jnp.where(strict, ab[SPAN:], 0.0).astype(BF)
                work.append((d, at, jnp.where(strict, ab[:SPAN], 0.0)))
        near = ti // 4 == ji // 4
        full = [a for _, _, a in work]
        base = [jnp.where(near, a, 0.0) for a in full]
        square = [mm(a.astype(BF), spread(a, mask)) for a in base]
        inverse = [eye + a for a in base]
        inverse = [t + mm(t.astype(BF), spread(a2, mask)) for t, a2 in zip(inverse, square)]
        size = 4
        while size < SPAN:
            far = jnp.logical_and(ti // (2 * size) == ji // (2 * size), ti // size != ji // size)
            first = [
                mm(t.astype(BF), spread(jnp.where(far, a, 0.0), mask))
                for t, a in zip(inverse, full)
            ]
            inverse = [t + mm(f.astype(BF), spread(t, mask)) for t, f in zip(inverse, first)]
            size *= 2
        for (d, at, _), t in zip(work, inverse):
            t_s[d, at, :] = (t - eye).astype(BF)

    for settle, ready in arrivals:
        settle()
        project(ready)
        invert(ready)

    state_s[...] = jnp.zeros_like(state_s)

    @pl.loop(0, blocks)
    def _(step):
        mask = head_ones()
        for d in range(2):
            block = step if d == 0 else blocks - 1 - step
            two = pl.ds(pl.multiple_of(block * 2 * SPAN, 2 * SPAN), 2 * SPAN)
            at = pl.ds(pl.multiple_of(block * SPAN, SPAN), SPAN)
            state = state_s[d]
            read = lax.dot_general(
                qe_s[d, two, :], state.astype(BF), NT, preferred_element_type=F32
            )
            x = cv_s[at, :] + read[:SPAN]
            exact = x + mm(t_s[d, at, :], spread(x, mask))
            a = exact.astype(BF)
            y_s[d, at, :] = read[SPAN:] + mm(b_s[d, at, :], spread(a, mask)) + diag_s[d, at, :] * exact
            decay = decay_s[d, pl.ds(pl.multiple_of(block * 8, 8), 8), :][:1]
            put = lax.dot_general(a, kend_s[d, at, :], TN, preferred_element_type=F32)
            state_s[d] = state * decay + put * mask.astype(F32)

    @pl.loop(0, length // rows)
    def _(step):
        at = pl.ds(pl.multiple_of(step * rows, rows), rows)
        ones = head_ones()
        total = own_s[at, :]
        for d in range(2):
            y = y_s[d, at, :]
            centred = y - head_sum(y, ones) * (1.0 / HEAD)
            variance = head_sum(centred * centred, ones) * (1.0 / HEAD)
            total = total + centred * lax.rsqrt(variance + 0.00064) * gain_ref[...]
        out_ref[at, :] = total.astype(BF)


MESH = pl.DeviceIdType.MESH


def whole_kernel(
    sp, dp, tok_ref, w_ref, up_ref, floor_ref, rate_ref, diag_ref, gain_ref, out_ref,
    tok_all, w_all, out_all, slots,
    ring_out, ring_in, far_out, far_in, pass_out, pass_in, back_out, back_in, *scratch,
):
    rows = tok_ref.shape[0]
    half_rows = rows // 2
    depth = w_ref.shape[0]
    chans = out_all.shape[1]
    chips = dp // 2
    z = lax.axis_index("sp")
    me = lax.axis_index("dp")
    chip = me // 2
    core = me % 2
    partner = chip * 2 + 1 - core

    def peer(k):
        return lax.rem(chip + k, chips) * 2 + core

    def z_peer(k):
        return lax.rem(z + k, sp)

    barrier = pltpu.get_barrier_semaphore()
    for target in [(z, partner)] + [(z, peer(k)) for k in range(1, chips)] + [
        (z_peer(k), me) for k in range(1, sp)
    ]:
        pl.semaphore_signal(barrier, inc=1, device_id=target, device_id_type=MESH)
    pl.semaphore_wait(barrier, chips + sp - 1)

    def remote(src, dst, out_sem, in_sem, target):
        copy = pltpu.make_async_remote_copy(
            src_ref=src, dst_ref=dst, send_sem=out_sem, recv_sem=in_sem,
            device_id=target, device_id_type=MESH,
        )
        copy.start()
        return copy

    def w_at(device):
        return pl.ds(pl.multiple_of(device * depth, depth), depth)

    def ring_step(s):
        copies = []
        for way in range(2):
            owner = z_peer(sp - s) if way == 0 else z_peer(s)
            at = pl.ds(
                pl.multiple_of(owner * rows + way * half_rows, half_rows), half_rows
            )
            first = tok_ref.at[pl.ds(way * half_rows, half_rows), :]
            copies.append(
                remote(
                    first if s == 0 else tok_all.at[at, :], tok_all.at[at, :],
                    ring_out.at[way, s], ring_in.at[way, s],
                    (z_peer(1) if way == 0 else z_peer(sp - 1), me),
                )
            )
        return copies

    ring = [ring_step(0)] if sp > 1 else []
    far = [
        remote(w_ref, w_all.at[w_at(me), :], far_out.at[k], far_in.at[k], (z, peer(k)))
        for k in range(1, chips)
    ]
    passed = [remote(w_ref, w_all.at[w_at(me), :], pass_out.at[0], pass_in.at[0], (z, partner))]
    w_all[w_at(me), :] = w_ref[...]
    tok_all[pl.ds(pl.multiple_of(z * rows, rows), rows), :] = tok_ref[...]
    for s in range(max(sp, chips) - 1):
        if s < sp - 2:
            for copy in ring[s]:
                copy.wait_recv()
            ring.append(ring_step(s + 1))
        if s < chips - 1:
            far[s].wait_recv()
            block = w_at(peer(chips - 1 - s))
            passed.append(
                remote(
                    w_all.at[block, :], w_all.at[block, :],
                    pass_out.at[s + 1], pass_in.at[s + 1], (z, partner),
                )
            )
    for copy in passed:
        copy.wait_recv()

    def last_ring():
        for copy in ring[-1]:
            copy.wait_recv()

    per = rows // SPAN
    arrivals = [(lambda: None, [z * per + b for b in range(per)])]
    for s in range(sp - 1):
        before, after = z_peer(sp - 1 - s), z_peer(s + 1)
        ready = [before * per + b for b in range(per // 2)]
        ready += [after * per + b for b in range(per // 2, per)]
        arrivals.append((last_ring if s == sp - 2 else lambda: None, ready))

    core_kernel(
        tok_all, w_all, up_ref, floor_ref, rate_ref, diag_ref, gain_ref, out_all, *scratch,
        arrivals=arrivals,
    )
    for copy in far + passed + [c for pair in ring for c in pair]:
        copy.wait_send()

    def out_at(owner):
        return pl.ds(pl.multiple_of(owner * rows, rows), rows)

    back = [
        remote(
            out_all.at[out_at(z_peer(k)), :], slots.at[z], back_out.at[k], back_in.at[k],
            (z_peer(k), me),
        )
        for k in range(1, sp)
    ]
    slots[z] = out_all[out_at(z), :]
    for copy in back:
        copy.wait()
    for s in range(sp):
        out_ref[:, s * chans : (s + 1) * chans] = slots[s]


def whole_call(sp, dp, rows, depth, chans, width):
    vm = pltpu.VMEM
    dma = pltpu.SemaphoreType.DMA
    length = rows * sp
    both = lambda n, dt: vm((2, n, chans), dt)
    return pl.pallas_call(
        functools.partial(whole_kernel, sp, dp),
        out_shape=jax.ShapeDtypeStruct((rows, chans * sp), BF),
        in_specs=[pl.BlockSpec(memory_space=vm)] * 7,
        out_specs=pl.BlockSpec(memory_space=vm),
        scratch_shapes=[
            vm((length, depth), BF), vm((depth, width), BF), vm((length, chans), BF),
            vm((sp, rows, chans), BF),
            dma((2, sp)), dma((2, sp)), dma((dp,)), dma((dp,)), dma((dp,)), dma((dp,)),
            dma((sp,)), dma((sp,)),
            both(2 * length, BF), both(length, BF), both(2 * length, BF), both(length, BF),
            vm((length, chans), F32), vm((length, chans), F32),
            both(length // SPAN * 8, F32), both(length, F32), both(length, BF), both(length, BF),
            vm((2, chans, chans), F32), both(length, F32),
        ],
        compiler_params=pltpu.CompilerParams(
            vmem_limit_bytes=58 * 1024 * 1024, collective_id=0, has_side_effects=True
        ),
        name="whole",
    )


def halves_kernel(
    sp, side, other, tok_ref, wr_ref, wk_ref, wv_ref, wd_ref, up_ref, floor_ref, rate_ref, diag_ref, gain_ref,
    out_ref, tok_all, wk_all, wv_all, wr_all, wd_all, up_s, floor_s, rate_s, diag_s, gain_s, out_all,
    w_in, w_out, relay_out, d_in, d_pass, t_in, t_pass, t_out, t_fwd, p_in, p_out, o_in, o_out, here, *scratch,
):
    rows = tok_ref.shape[0]
    depth = wk_ref.shape[0]
    chans = wk_all.shape[1]
    half = sp // 2
    part = rows // 4
    z = lax.axis_index("sp")
    me = lax.axis_index("dp")
    core = me % 2
    chip = me // 2
    cy, cx = chip // side, chip % side
    h = z // half
    j = z % half
    u = jnp.where(h == 1, j, half - 1 - j)
    slot = u * 2 + core
    partner = chip * 2 + 1 - core

    def layer(hh, uu):
        return half - 1 - uu + hh * (2 * uu + 1)

    def x_peer(k):
        return cy * side + lax.rem(cx + k, side)

    def y_peer(k):
        return lax.rem(cy + k, other) * side + cx

    x_peers = [x_peer(k) for k in range(1, side)]
    y_peers = [y_peer(k) for k in range(1, other)]

    def local(src, dst, n):
        copy = pltpu.make_async_copy(src, dst, here.at[n])
        copy.start()
        return copy

    def cols(who):
        return pl.ds(pl.multiple_of(who * chans, chans), chans)

    mine = at_row(me * depth, depth)
    own = [
        local(wd_ref, wd_all.at[mine, :], 0),
        local(wk_ref.at[:, cols(slot)], wk_all.at[mine, :], 1),
        local(up_ref.at[:, :, cols(slot)], up_s, 2),
        local(floor_ref.at[:, cols(slot)], floor_s, 3),
        local(wv_ref.at[:, cols(slot)], wv_all.at[mine, :], 4),
        local(wr_ref.at[:, cols(slot)], wr_all.at[mine, :], 5),
    ]

    @pl.when(core == h)
    def _():
        local(tok_ref, tok_all.at[at_row(z * rows, rows), :], 6)

    barrier = pltpu.get_barrier_semaphore()
    greet = [(z, p * 2 + k) for p in x_peers + y_peers for k in range(2)]
    greet += [(lax.rem(z + n, sp), chip * 2 + k) for n in range(1, sp) for k in range(2)]
    greet.append((z, partner))
    for target in greet:
        pl.semaphore_signal(barrier, inc=1, device_id=target, device_id_type=MESH)
    pl.semaphore_wait(barrier, len(greet))

    def remote(src, dst, out_sem, in_sem, target):
        return pltpu.make_async_remote_copy(
            src_ref=src, dst_ref=dst, send_sem=out_sem, recv_sem=in_sem,
            device_id=target, device_id_type=MESH,
        )

    def go(copy):
        copy.start()
        return copy

    sent = []
    wide = chans // WIDE
    pieces = [(wk_ref, wk_all, 0, chans), (wv_ref, wv_all, 0, chans)]
    pieces += [(wr_ref, wr_all, p * WIDE, WIDE) for p in range(wide)]
    decay = len(pieces)

    def take(n, who):
        src, _, low, size = pieces[n]
        return src.at[:, pl.ds(pl.multiple_of(who * chans + low, WIDE), size)]

    def landing(n, block):
        _, dst, low, size = pieces[n]
        return dst.at[block, low : low + size]

    def direct(n):
        for i, p in enumerate(x_peers + y_peers):
            for k in range(2):
                sent.append(go(remote(
                    take(n, u * 2 + k), landing(n, mine),
                    w_out.at[n, i * 2 + k], w_in.at[n, me], (z, p * 2 + k),
                )))
        last = 2 * len(x_peers + y_peers)
        sent.append(go(remote(
            take(n, u * 2 + 1 - core), landing(n, mine),
            w_out.at[n, last], w_in.at[n, me], (z, partner),
        )))

    def wait_for(sem, dst):
        remote(dst, dst, sem, sem, (z, partner)).wait_recv()

    def arrived(sem, dst, block):
        wait_for(sem, dst.at[block, :])

    def w_rows(p, c):
        return at_row((p * 2 + c) * depth, depth)

    def relay(n):
        count = 0
        for c, froms, tos in ((0, x_peers, y_peers), (1, y_peers, x_peers)):
            for p in froms:
                block = w_rows(p, c)
                wait_for(w_in.at[n, p * 2 + c], landing(n, block))
                for q in tos:
                    sent.append(go(remote(
                        landing(n, block), landing(n, block),
                        relay_out.at[n, count], w_in.at[n, p * 2 + c], (z, q * 2 + core),
                    )))
                    count += 1

    def finish(n):
        for c, others in ((1, x_peers), (0, y_peers)):
            for p in others:
                wait_for(w_in.at[n, p * 2 + c], landing(n, w_rows(p, c)))
        for ky in range(1, other):
            for kx in range(1, side):
                p = lax.rem(cy + ky, other) * side + lax.rem(cx + kx, side)
                for c in range(2):
                    wait_for(w_in.at[n, p * 2 + c], landing(n, w_rows(p, c)))
        wait_for(w_in.at[n, partner], landing(n, w_rows(chip, 1 - core)))

    def decay_direct():
        for i, p in enumerate(x_peers + y_peers):
            sent.append(go(remote(
                wd_ref, wd_all.at[mine, :], w_out.at[decay, i], d_in.at[me], (z, p * 2 + core))))
        sent.append(go(remote(
            wd_ref, wd_all.at[mine, :], w_out.at[decay, len(x_peers + y_peers)], d_in.at[me], (z, partner))))

    def decay_pass(p, n):
        block = w_rows(p, core)
        sent.append(go(remote(
            wd_all.at[block, :], wd_all.at[block, :], d_pass.at[n], d_in.at[p * 2 + core], (z, partner))))

    late = []

    def decay_relay():
        for c, froms, tos in ((0, x_peers, y_peers), (1, y_peers, x_peers)):
            @pl.when(core == c)
            def _():
                count = 0
                for p in froms:
                    block = w_rows(p, c)
                    arrived(d_in.at[p * 2 + c], wd_all, block)
                    for q in tos:
                        go(remote(
                            wd_all.at[block, :], wd_all.at[block, :],
                            relay_out.at[decay, count], d_in.at[p * 2 + c], (z, q * 2 + c)))
                        count += 1
                for p in tos:
                    arrived(d_in.at[p * 2 + c], wd_all, w_rows(p, c))

            def close(c=c, froms=froms, tos=tos):
                @pl.when(core == c)
                def _():
                    count = 0
                    for p in froms:
                        block = w_rows(p, c)
                        for q in tos:
                            remote(
                                wd_all.at[block, :], wd_all.at[block, :],
                                relay_out.at[decay, count], d_in.at[p * 2 + c], (z, q * 2 + c)).wait_send()
                            count += 1

            late.append(close)
        for n, p in enumerate(x_peers + y_peers):
            decay_pass(p, n)

    def decay_finish():
        n = len(x_peers + y_peers)
        corners = [
            lax.rem(cy + ky, other) * side + lax.rem(cx + kx, side)
            for ky in range(1, other) for kx in range(1, side)
        ]
        for p in corners:
            arrived(d_in.at[p * 2 + core], wd_all, w_rows(p, core))
            decay_pass(p, n)
            n += 1
        arrived(d_in.at[partner], wd_all, w_rows(chip, 1 - core))
        for p in x_peers + y_peers + corners:
            arrived(d_in.at[p * 2 + 1 - core], wd_all, w_rows(p, 1 - core))

    def t_rows(s, i):
        return at_row(s * rows + i * part, part)

    def block_sends(act):
        def all_parts(target_layer, first):
            for i in range(4):
                act(remote(
                    tok_ref.at[pl.ds(i * part, part), :], tok_all.at[t_rows(z, i), :],
                    t_out.at[first + i], t_in.at[z, i // 2], (target_layer, chip * 2 + i % 2)))

        @pl.when(core != h)
        def _():
            all_parts(layer(core, 0), 0)

        @pl.when(jnp.logical_and(core == h, u + 1 < half))
        def _():
            all_parts(layer(h, u + 1), 0)

        @pl.when(jnp.logical_and(core == h, u > 0))
        def _():
            all_parts(layer(h, u - 1), 4)

        @pl.when(core == h)
        def _():
            act(remote(
                tok_ref, tok_all.at[at_row(z * rows, rows), :], t_out.at[8], t_pass.at[z, 0], (z, partner)))

    def forward(s, outward, inward, n, q, act):
        block = t_rows(s, 2 * q + core)
        for cond, step in ((outward, 1), (inward, -1)):
            if cond is not None:
                @pl.when(cond)
                def _():
                    act(remote(
                        tok_all.at[block, :], tok_all.at[block, :], t_fwd.at[0, n, q], t_in.at[s, q],
                        (layer(h, u + step), me)))
        act(remote(
            tok_all.at[block, :], tok_all.at[block, :], t_fwd.at[1, n, q], t_pass.at[s, q], (z, partner)))

    near = [lax.rem(u + k, half) for k in range(1, half)]
    sources = [
        (layer(h, v), jnp.logical_and(u > v, u + 1 < half), jnp.logical_and(u < v, u > 0)) for v in near
    ]
    sources += [(layer(1 - h, v), u + 1 < half, None) for v in range(half)]

    def take_tokens(n, q):
        s, outward, inward = sources[n]
        arrived(t_in.at[s, q], tok_all, t_rows(s, 2 * q + core))
        forward(s, outward, inward, n, q, go)

    def take_far(now, q):
        @pl.when(now)
        def _():
            for n in range(half - 1, len(sources)):
                take_tokens(n, q)

    def own_tokens():
        block = at_row(z * rows, rows)

        @pl.when(core == h)
        def _():
            pltpu.make_async_copy(tok_ref, tok_all.at[block, :], here.at[6]).wait()

        @pl.when(core != h)
        def _():
            arrived(t_pass.at[z, 0], tok_all, block)

    def passed_tokens(n):
        s = sources[n][0]
        for q in range(2):
            arrived(t_pass.at[s, q], tok_all, t_rows(s, 2 * q + 1 - core))

    goal = (layer(core, z // 2), chip * 2 + z % 2)
    stay = jnp.logical_and(goal[0] == z, z % 2 == core)
    smalls = [(rate_ref, rate_s), (diag_ref, diag_s), (gain_ref, gain_s)]

    @pl.when(jnp.logical_not(stay))
    def _():
        for n, (src, dst) in enumerate(smalls):
            go(remote(src, dst, p_out.at[n], p_in.at[n], goal))

    @pl.when(stay)
    def _():
        for n, (src, dst) in enumerate(smalls):
            pltpu.make_async_copy(src, dst, p_in.at[n]).start()

    decay_direct()
    block_sends(go)
    direct(0)
    decay_relay()
    take_far(u + 1 < half, 0)
    relay(0)
    direct(1)
    direct(2)
    for n in range(half - 1):
        for q in range(2):
            take_tokens(n, q)
    take_far(u + 1 < half, 1)
    decay_finish()
    for n in (0, 2, 3):
        own[n].wait()
    own_tokens()
    for n in range(half - 1):
        passed_tokens(n)
    work = Core(
        tok_all, wk_all, wd_all, wv_all, wr_all, up_s, floor_s, rate_s, diag_s, gain_s, out_all, scratch)
    near_rows = h * half * rows
    far_rows = (1 - h) * half * rows
    work.decays(near_rows)
    take_far(u + 1 == half, 0)
    finish(0)
    own[1].wait()

    @pl.when(jnp.logical_not(stay))
    def _():
        for n, (src, dst) in enumerate(smalls):
            remote(src, dst, p_out.at[n], p_in.at[n], goal).wait_send()
    for n, (src, dst) in enumerate(smalls):
        remote(dst, dst, p_in.at[n], p_in.at[n], (z, partner)).wait_recv()

    units = work.keys(near_rows)
    work.invert(units)
    take_far(u + 1 == half, 1)
    for n in range(half - 1, len(sources)):
        passed_tokens(n)
    work.decays(far_rows)
    units = work.keys(far_rows)
    relay(1)
    for p in range(1, wide):
        direct(2 + p)
    work.invert(units)
    relay(2)
    finish(1)
    own[4].wait()
    work.values()
    work.scan()

    def give(s, p, n, act):
        block = at_row(s * rows, rows)
        low = p * WIDE
        act(remote(
            out_all.at[block, low : low + WIDE],
            out_ref.at[:, pl.ds(pl.multiple_of(slot * chans + low, WIDE), WIDE)],
            o_out.at[p, n], o_in.at[p, slot], (s, chip * 2 + h)))

    def give_far(p, act):
        for v in range(half):
            give(layer(1 - h, v), p, v, act)

    def give_near(p, act):
        for n in range(half - 1):
            give(sources[n][0], p, half + n, act)

        @pl.when(core != h)
        def _():
            give(z, p, sp - 1, act)

    own[5].wait()
    for p in range(wide):
        if p + 1 < wide:
            relay(3 + p)
        finish(2 + p)
        work.outputs(far_rows, half * rows, p)
        give_far(p, go)
        work.outputs(near_rows, half * rows, p)
        give_near(p, go)

    @pl.when(core == h)
    def _():
        out_ref[:, cols(slot)] = out_all[at_row(z * rows, rows), :]

    def stop(copy):
        copy.wait_send()

    block_sends(stop)
    for n, (s, outward, inward) in enumerate(sources):
        for q in range(2):
            forward(s, outward, inward, n, q, stop)
    for copy in sent:
        copy.wait_send()
    for close in late:
        close()
    for p in range(wide):
        give_far(p, stop)
        give_near(p, stop)
        for g in range(sp):
            low = g * chans + p * WIDE

            @pl.when(jnp.logical_not(jnp.logical_and(core == h, slot == g)))
            def _():
                wait_for(o_in.at[p, g], out_ref.at[:, low : low + WIDE])


def halves_call(sp, dp, side, rows, width, depth, chans, rank):
    vm = pltpu.VMEM
    dma = pltpu.SemaphoreType.DMA
    chips = dp // 2
    other = chips // side
    peers = side + other - 2
    corners = (side - 1) * (other - 1)
    length = rows * sp
    wide = chans // WIDE
    return pl.pallas_call(
        functools.partial(halves_kernel, sp, side, other),
        out_shape=jax.ShapeDtypeStruct((rows, chans * sp), BF),
        in_specs=[pl.BlockSpec(memory_space=pl.ANY)] * 10,
        out_specs=pl.BlockSpec(memory_space=vm),
        scratch_shapes=[
            vm((length, width), BF), vm((width, chans), BF), vm((width, chans), BF), vm((width, chans), BF),
            vm((width, 2 * rank), BF), vm((2, rank, chans), BF), vm((2, chans), F32), vm((2, chans), F32),
            vm((2, chans), F32), vm((1, chans), F32), vm((length, chans), BF),
            dma((2 + wide, dp)), dma((3 + wide, 2 * peers + 1)), dma((3 + wide, 2 * corners)), dma((dp,)), dma((peers + corners,)),
            dma((sp, 2)), dma((sp, 2)), dma((9,)), dma((2, sp, 2)), dma((3,)), dma((3,)), dma((wide, sp)), dma((wide, sp)),
            dma((7,)),
        ] + core_scratch(length, chans),
        compiler_params=pltpu.CompilerParams(
            vmem_limit_bytes=58 * 1024 * 1024, collective_id=0, has_side_effects=True
        ),
        name="halves",
    )


def per_device(
    sp, dp,
    tokens, receptance_weight, key_projection_weight, value_projection_weight,
    decay_down_weight, decay_up_weight, decay_floor_level, correction_rate_logit,
    diagonal_address_factor, head_norm_gain,
):
    rows, width = tokens.shape[1:]
    depth, channels = receptance_weight.shape
    chans = channels // sp
    side = math.isqrt(dp // 2)
    gain = head_norm_gain[None, :]
    if chans % 128 == 0 and sp % 2 == 0 and dp == 2 * side * side and rows % SPAN == 0:
        mixed = halves_call(sp, dp, side, rows, width, depth, chans, decay_up_weight.shape[1])(
            tokens[0], receptance_weight, key_projection_weight, value_projection_weight, decay_down_weight,
            decay_up_weight, decay_floor_level, correction_rate_logit, diagonal_address_factor, gain)
        return mixed[None]
    start = lax.axis_index("sp") * chans

    def mine(x):
        return lax.dynamic_slice_in_dim(x, start, chans, axis=x.ndim - 1)

    packed = jnp.concatenate(
        [mine(receptance_weight), mine(key_projection_weight), mine(value_projection_weight),
         decay_down_weight], axis=1)
    mixed = whole_call(sp, dp, rows, width, chans, packed.shape[1])(
        tokens[0], packed, mine(decay_up_weight), mine(decay_floor_level),
        correction_rate_logit, diagonal_address_factor, gain)
    return mixed[None]


def solution(mesh):
    in_specs = (
        P("dp", "sp", None), P("dp", None), P("dp", None), P("dp", None), P("dp", None),
        P(), P(), P(None, "sp"), P(None, "sp"), P("sp"),
    )
    return jax.shard_map(
        functools.partial(per_device, mesh.shape["sp"], mesh.shape["dp"]), mesh=mesh, in_specs=in_specs,
        out_specs=P("dp", "sp", None), check_vma=False,
    )
```

```python
import functools, math
import jax, jax.numpy as jnp
from jax import lax
from jax.experimental import pallas as pl
from jax.experimental.pallas import tpu as pltpu
from jax.sharding import PartitionSpec as P
HEAD = 64
SPAN = 64
BF = jnp.bfloat16
F32 = jnp.float32
NT = (((1,), (1,)), ((), ()))
TN = (((0,), (0,)), ((), ()))


def mm(a, b):
    return jnp.dot(a, b, preferred_element_type=F32)


def dot(a, b, dims):
    return lax.dot_general(a, b, dims, preferred_element_type=F32)


def split(x):
    hi = x.astype(BF)
    return hi, (x - hi.astype(F32)).astype(BF)


def iota(shape, axis):
    return lax.broadcasted_iota(jnp.int32, shape, axis)


def head_ones(chans):
    return (iota((chans, chans), 0) // HEAD == iota((chans, chans), 1) // HEAD).astype(BF)


def head_sum(x, ones):
    hi, lo = split(x)
    if ones.shape[0] > WIDE:
        return mm(hi, ones) + mm(lo, ones)
    return mm(jnp.concatenate([hi, lo], axis=1), jnp.concatenate([ones, ones], axis=0))


def spread(x, mask):
    x = x.astype(BF)
    heads = mask.shape[0] // HEAD
    if heads > 1:
        x = jnp.concatenate([x] * heads, axis=0)
    return x * mask


WIDE = 128


def lanes(x, p):
    return x[:, p * WIDE : (p + 1) * WIDE]


def by_head(x, y, mask, dims=None):
    parts = []
    for p in range(x.shape[1] // WIDE):
        block = spread(lanes(y, p), mask)
        a = lanes(x, p).astype(BF)
        parts.append(mm(a, block) if dims is None else dot(a, block, dims))
    return jnp.concatenate(parts, axis=1)


def at_row(start, size):
    return pl.ds(pl.multiple_of(start, size), size)


class Core:
    def __init__(self, tok, wk, wd, wv, wr, up, floor, rate, diag, gain, out, scratch):
        self.tok, self.wk, self.wd, self.wv, self.wr = tok, wk, wd, wv, wr
        self.up, self.floor, self.rate, self.diag, self.gain, self.out = up, floor, rate, diag, gain, out
        (self.pk_s, self.pv_s, self.inv_s, self.grow_s, self.past_s, self.shrink_s, self.g_s, self.wp_s, self.kend_s,
         self.t_s, self.teg_s, self.step_s, self.tcv_s, self.put_s, self.state_s) = scratch
        self.length, self.chans = out.shape
        self.heads = self.chans // HEAD
        self.rank = up.shape[1]
        self.blocks = self.length // SPAN
        self.half = self.length // 2

    def unit(self, block):
        return at_row(block * SPAN, SPAN)

    def decays(self, start):
        chans, rank, tile = self.chans, self.rank, self.half
        lowered = jnp.tanh(mm(self.tok[at_row(start, tile), :], self.wd[...])).astype(BF)
        ri = iota((SPAN, SPAN), 0)
        ci = iota((SPAN, SPAN), 1)
        first = start // SPAN
        pres = [
            (mm(lowered[:, d * rank : (d + 1) * rank], self.up[d]) + self.floor[d : d + 1, :])
            .astype(BF).astype(F32) for d in range(2)
        ]
        for s in range(tile // SPAN):
            falls = [
                -math.exp(-0.5) * jax.nn.sigmoid(pre[s * SPAN : (s + 1) * SPAN]) for pre in pres
            ]
            here = self.unit(first + s)
            for d, fall in enumerate(falls):
                tri = ((ci <= ri) if d == 0 else (ci >= ri)).astype(BF)
                hi, lo = split(fall)
                inside = mm(tri, hi) + mm(tri, lo)
                mid = 0.5 * (inside[SPAN - 1 :] if d == 0 else inside[:1])
                inside = inside - mid
                self.grow_s[d, here, :] = jnp.exp(inside)
                self.past_s[d, here, :] = jnp.exp(inside - fall)
                self.shrink_s[d, here, :] = jnp.exp(-inside)
                self.g_s[d, pl.ds(pl.multiple_of((first + s) * 8, 8), 8), :] = jnp.broadcast_to(
                    jnp.exp(mid), (8, chans))

    def g_of(self, d, block):
        return self.g_s[d, pl.ds(pl.multiple_of(block * 8, 8), 8), :][:1]

    def keys(self, start):
        chans, tile = self.chans, self.half
        at = at_row(start, tile)
        first = start // SPAN
        pk = mm(self.tok[at, :], self.wk[...]).astype(BF)
        self.pk_s[at, :] = pk
        pk = pk.astype(F32)
        inv = lax.rsqrt(head_sum(pk * pk, head_ones(chans)) + 1.0)
        self.inv_s[at, :] = inv
        normed = pk * inv
        rates = jax.nn.sigmoid(self.rate[...])
        units = []
        for s in range(tile // SPAN):
            cut = slice(s * SPAN, (s + 1) * SPAN)
            here = self.unit(first + s)
            for d in range(2):
                g = self.g_of(d, first + s)
                e = -normed[cut] * self.past_s[d, here, :]
                w = normed[cut] * rates[d : d + 1, :] * self.shrink_s[d, here, :]
                self.wp_s[d, here, :] = w.astype(BF)
                self.kend_s[d, here, :] = (w * g).astype(BF)
                units.append((d, first + s, e.astype(BF), (e * g).astype(BF)))
        return units

    def strict(self, d):
        ti = iota((SPAN, self.chans), 0)
        ji = iota((SPAN, self.chans), 1) % HEAD
        return (ti > ji) if d == 0 else (ti < ji)

    def invert(self, units):
        chans = self.chans
        mask = head_ones(WIDE)
        ti = iota((SPAN, chans), 0)
        ji = iota((SPAN, chans), 1) % HEAD
        eye = (ti == ji).astype(F32)
        full = [
            jnp.where(self.strict(d), by_head(e, self.wp_s[d, self.unit(block), :], mask, NT), 0.0)
            for d, block, e, _ in units
        ]
        near = ti // 4 == ji // 4
        base = [jnp.where(near, a, 0.0) for a in full]
        square = [by_head(a, a, mask) for a in base]
        inverse = [eye + a for a in base]
        inverse = [t + by_head(t, a2, mask) for t, a2 in zip(inverse, square)]
        size = 4
        while size < SPAN:
            far = jnp.logical_and(ti // (2 * size) == ji // (2 * size), ti // size != ji // size)
            first = [by_head(t, jnp.where(far, a, 0.0), mask) for t, a in zip(inverse, full)]
            inverse = [t + by_head(f, t, mask) for t, f in zip(inverse, first)]
            size *= 2
        tegs = []
        for (d, block, _, eg), t in zip(units, inverse):
            t = (t - eye).astype(BF)
            self.t_s[d, self.unit(block), :] = t
            tegs.append((eg.astype(F32) + by_head(t, eg, mask)).astype(BF))
        ones = head_ones(chans)
        for (d, block, _, _), teg in zip(units, tegs):
            self.teg_s[d, self.unit(block), :] = teg
            self.step_s[d, at_row(block * chans, chans), :] = (
                dot(teg, self.kend_s[d, self.unit(block), :], TN).astype(BF) * ones)

    def values(self):
        chans = self.chans
        small = head_ones(WIDE)
        mask = head_ones(chans).astype(F32)
        pv = mm(self.tok[...], self.wv[...]).astype(BF)
        self.pv_s[...] = pv
        cv = pv.astype(F32) / self.inv_s[...]
        each = 4
        for group in range(0, self.blocks, each):
            work = []
            for block in range(group, min(group + each, self.blocks)):
                cut = slice(block * SPAN, (block + 1) * SPAN)
                for d in range(2):
                    tcv = cv[cut] + by_head(self.t_s[d, cut, :], cv[cut], small)
                    self.tcv_s[d, cut, :] = tcv
                    work.append((d, cut, tcv.astype(BF)))
            puts = [dot(tcv, self.kend_s[d, cut, :], TN) for d, cut, tcv in work]
            for (d, cut, _), put in zip(work, puts):
                put = put * mask
                self.put_s[d, cut, :] = sum(put[h * HEAD : (h + 1) * HEAD] for h in range(self.heads))

    def scan(self):
        states = [jnp.zeros((HEAD, self.chans), F32) for _ in range(2)]
        for step in range(self.blocks):
            for d in range(2):
                block = step if d == 0 else self.blocks - 1 - step
                cut = slice(block * SPAN, (block + 1) * SPAN)
                state = states[d]
                low = state.astype(BF)
                self.state_s[d, cut, :] = low
                if step < self.blocks - 1:
                    g = self.g_s[d, block * 8 : block * 8 + 1, :]
                    step_w = self.step_s[d, block * self.chans : (block + 1) * self.chans, :]
                    states[d] = state * (g * g) + mm(low, step_w) + self.put_s[d, cut, :]

    def outputs(self, start, tile, p):
        mask = head_ones(WIDE)
        at = at_row(start, tile)
        cols = slice(p * WIDE, (p + 1) * WIDE)
        first = start // SPAN
        pr = mm(self.tok[at, :], self.wr[:, cols]).astype(BF).astype(F32)
        pp = pr * self.pk_s[at, cols].astype(F32)
        rates = jax.nn.sigmoid(self.rate[:, cols])
        both = jnp.sum(rates * self.diag[:, cols], axis=0, keepdims=True)
        inv = self.inv_s[at, cols]
        total = head_sum(pp * both, mask) * self.pv_s[at, cols].astype(F32)
        diags = [head_sum(pp * rates[d : d + 1, :], mask) * inv for d in range(2)]
        ti = iota((SPAN, WIDE), 0)
        ji = iota((SPAN, WIDE), 1) % HEAD
        units = [(d, s) for s in range(tile // SPAN) for d in range(2)]
        bs, reads = [], []
        for d, s in units:
            here = self.unit(first + s)
            q = pr[s * SPAN : (s + 1) * SPAN] * self.grow_s[d, here, cols]
            bs.append(by_head(q, self.wp_s[d, here, cols], mask, NT))
            g = self.g_s[d, pl.ds(pl.multiple_of((first + s) * 8, 8), 8), cols][:1]
            lhs = jnp.concatenate([self.teg_s[d, here, cols], (q * g).astype(BF)], axis=0)
            reads.append(by_head(lhs, self.state_s[d, here, cols], mask, NT))
        ys = [[], []]
        for (d, s), b, read in zip(units, bs, reads):
            exact = self.tcv_s[d, self.unit(first + s), cols] + read[:SPAN]
            b = jnp.where((ti > ji) if d == 0 else (ti < ji), b, 0.0)
            ys[d].append(
                read[SPAN:] + by_head(b, exact, mask) + diags[d][s * SPAN : (s + 1) * SPAN] * exact)
        ys = [jnp.concatenate(y, axis=0) for y in ys]
        means = [head_sum(y, mask) * (1.0 / HEAD) for y in ys]
        centred = [y - mean for y, mean in zip(ys, means)]
        variances = [head_sum(c * c, mask) * (1.0 / HEAD) for c in centred]
        for c, variance in zip(centred, variances):
            total = total + c * lax.rsqrt(variance + 0.00064) * self.gain[:, cols]
        self.out[at, cols] = total.astype(BF)


def core_scratch(length, chans):
    vm = pltpu.VMEM
    both = lambda n, dt: vm((2, n, chans), dt)
    blocks = length // SPAN
    return [
        vm((length, chans), BF), vm((length, chans), BF), vm((length, chans), F32),
        both(length, F32), both(length, F32), both(length, F32), both(blocks * 8, F32),
        both(length, BF), both(length, BF),
        both(length, BF), both(length, BF), both(blocks * chans, BF), both(length, F32),
        both(length, F32), both(length, BF),
    ]


def core_kernel(
    tok_ref, w_ref, up_ref, floor_ref, rate_ref, diag_ref, gain_ref, out_ref,
    eq_s, wp_s, qe_s, kend_s, cv_s, own_s, decay_s, diag_s, t_s, b_s, state_s, y_s,
    arrivals=(),
):
    length, chans = out_ref.shape
    heads = chans // HEAD
    rank = up_ref.shape[1]
    rows = min(256, length)
    blocks = length // SPAN

    def head_ones():
        return (iota((chans, chans), 0) // HEAD == iota((chans, chans), 1) // HEAD).astype(BF)

    def head_sum(x, ones):
        hi, lo = split(x)
        return mm(hi, ones) + mm(lo, ones)

    def at_block(block):
        return pl.ds(pl.multiple_of(block * SPAN, SPAN), SPAN)

    def project(ready):
        tile = SPAN * len(ready)

        def put(ref, x, *lead):
            for s, block in enumerate(ready):
                ref[(*lead, at_block(block), slice(None))] = x[s * SPAN : (s + 1) * SPAN]

        source = jnp.concatenate([tok_ref[at_block(block), :] for block in ready], axis=0)
        pr = mm(source, w_ref[:, :chans]).astype(BF).astype(F32)
        pk = mm(source, w_ref[:, chans : 2 * chans]).astype(BF).astype(F32)
        pv = mm(source, w_ref[:, 2 * chans : 3 * chans]).astype(BF).astype(F32)
        lowered = jnp.tanh(mm(source, w_ref[:, 3 * chans :])).astype(BF)
        ones = head_ones()
        norm2 = head_sum(pk * pk, ones) + 1.0
        inv = lax.rsqrt(norm2)
        scale = norm2 * inv
        normed = pk * inv
        put(cv_s, scale * pv)
        rates = jax.nn.sigmoid(rate_ref[...])
        both = jnp.sum(rates * diag_ref[...], axis=0, keepdims=True)
        put(own_s, head_sum(pr * pk * both, ones) * pv)
        ri = iota((tile, tile), 0)
        ci = iota((tile, tile), 1)
        same = ri // SPAN == ci // SPAN
        whole = same.astype(BF)
        for d in range(2):
            pre = (
                mm(lowered[:, d * rank : (d + 1) * rank], up_ref[d]) + floor_ref[d : d + 1, :]
            ).astype(BF).astype(F32)
            fall = -math.exp(-0.5) * jax.nn.sigmoid(pre)
            tri = jnp.logical_and(same, (ci <= ri) if d == 0 else (ci >= ri)).astype(BF)
            hi, lo = split(fall)
            inclusive = mm(tri, hi) + mm(tri, lo)
            final = mm(whole, hi) + mm(whole, lo)
            half = 0.5 * final
            grow = jnp.exp(inclusive - half)
            shrink = jnp.exp(half - inclusive)
            g = jnp.exp(half)
            e = -normed * (grow * jnp.exp(-fall))
            q = pr * grow
            w = normed * rates[d : d + 1, :] * shrink
            put(wp_s, w.astype(BF), d)
            put(kend_s, (w * g).astype(BF), d)
            eb, qb = e.astype(BF), q.astype(BF)
            eg, qg = (e * g).astype(BF), (q * g).astype(BF)
            g2 = g * g
            put(diag_s, head_sum(pr * normed * rates[d : d + 1, :], ones), d)
            for s, block in enumerate(ready):
                cut = slice(s * SPAN, (s + 1) * SPAN)
                base = pl.multiple_of(block * 2 * SPAN, 2 * SPAN)
                eq_s[d, pl.ds(base, SPAN), :] = eb[cut]
                eq_s[d, pl.ds(base + SPAN, SPAN), :] = qb[cut]
                qe_s[d, pl.ds(base, SPAN), :] = eg[cut]
                qe_s[d, pl.ds(base + SPAN, SPAN), :] = qg[cut]
                decay_s[d, pl.ds(pl.multiple_of(block * 8, 8), 8), :] = g2[
                    s * SPAN : s * SPAN + 8
                ]

    def spread(x, mask):
        x = x.astype(BF)
        if heads > 1:
            x = jnp.concatenate([x] * heads, axis=0)
        return x * mask

    def invert(ready):
        mask = head_ones()
        ti = iota((SPAN, chans), 0)
        ji = iota((SPAN, chans), 1) % HEAD
        eye = (ti == ji).astype(F32)
        work = []
        for block in ready:
            for d in range(2):
                two = pl.ds(pl.multiple_of(block * 2 * SPAN, 2 * SPAN), 2 * SPAN)
                at = pl.ds(pl.multiple_of(block * SPAN, SPAN), SPAN)
                ab = lax.dot_general(
                    eq_s[d, two, :], spread(wp_s[d, at, :], mask), NT, preferred_element_type=F32
                )
                strict = (ti > ji) if d == 0 else (ti < ji)
                b_s[d, at, :] = jnp.where(strict, ab[SPAN:], 0.0).astype(BF)
                work.append((d, at, jnp.where(strict, ab[:SPAN], 0.0)))
        near = ti // 4 == ji // 4
        full = [a for _, _, a in work]
        base = [jnp.where(near, a, 0.0) for a in full]
        square = [mm(a.astype(BF), spread(a, mask)) for a in base]
        inverse = [eye + a for a in base]
        inverse = [t + mm(t.astype(BF), spread(a2, mask)) for t, a2 in zip(inverse, square)]
        size = 4
        while size < SPAN:
            far = jnp.logical_and(ti // (2 * size) == ji // (2 * size), ti // size != ji // size)
            first = [
                mm(t.astype(BF), spread(jnp.where(far, a, 0.0), mask))
                for t, a in zip(inverse, full)
            ]
            inverse = [t + mm(f.astype(BF), spread(t, mask)) for t, f in zip(inverse, first)]
            size *= 2
        for (d, at, _), t in zip(work, inverse):
            t_s[d, at, :] = (t - eye).astype(BF)

    for settle, ready in arrivals:
        settle()
        project(ready)
        invert(ready)

    state_s[...] = jnp.zeros_like(state_s)

    @pl.loop(0, blocks)
    def _(step):
        mask = head_ones()
        for d in range(2):
            block = step if d == 0 else blocks - 1 - step
            two = pl.ds(pl.multiple_of(block * 2 * SPAN, 2 * SPAN), 2 * SPAN)
            at = pl.ds(pl.multiple_of(block * SPAN, SPAN), SPAN)
            state = state_s[d]
            read = lax.dot_general(
                qe_s[d, two, :], state.astype(BF), NT, preferred_element_type=F32
            )
            x = cv_s[at, :] + read[:SPAN]
            exact = x + mm(t_s[d, at, :], spread(x, mask))
            a = exact.astype(BF)
            y_s[d, at, :] = read[SPAN:] + mm(b_s[d, at, :], spread(a, mask)) + diag_s[d, at, :] * exact
            decay = decay_s[d, pl.ds(pl.multiple_of(block * 8, 8), 8), :][:1]
            put = lax.dot_general(a, kend_s[d, at, :], TN, preferred_element_type=F32)
            state_s[d] = state * decay + put * mask.astype(F32)

    @pl.loop(0, length // rows)
    def _(step):
        at = pl.ds(pl.multiple_of(step * rows, rows), rows)
        ones = head_ones()
        total = own_s[at, :]
        for d in range(2):
            y = y_s[d, at, :]
            centred = y - head_sum(y, ones) * (1.0 / HEAD)
            variance = head_sum(centred * centred, ones) * (1.0 / HEAD)
            total = total + centred * lax.rsqrt(variance + 0.00064) * gain_ref[...]
        out_ref[at, :] = total.astype(BF)


MESH = pl.DeviceIdType.MESH


def whole_kernel(
    sp, dp, tok_ref, w_ref, up_ref, floor_ref, rate_ref, diag_ref, gain_ref, out_ref,
    tok_all, w_all, out_all, slots,
    ring_out, ring_in, far_out, far_in, pass_out, pass_in, back_out, back_in, *scratch,
):
    rows = tok_ref.shape[0]
    half_rows = rows // 2
    depth = w_ref.shape[0]
    chans = out_all.shape[1]
    chips = dp // 2
    z = lax.axis_index("sp")
    me = lax.axis_index("dp")
    chip = me // 2
    core = me % 2
    partner = chip * 2 + 1 - core

    def peer(k):
        return lax.rem(chip + k, chips) * 2 + core

    def z_peer(k):
        return lax.rem(z + k, sp)

    barrier = pltpu.get_barrier_semaphore()
    for target in [(z, partner)] + [(z, peer(k)) for k in range(1, chips)] + [
        (z_peer(k), me) for k in range(1, sp)
    ]:
        pl.semaphore_signal(barrier, inc=1, device_id=target, device_id_type=MESH)
    pl.semaphore_wait(barrier, chips + sp - 1)

    def remote(src, dst, out_sem, in_sem, target):
        copy = pltpu.make_async_remote_copy(
            src_ref=src, dst_ref=dst, send_sem=out_sem, recv_sem=in_sem,
            device_id=target, device_id_type=MESH,
        )
        copy.start()
        return copy

    def w_at(device):
        return pl.ds(pl.multiple_of(device * depth, depth), depth)

    def ring_step(s):
        copies = []
        for way in range(2):
            owner = z_peer(sp - s) if way == 0 else z_peer(s)
            at = pl.ds(
                pl.multiple_of(owner * rows + way * half_rows, half_rows), half_rows
            )
            first = tok_ref.at[pl.ds(way * half_rows, half_rows), :]
            copies.append(
                remote(
                    first if s == 0 else tok_all.at[at, :], tok_all.at[at, :],
                    ring_out.at[way, s], ring_in.at[way, s],
                    (z_peer(1) if way == 0 else z_peer(sp - 1), me),
                )
            )
        return copies

    ring = [ring_step(0)] if sp > 1 else []
    far = [
        remote(w_ref, w_all.at[w_at(me), :], far_out.at[k], far_in.at[k], (z, peer(k)))
        for k in range(1, chips)
    ]
    passed = [remote(w_ref, w_all.at[w_at(me), :], pass_out.at[0], pass_in.at[0], (z, partner))]
    w_all[w_at(me), :] = w_ref[...]
    tok_all[pl.ds(pl.multiple_of(z * rows, rows), rows), :] = tok_ref[...]
    for s in range(max(sp, chips) - 1):
        if s < sp - 2:
            for copy in ring[s]:
                copy.wait_recv()
            ring.append(ring_step(s + 1))
        if s < chips - 1:
            far[s].wait_recv()
            block = w_at(peer(chips - 1 - s))
            passed.append(
                remote(
                    w_all.at[block, :], w_all.at[block, :],
                    pass_out.at[s + 1], pass_in.at[s + 1], (z, partner),
                )
            )
    for copy in passed:
        copy.wait_recv()

    def last_ring():
        for copy in ring[-1]:
            copy.wait_recv()

    per = rows // SPAN
    arrivals = [(lambda: None, [z * per + b for b in range(per)])]
    for s in range(sp - 1):
        before, after = z_peer(sp - 1 - s), z_peer(s + 1)
        ready = [before * per + b for b in range(per // 2)]
        ready += [after * per + b for b in range(per // 2, per)]
        arrivals.append((last_ring if s == sp - 2 else lambda: None, ready))

    core_kernel(
        tok_all, w_all, up_ref, floor_ref, rate_ref, diag_ref, gain_ref, out_all, *scratch,
        arrivals=arrivals,
    )
    for copy in far + passed + [c for pair in ring for c in pair]:
        copy.wait_send()

    def out_at(owner):
        return pl.ds(pl.multiple_of(owner * rows, rows), rows)

    back = [
        remote(
            out_all.at[out_at(z_peer(k)), :], slots.at[z], back_out.at[k], back_in.at[k],
            (z_peer(k), me),
        )
        for k in range(1, sp)
    ]
    slots[z] = out_all[out_at(z), :]
    for copy in back:
        copy.wait()
    for s in range(sp):
        out_ref[:, s * chans : (s + 1) * chans] = slots[s]


def whole_call(sp, dp, rows, depth, chans, width):
    vm = pltpu.VMEM
    dma = pltpu.SemaphoreType.DMA
    length = rows * sp
    both = lambda n, dt: vm((2, n, chans), dt)
    return pl.pallas_call(
        functools.partial(whole_kernel, sp, dp),
        out_shape=jax.ShapeDtypeStruct((rows, chans * sp), BF),
        in_specs=[pl.BlockSpec(memory_space=vm)] * 7,
        out_specs=pl.BlockSpec(memory_space=vm),
        scratch_shapes=[
            vm((length, depth), BF), vm((depth, width), BF), vm((length, chans), BF),
            vm((sp, rows, chans), BF),
            dma((2, sp)), dma((2, sp)), dma((dp,)), dma((dp,)), dma((dp,)), dma((dp,)),
            dma((sp,)), dma((sp,)),
            both(2 * length, BF), both(length, BF), both(2 * length, BF), both(length, BF),
            vm((length, chans), F32), vm((length, chans), F32),
            both(length // SPAN * 8, F32), both(length, F32), both(length, BF), both(length, BF),
            vm((2, chans, chans), F32), both(length, F32),
        ],
        compiler_params=pltpu.CompilerParams(
            vmem_limit_bytes=58 * 1024 * 1024, collective_id=0, has_side_effects=True
        ),
        name="whole",
    )


def halves_kernel(
    sp, side, other, tok_ref, wr_ref, wk_ref, wv_ref, wd_ref, up_ref, floor_ref, rate_ref, diag_ref, gain_ref,
    out_ref, tok_all, wk_all, wv_all, wr_all, wd_all, up_s, floor_s, rate_s, diag_s, gain_s, out_all,
    w_in, w_out, relay_out, d_in, d_pass, t_in, t_pass, t_out, t_fwd, p_in, p_out, o_in, o_out, here, *scratch,
):
    rows = tok_ref.shape[0]
    depth = wk_ref.shape[0]
    chans = wk_all.shape[1]
    half = sp // 2
    part = rows // 4
    z = lax.axis_index("sp")
    me = lax.axis_index("dp")
    core = me % 2
    chip = me // 2
    cy, cx = chip // side, chip % side
    h = z // half
    j = z % half
    u = jnp.where(h == 1, j, half - 1 - j)
    slot = u * 2 + core
    partner = chip * 2 + 1 - core

    def layer(hh, uu):
        return half - 1 - uu + hh * (2 * uu + 1)

    def x_peer(k):
        return cy * side + lax.rem(cx + k, side)

    def y_peer(k):
        return lax.rem(cy + k, other) * side + cx

    x_peers = [x_peer(k) for k in range(1, side)]
    y_peers = [y_peer(k) for k in range(1, other)]

    def local(src, dst, n):
        copy = pltpu.make_async_copy(src, dst, here.at[n])
        copy.start()
        return copy

    def cols(who):
        return pl.ds(pl.multiple_of(who * chans, chans), chans)

    mine = at_row(me * depth, depth)
    own = [
        local(wd_ref, wd_all.at[mine, :], 0),
        local(wk_ref.at[:, cols(slot)], wk_all.at[mine, :], 1),
        local(up_ref.at[:, :, cols(slot)], up_s, 2),
        local(floor_ref.at[:, cols(slot)], floor_s, 3),
        local(wv_ref.at[:, cols(slot)], wv_all.at[mine, :], 4),
        local(wr_ref.at[:, cols(slot)], wr_all.at[mine, :], 5),
    ]

    @pl.when(core == h)
    def _():
        local(tok_ref, tok_all.at[at_row(z * rows, rows), :], 6)

    barrier = pltpu.get_barrier_semaphore()
    greet = [(z, p * 2 + k) for p in x_peers + y_peers for k in range(2)]
    greet += [(lax.rem(z + n, sp), chip * 2 + k) for n in range(1, sp) for k in range(2)]
    greet.append((z, partner))
    for target in greet:
        pl.semaphore_signal(barrier, inc=1, device_id=target, device_id_type=MESH)
    pl.semaphore_wait(barrier, len(greet))

    def remote(src, dst, out_sem, in_sem, target):
        return pltpu.make_async_remote_copy(
            src_ref=src, dst_ref=dst, send_sem=out_sem, recv_sem=in_sem,
            device_id=target, device_id_type=MESH,
        )

    def go(copy):
        copy.start()
        return copy

    sent = []
    wide = chans // WIDE
    pieces = [(wk_ref, wk_all, 0, chans), (wv_ref, wv_all, 0, chans)]
    pieces += [(wr_ref, wr_all, p * WIDE, WIDE) for p in range(wide)]
    decay = len(pieces)

    def take(n, who):
        src, _, low, size = pieces[n]
        return src.at[:, pl.ds(pl.multiple_of(who * chans + low, WIDE), size)]

    def landing(n, block):
        _, dst, low, size = pieces[n]
        return dst.at[block, low : low + size]

    def direct(n):
        for i, p in enumerate(x_peers + y_peers):
            for k in range(2):
                sent.append(go(remote(
                    take(n, u * 2 + k), landing(n, mine),
                    w_out.at[n, i * 2 + k], w_in.at[n, me], (z, p * 2 + k),
                )))
        last = 2 * len(x_peers + y_peers)
        sent.append(go(remote(
            take(n, u * 2 + 1 - core), landing(n, mine),
            w_out.at[n, last], w_in.at[n, me], (z, partner),
        )))

    def wait_for(sem, dst):
        remote(dst, dst, sem, sem, (z, partner)).wait_recv()

    def arrived(sem, dst, block):
        wait_for(sem, dst.at[block, :])

    def w_rows(p, c):
        return at_row((p * 2 + c) * depth, depth)

    def relay(n):
        count = 0
        for c, froms, tos in ((0, x_peers, y_peers), (1, y_peers, x_peers)):
            for p in froms:
                block = w_rows(p, c)
                wait_for(w_in.at[n, p * 2 + c], landing(n, block))
                for q in tos:
                    sent.append(go(remote(
                        landing(n, block), landing(n, block),
                        relay_out.at[n, count], w_in.at[n, p * 2 + c], (z, q * 2 + core),
                    )))
                    count += 1

    def finish(n):
        for c, others in ((1, x_peers), (0, y_peers)):
            for p in others:
                wait_for(w_in.at[n, p * 2 + c], landing(n, w_rows(p, c)))
        for ky in range(1, other):
            for kx in range(1, side):
                p = lax.rem(cy + ky, other) * side + lax.rem(cx + kx, side)
                for c in range(2):
                    wait_for(w_in.at[n, p * 2 + c], landing(n, w_rows(p, c)))
        wait_for(w_in.at[n, partner], landing(n, w_rows(chip, 1 - core)))

    def decay_direct():
        for i, p in enumerate(x_peers + y_peers):
            sent.append(go(remote(
                wd_ref, wd_all.at[mine, :], w_out.at[decay, i], d_in.at[me], (z, p * 2 + core))))
        sent.append(go(remote(
            wd_ref, wd_all.at[mine, :], w_out.at[decay, len(x_peers + y_peers)], d_in.at[me], (z, partner))))

    def decay_pass(p, n):
        block = w_rows(p, core)
        sent.append(go(remote(
            wd_all.at[block, :], wd_all.at[block, :], d_pass.at[n], d_in.at[p * 2 + core], (z, partner))))

    late = []

    def decay_relay():
        for c, froms, tos in ((0, x_peers, y_peers), (1, y_peers, x_peers)):
            @pl.when(core == c)
            def _():
                count = 0
                for p in froms:
                    block = w_rows(p, c)
                    arrived(d_in.at[p * 2 + c], wd_all, block)
                    for q in tos:
                        go(remote(
                            wd_all.at[block, :], wd_all.at[block, :],
                            relay_out.at[decay, count], d_in.at[p * 2 + c], (z, q * 2 + c)))
                        count += 1
                for p in tos:
                    arrived(d_in.at[p * 2 + c], wd_all, w_rows(p, c))

            def close(c=c, froms=froms, tos=tos):
                @pl.when(core == c)
                def _():
                    count = 0
                    for p in froms:
                        block = w_rows(p, c)
                        for q in tos:
                            remote(
                                wd_all.at[block, :], wd_all.at[block, :],
                                relay_out.at[decay, count], d_in.at[p * 2 + c], (z, q * 2 + c)).wait_send()
                            count += 1

            late.append(close)
        for n, p in enumerate(x_peers + y_peers):
            decay_pass(p, n)

    def decay_finish():
        n = len(x_peers + y_peers)
        corners = [
            lax.rem(cy + ky, other) * side + lax.rem(cx + kx, side)
            for ky in range(1, other) for kx in range(1, side)
        ]
        for p in corners:
            arrived(d_in.at[p * 2 + core], wd_all, w_rows(p, core))
            decay_pass(p, n)
            n += 1
        arrived(d_in.at[partner], wd_all, w_rows(chip, 1 - core))
        for p in x_peers + y_peers + corners:
            arrived(d_in.at[p * 2 + 1 - core], wd_all, w_rows(p, 1 - core))

    def t_rows(s, i):
        return at_row(s * rows + i * part, part)

    def block_sends(act):
        def all_parts(target_layer, first):
            for i in range(4):
                act(remote(
                    tok_ref.at[pl.ds(i * part, part), :], tok_all.at[t_rows(z, i), :],
                    t_out.at[first + i], t_in.at[z, i // 2], (target_layer, chip * 2 + i % 2)))

        @pl.when(core != h)
        def _():
            all_parts(layer(core, 0), 0)

        @pl.when(jnp.logical_and(core == h, u + 1 < half))
        def _():
            all_parts(layer(h, u + 1), 0)

        @pl.when(jnp.logical_and(core == h, u > 0))
        def _():
            all_parts(layer(h, u - 1), 4)

        @pl.when(core == h)
        def _():
            act(remote(
                tok_ref, tok_all.at[at_row(z * rows, rows), :], t_out.at[8], t_pass.at[z, 0], (z, partner)))

    def forward(s, outward, inward, n, q, act):
        block = t_rows(s, 2 * q + core)
        for cond, step in ((outward, 1), (inward, -1)):
            if cond is not None:
                @pl.when(cond)
                def _():
                    act(remote(
                        tok_all.at[block, :], tok_all.at[block, :], t_fwd.at[0, n, q], t_in.at[s, q],
                        (layer(h, u + step), me)))
        act(remote(
            tok_all.at[block, :], tok_all.at[block, :], t_fwd.at[1, n, q], t_pass.at[s, q], (z, partner)))

    near = [lax.rem(u + k, half) for k in range(1, half)]
    sources = [
        (layer(h, v), jnp.logical_and(u > v, u + 1 < half), jnp.logical_and(u < v, u > 0)) for v in near
    ]
    sources += [(layer(1 - h, v), u + 1 < half, None) for v in range(half)]

    def take_tokens(n, q):
        s, outward, inward = sources[n]
        arrived(t_in.at[s, q], tok_all, t_rows(s, 2 * q + core))
        forward(s, outward, inward, n, q, go)

    def take_far(now, q):
        @pl.when(now)
        def _():
            for n in range(half - 1, len(sources)):
                take_tokens(n, q)

    def own_tokens():
        block = at_row(z * rows, rows)

        @pl.when(core == h)
        def _():
            pltpu.make_async_copy(tok_ref, tok_all.at[block, :], here.at[6]).wait()

        @pl.when(core != h)
        def _():
            arrived(t_pass.at[z, 0], tok_all, block)

    def passed_tokens(n):
        s = sources[n][0]
        for q in range(2):
            arrived(t_pass.at[s, q], tok_all, t_rows(s, 2 * q + 1 - core))

    goal = (layer(core, z // 2), chip * 2 + z % 2)
    stay = jnp.logical_and(goal[0] == z, z % 2 == core)
    smalls = [(rate_ref, rate_s), (diag_ref, diag_s), (gain_ref, gain_s)]

    @pl.when(jnp.logical_not(stay))
    def _():
        for n, (src, dst) in enumerate(smalls):
            go(remote(src, dst, p_out.at[n], p_in.at[n], goal))

    @pl.when(stay)
    def _():
        for n, (src, dst) in enumerate(smalls):
            pltpu.make_async_copy(src, dst, p_in.at[n]).start()

    decay_direct()
    block_sends(go)
    direct(0)
    decay_relay()
    take_far(u + 1 < half, 0)
    relay(0)
    direct(1)
    direct(2)
    for n in range(half - 1):
        for q in range(2):
            take_tokens(n, q)
    take_far(u + 1 < half, 1)
    decay_finish()
    for n in (0, 2, 3):
        own[n].wait()
    own_tokens()
    for n in range(half - 1):
        passed_tokens(n)
    work = Core(
        tok_all, wk_all, wd_all, wv_all, wr_all, up_s, floor_s, rate_s, diag_s, gain_s, out_all, scratch)
    near_rows = h * half * rows
    far_rows = (1 - h) * half * rows
    work.decays(near_rows)
    take_far(u + 1 == half, 0)
    finish(0)
    own[1].wait()

    @pl.when(jnp.logical_not(stay))
    def _():
        for n, (src, dst) in enumerate(smalls):
            remote(src, dst, p_out.at[n], p_in.at[n], goal).wait_send()
    for n, (src, dst) in enumerate(smalls):
        remote(dst, dst, p_in.at[n], p_in.at[n], (z, partner)).wait_recv()

    units = work.keys(near_rows)
    work.invert(units)
    take_far(u + 1 == half, 1)
    relay(1)
    for p in range(1, wide):
        direct(2 + p)
    for n in range(half - 1, len(sources)):
        passed_tokens(n)
    work.decays(far_rows)
    units = work.keys(far_rows)
    work.invert(units)
    relay(2)
    finish(1)
    own[4].wait()
    work.values()
    for p in range(1, wide):
        relay(2 + p)
    work.scan()

    def give(s, p, n, act):
        block = at_row(s * rows, rows)
        low = p * WIDE
        act(remote(
            out_all.at[block, low : low + WIDE],
            out_ref.at[:, pl.ds(pl.multiple_of(slot * chans + low, WIDE), WIDE)],
            o_out.at[p, n], o_in.at[p, slot], (s, chip * 2 + h)))

    def give_far(p, act):
        for v in range(half):
            give(layer(1 - h, v), p, v, act)

    def give_near(p, act):
        for n in range(half - 1):
            give(sources[n][0], p, half + n, act)

        @pl.when(core != h)
        def _():
            give(z, p, sp - 1, act)

    own[5].wait()
    for p in range(wide):
        finish(2 + p)
        work.outputs(far_rows, half * rows, p)
        give_far(p, go)
        work.outputs(near_rows, half * rows, p)
        give_near(p, go)

    @pl.when(core == h)
    def _():
        out_ref[:, cols(slot)] = out_all[at_row(z * rows, rows), :]

    def stop(copy):
        copy.wait_send()

    block_sends(stop)
    for n, (s, outward, inward) in enumerate(sources):
        for q in range(2):
            forward(s, outward, inward, n, q, stop)
    for copy in sent:
        copy.wait_send()
    for close in late:
        close()
    for p in range(wide):
        give_far(p, stop)
        give_near(p, stop)
        for g in range(sp):
            low = g * chans + p * WIDE

            @pl.when(jnp.logical_not(jnp.logical_and(core == h, slot == g)))
            def _():
                wait_for(o_in.at[p, g], out_ref.at[:, low : low + WIDE])


def halves_call(sp, dp, side, rows, width, depth, chans, rank):
    vm = pltpu.VMEM
    dma = pltpu.SemaphoreType.DMA
    chips = dp // 2
    other = chips // side
    peers = side + other - 2
    corners = (side - 1) * (other - 1)
    length = rows * sp
    wide = chans // WIDE
    return pl.pallas_call(
        functools.partial(halves_kernel, sp, side, other),
        out_shape=jax.ShapeDtypeStruct((rows, chans * sp), BF),
        in_specs=[pl.BlockSpec(memory_space=pl.ANY)] * 10,
        out_specs=pl.BlockSpec(memory_space=vm),
        scratch_shapes=[
            vm((length, width), BF), vm((width, chans), BF), vm((width, chans), BF), vm((width, chans), BF),
            vm((width, 2 * rank), BF), vm((2, rank, chans), BF), vm((2, chans), F32), vm((2, chans), F32),
            vm((2, chans), F32), vm((1, chans), F32), vm((length, chans), BF),
            dma((2 + wide, dp)), dma((3 + wide, 2 * peers + 1)), dma((3 + wide, 2 * corners)), dma((dp,)), dma((peers + corners,)),
            dma((sp, 2)), dma((sp, 2)), dma((9,)), dma((2, sp, 2)), dma((3,)), dma((3,)), dma((wide, sp)), dma((wide, sp)),
            dma((7,)),
        ] + core_scratch(length, chans),
        compiler_params=pltpu.CompilerParams(
            vmem_limit_bytes=32 * 1024 * 1024, collective_id=0, has_side_effects=True
        ),
        name="halves",
    )


def per_device(
    sp, dp,
    tokens, receptance_weight, key_projection_weight, value_projection_weight,
    decay_down_weight, decay_up_weight, decay_floor_level, correction_rate_logit,
    diagonal_address_factor, head_norm_gain,
):
    rows, width = tokens.shape[1:]
    depth, channels = receptance_weight.shape
    chans = channels // sp
    side = math.isqrt(dp // 2)
    gain = head_norm_gain[None, :]
    if chans % 128 == 0 and sp % 2 == 0 and dp == 2 * side * side and rows % SPAN == 0:
        given = [
            tokens[0], receptance_weight, key_projection_weight, value_projection_weight, decay_down_weight,
            decay_up_weight, decay_floor_level, correction_rate_logit, diagonal_address_factor, gain]
        given = [pltpu.with_memory_space_constraint(x, pltpu.HBM) for x in given]
        mixed = halves_call(sp, dp, side, rows, width, depth, chans, decay_up_weight.shape[1])(*given)
        return mixed[None]
    start = lax.axis_index("sp") * chans

    def mine(x):
        return lax.dynamic_slice_in_dim(x, start, chans, axis=x.ndim - 1)

    packed = jnp.concatenate(
        [mine(receptance_weight), mine(key_projection_weight), mine(value_projection_weight),
         decay_down_weight], axis=1)
    mixed = whole_call(sp, dp, rows, width, chans, packed.shape[1])(
        tokens[0], packed, mine(decay_up_weight), mine(decay_floor_level),
        correction_rate_logit, diagonal_address_factor, gain)
    return mixed[None]


def solution(mesh):
    in_specs = (
        P("dp", "sp", None), P("dp", None), P("dp", None), P("dp", None), P("dp", None),
        P(), P(), P(None, "sp"), P(None, "sp"), P("sp"),
    )
    return jax.shard_map(
        functools.partial(per_device, mesh.shape["sp"], mesh.shape["dp"]), mesh=mesh, in_specs=in_specs,
        out_specs=P("dp", "sp", None), check_vma=False,
    )
```

```python
import functools, math
import jax, jax.numpy as jnp
from jax import lax
from jax.experimental import pallas as pl
from jax.experimental.pallas import tpu as pltpu
from jax.sharding import PartitionSpec as P
HEAD = 64
SPAN = 64
BF = jnp.bfloat16
F32 = jnp.float32
NT = (((1,), (1,)), ((), ()))
TN = (((0,), (0,)), ((), ()))


def mm(a, b):
    return jnp.dot(a, b, preferred_element_type=F32)


def dot(a, b, dims):
    return lax.dot_general(a, b, dims, preferred_element_type=F32)


def split(x):
    hi = x.astype(BF)
    return hi, (x - hi.astype(F32)).astype(BF)


def iota(shape, axis):
    return lax.broadcasted_iota(jnp.int32, shape, axis)


def head_ones(chans):
    return (iota((chans, chans), 0) // HEAD == iota((chans, chans), 1) // HEAD).astype(BF)


def head_sum(x, ones):
    hi, lo = split(x)
    if ones.shape[0] > WIDE:
        return mm(hi, ones) + mm(lo, ones)
    return mm(jnp.concatenate([hi, lo], axis=1), jnp.concatenate([ones, ones], axis=0))


def spread(x, mask):
    x = x.astype(BF)
    heads = mask.shape[0] // HEAD
    if heads > 1:
        x = jnp.concatenate([x] * heads, axis=0)
    return x * mask


WIDE = 128


def lanes(x, p):
    return x[:, p * WIDE : (p + 1) * WIDE]


def by_head(x, y, mask, dims=None):
    parts = []
    for p in range(x.shape[1] // WIDE):
        block = spread(lanes(y, p), mask)
        a = lanes(x, p).astype(BF)
        parts.append(mm(a, block) if dims is None else dot(a, block, dims))
    return jnp.concatenate(parts, axis=1)


def at_row(start, size):
    return pl.ds(pl.multiple_of(start, size), size)


def halved(tok, start, size, w):
    part = size // 2
    return jnp.concatenate([mm(tok[at_row(start + i * part, part), :], w) for i in range(2)], axis=0)


class Core:
    def __init__(self, tok, wk, wd, wv, wr, up, floor, rate, diag, gain, out, scratch):
        self.tok, self.wk, self.wd, self.wv, self.wr = tok, wk, wd, wv, wr
        self.up, self.floor, self.rate, self.diag, self.gain, self.out = up, floor, rate, diag, gain, out
        (self.pk_s, self.pv_s, self.inv_s, self.grow_s, self.past_s, self.shrink_s, self.g_s, self.wp_s, self.kend_s,
         self.t_s, self.teg_s, self.step_s, self.tcv_s, self.put_s, self.state_s) = scratch
        self.length, self.chans = out.shape
        self.heads = self.chans // HEAD
        self.rank = up.shape[1]
        self.blocks = self.length // SPAN
        self.half = self.length // 2

    def unit(self, block):
        return at_row(block * SPAN, SPAN)

    def decays(self, start):
        chans, rank, tile = self.chans, self.rank, self.half
        lowered = jnp.tanh(halved(self.tok, start, tile, self.wd[...])).astype(BF)
        ri = iota((SPAN, SPAN), 0)
        ci = iota((SPAN, SPAN), 1)
        first = start // SPAN
        pres = [
            (mm(lowered[:, d * rank : (d + 1) * rank], self.up[d]) + self.floor[d : d + 1, :])
            .astype(BF).astype(F32) for d in range(2)
        ]
        for s in range(tile // SPAN):
            falls = [
                -math.exp(-0.5) * jax.nn.sigmoid(pre[s * SPAN : (s + 1) * SPAN]) for pre in pres
            ]
            here = self.unit(first + s)
            for d, fall in enumerate(falls):
                tri = ((ci <= ri) if d == 0 else (ci >= ri)).astype(BF)
                hi, lo = split(fall)
                inside = mm(tri, hi) + mm(tri, lo)
                mid = 0.5 * (inside[SPAN - 1 :] if d == 0 else inside[:1])
                inside = inside - mid
                self.grow_s[d, here, :] = jnp.exp(inside)
                self.past_s[d, here, :] = jnp.exp(inside - fall)
                self.shrink_s[d, here, :] = jnp.exp(-inside)
                self.g_s[d, pl.ds(pl.multiple_of((first + s) * 8, 8), 8), :] = jnp.broadcast_to(
                    jnp.exp(mid), (8, chans))

    def g_of(self, d, block):
        return self.g_s[d, pl.ds(pl.multiple_of(block * 8, 8), 8), :][:1]

    def keys(self, start):
        chans, tile = self.chans, self.half
        at = at_row(start, tile)
        first = start // SPAN
        pk = halved(self.tok, start, tile, self.wk[...]).astype(BF)
        self.pk_s[at, :] = pk
        pk = pk.astype(F32)
        inv = lax.rsqrt(head_sum(pk * pk, head_ones(chans)) + 1.0)
        self.inv_s[at, :] = inv
        normed = pk * inv
        rates = jax.nn.sigmoid(self.rate[...])
        units = []
        for s in range(tile // SPAN):
            cut = slice(s * SPAN, (s + 1) * SPAN)
            here = self.unit(first + s)
            for d in range(2):
                g = self.g_of(d, first + s)
                e = -normed[cut] * self.past_s[d, here, :]
                w = normed[cut] * rates[d : d + 1, :] * self.shrink_s[d, here, :]
                self.wp_s[d, here, :] = w.astype(BF)
                self.kend_s[d, here, :] = (w * g).astype(BF)
                units.append((d, first + s, e.astype(BF), (e * g).astype(BF)))
        return units

    def strict(self, d):
        ti = iota((SPAN, self.chans), 0)
        ji = iota((SPAN, self.chans), 1) % HEAD
        return (ti > ji) if d == 0 else (ti < ji)

    def invert(self, units):
        chans = self.chans
        mask = head_ones(WIDE)
        ti = iota((SPAN, chans), 0)
        ji = iota((SPAN, chans), 1) % HEAD
        eye = (ti == ji).astype(F32)
        full = [
            jnp.where(self.strict(d), by_head(e, self.wp_s[d, self.unit(block), :], mask, NT), 0.0)
            for d, block, e, _ in units
        ]
        near = ti // 4 == ji // 4
        base = [jnp.where(near, a, 0.0) for a in full]
        square = [by_head(a, a, mask) for a in base]
        inverse = [eye + a for a in base]
        inverse = [t + by_head(t, a2, mask) for t, a2 in zip(inverse, square)]
        size = 4
        while size < SPAN:
            far = jnp.logical_and(ti // (2 * size) == ji // (2 * size), ti // size != ji // size)
            first = [by_head(t, jnp.where(far, a, 0.0), mask) for t, a in zip(inverse, full)]
            inverse = [t + by_head(f, t, mask) for t, f in zip(inverse, first)]
            size *= 2
        tegs = []
        for (d, block, _, eg), t in zip(units, inverse):
            t = (t - eye).astype(BF)
            self.t_s[d, self.unit(block), :] = t
            tegs.append((eg.astype(F32) + by_head(t, eg, mask)).astype(BF))
        ones = head_ones(chans)
        for (d, block, _, _), teg in zip(units, tegs):
            self.teg_s[d, self.unit(block), :] = teg
            self.step_s[d, at_row(block * chans, chans), :] = (
                dot(teg, self.kend_s[d, self.unit(block), :], TN).astype(BF) * ones)

    def values(self):
        chans = self.chans
        small = head_ones(WIDE)
        mask = head_ones(chans).astype(F32)
        for r in range(0, self.length, self.half):
            self.pv_s[r : r + self.half, :] = mm(self.tok[r : r + self.half, :], self.wv[...]).astype(BF)
        cv = self.pv_s[...].astype(F32) / self.inv_s[...]
        each = 4
        for group in range(0, self.blocks, each):
            work = []
            for block in range(group, min(group + each, self.blocks)):
                cut = slice(block * SPAN, (block + 1) * SPAN)
                for d in range(2):
                    tcv = cv[cut] + by_head(self.t_s[d, cut, :], cv[cut], small)
                    self.tcv_s[d, cut, :] = tcv
                    work.append((d, cut, tcv.astype(BF)))
            puts = [dot(tcv, self.kend_s[d, cut, :], TN) for d, cut, tcv in work]
            for (d, cut, _), put in zip(work, puts):
                put = put * mask
                self.put_s[d, cut, :] = sum(put[h * HEAD : (h + 1) * HEAD] for h in range(self.heads))

    def scan(self):
        states = [jnp.zeros((HEAD, self.chans), F32) for _ in range(2)]
        for step in range(self.blocks):
            for d in range(2):
                block = step if d == 0 else self.blocks - 1 - step
                cut = slice(block * SPAN, (block + 1) * SPAN)
                state = states[d]
                low = state.astype(BF)
                self.state_s[d, cut, :] = low
                if step < self.blocks - 1:
                    g = self.g_s[d, block * 8 : block * 8 + 1, :]
                    step_w = self.step_s[d, block * self.chans : (block + 1) * self.chans, :]
                    states[d] = state * (g * g) + mm(low, step_w) + self.put_s[d, cut, :]

    def outputs(self, start, tile, p):
        mask = head_ones(WIDE)
        at = at_row(start, tile)
        cols = slice(p * WIDE, (p + 1) * WIDE)
        first = start // SPAN
        pr = mm(self.tok[at, :], self.wr[:, cols]).astype(BF).astype(F32)
        pp = pr * self.pk_s[at, cols].astype(F32)
        rates = jax.nn.sigmoid(self.rate[:, cols])
        both = jnp.sum(rates * self.diag[:, cols], axis=0, keepdims=True)
        inv = self.inv_s[at, cols]
        total = head_sum(pp * both, mask) * self.pv_s[at, cols].astype(F32)
        diags = [head_sum(pp * rates[d : d + 1, :], mask) * inv for d in range(2)]
        ti = iota((SPAN, WIDE), 0)
        ji = iota((SPAN, WIDE), 1) % HEAD
        units = [(d, s) for s in range(tile // SPAN) for d in range(2)]
        bs, reads = [], []
        for d, s in units:
            here = self.unit(first + s)
            q = pr[s * SPAN : (s + 1) * SPAN] * self.grow_s[d, here, cols]
            bs.append(by_head(q, self.wp_s[d, here, cols], mask, NT))
            g = self.g_s[d, pl.ds(pl.multiple_of((first + s) * 8, 8), 8), cols][:1]
            lhs = jnp.concatenate([self.teg_s[d, here, cols], (q * g).astype(BF)], axis=0)
            reads.append(by_head(lhs, self.state_s[d, here, cols], mask, NT))
        ys = [[], []]
        for (d, s), b, read in zip(units, bs, reads):
            exact = self.tcv_s[d, self.unit(first + s), cols] + read[:SPAN]
            b = jnp.where((ti > ji) if d == 0 else (ti < ji), b, 0.0)
            ys[d].append(
                read[SPAN:] + by_head(b, exact, mask) + diags[d][s * SPAN : (s + 1) * SPAN] * exact)
        ys = [jnp.concatenate(y, axis=0) for y in ys]
        means = [head_sum(y, mask) * (1.0 / HEAD) for y in ys]
        centred = [y - mean for y, mean in zip(ys, means)]
        variances = [head_sum(c * c, mask) * (1.0 / HEAD) for c in centred]
        for c, variance in zip(centred, variances):
            total = total + c * lax.rsqrt(variance + 0.00064) * self.gain[:, cols]
        self.out[at, cols] = total.astype(BF)


def core_scratch(length, chans):
    vm = pltpu.VMEM
    both = lambda n, dt: vm((2, n, chans), dt)
    blocks = length // SPAN
    return [
        vm((length, chans), BF), vm((length, chans), BF), vm((length, chans), F32),
        both(length, F32), both(length, F32), both(length, F32), both(blocks * 8, F32),
        both(length, BF), both(length, BF),
        both(length, BF), both(length, BF), both(blocks * chans, BF), both(length, F32),
        both(length, F32), both(length, BF),
    ]


def core_kernel(
    tok_ref, w_ref, up_ref, floor_ref, rate_ref, diag_ref, gain_ref, out_ref,
    eq_s, wp_s, qe_s, kend_s, cv_s, own_s, decay_s, diag_s, t_s, b_s, state_s, y_s,
    arrivals=(),
):
    length, chans = out_ref.shape
    heads = chans // HEAD
    rank = up_ref.shape[1]
    rows = min(256, length)
    blocks = length // SPAN

    def head_ones():
        return (iota((chans, chans), 0) // HEAD == iota((chans, chans), 1) // HEAD).astype(BF)

    def head_sum(x, ones):
        hi, lo = split(x)
        return mm(hi, ones) + mm(lo, ones)

    def at_block(block):
        return pl.ds(pl.multiple_of(block * SPAN, SPAN), SPAN)

    def project(ready):
        tile = SPAN * len(ready)

        def put(ref, x, *lead):
            for s, block in enumerate(ready):
                ref[(*lead, at_block(block), slice(None))] = x[s * SPAN : (s + 1) * SPAN]

        source = jnp.concatenate([tok_ref[at_block(block), :] for block in ready], axis=0)
        pr = mm(source, w_ref[:, :chans]).astype(BF).astype(F32)
        pk = mm(source, w_ref[:, chans : 2 * chans]).astype(BF).astype(F32)
        pv = mm(source, w_ref[:, 2 * chans : 3 * chans]).astype(BF).astype(F32)
        lowered = jnp.tanh(mm(source, w_ref[:, 3 * chans :])).astype(BF)
        ones = head_ones()
        norm2 = head_sum(pk * pk, ones) + 1.0
        inv = lax.rsqrt(norm2)
        scale = norm2 * inv
        normed = pk * inv
        put(cv_s, scale * pv)
        rates = jax.nn.sigmoid(rate_ref[...])
        both = jnp.sum(rates * diag_ref[...], axis=0, keepdims=True)
        put(own_s, head_sum(pr * pk * both, ones) * pv)
        ri = iota((tile, tile), 0)
        ci = iota((tile, tile), 1)
        same = ri // SPAN == ci // SPAN
        whole = same.astype(BF)
        for d in range(2):
            pre = (
                mm(lowered[:, d * rank : (d + 1) * rank], up_ref[d]) + floor_ref[d : d + 1, :]
            ).astype(BF).astype(F32)
            fall = -math.exp(-0.5) * jax.nn.sigmoid(pre)
            tri = jnp.logical_and(same, (ci <= ri) if d == 0 else (ci >= ri)).astype(BF)
            hi, lo = split(fall)
            inclusive = mm(tri, hi) + mm(tri, lo)
            final = mm(whole, hi) + mm(whole, lo)
            half = 0.5 * final
            grow = jnp.exp(inclusive - half)
            shrink = jnp.exp(half - inclusive)
            g = jnp.exp(half)
            e = -normed * (grow * jnp.exp(-fall))
            q = pr * grow
            w = normed * rates[d : d + 1, :] * shrink
            put(wp_s, w.astype(BF), d)
            put(kend_s, (w * g).astype(BF), d)
            eb, qb = e.astype(BF), q.astype(BF)
            eg, qg = (e * g).astype(BF), (q * g).astype(BF)
            g2 = g * g
            put(diag_s, head_sum(pr * normed * rates[d : d + 1, :], ones), d)
            for s, block in enumerate(ready):
                cut = slice(s * SPAN, (s + 1) * SPAN)
                base = pl.multiple_of(block * 2 * SPAN, 2 * SPAN)
                eq_s[d, pl.ds(base, SPAN), :] = eb[cut]
                eq_s[d, pl.ds(base + SPAN, SPAN), :] = qb[cut]
                qe_s[d, pl.ds(base, SPAN), :] = eg[cut]
                qe_s[d, pl.ds(base + SPAN, SPAN), :] = qg[cut]
                decay_s[d, pl.ds(pl.multiple_of(block * 8, 8), 8), :] = g2[
                    s * SPAN : s * SPAN + 8
                ]

    def spread(x, mask):
        x = x.astype(BF)
        if heads > 1:
            x = jnp.concatenate([x] * heads, axis=0)
        return x * mask

    def invert(ready):
        mask = head_ones()
        ti = iota((SPAN, chans), 0)
        ji = iota((SPAN, chans), 1) % HEAD
        eye = (ti == ji).astype(F32)
        work = []
        for block in ready:
            for d in range(2):
                two = pl.ds(pl.multiple_of(block * 2 * SPAN, 2 * SPAN), 2 * SPAN)
                at = pl.ds(pl.multiple_of(block * SPAN, SPAN), SPAN)
                ab = lax.dot_general(
                    eq_s[d, two, :], spread(wp_s[d, at, :], mask), NT, preferred_element_type=F32
                )
                strict = (ti > ji) if d == 0 else (ti < ji)
                b_s[d, at, :] = jnp.where(strict, ab[SPAN:], 0.0).astype(BF)
                work.append((d, at, jnp.where(strict, ab[:SPAN], 0.0)))
        near = ti // 4 == ji // 4
        full = [a for _, _, a in work]
        base = [jnp.where(near, a, 0.0) for a in full]
        square = [mm(a.astype(BF), spread(a, mask)) for a in base]
        inverse = [eye + a for a in base]
        inverse = [t + mm(t.astype(BF), spread(a2, mask)) for t, a2 in zip(inverse, square)]
        size = 4
        while size < SPAN:
            far = jnp.logical_and(ti // (2 * size) == ji // (2 * size), ti // size != ji // size)
            first = [
                mm(t.astype(BF), spread(jnp.where(far, a, 0.0), mask))
                for t, a in zip(inverse, full)
            ]
            inverse = [t + mm(f.astype(BF), spread(t, mask)) for t, f in zip(inverse, first)]
            size *= 2
        for (d, at, _), t in zip(work, inverse):
            t_s[d, at, :] = (t - eye).astype(BF)

    for settle, ready in arrivals:
        settle()
        project(ready)
        invert(ready)

    state_s[...] = jnp.zeros_like(state_s)

    @pl.loop(0, blocks)
    def _(step):
        mask = head_ones()
        for d in range(2):
            block = step if d == 0 else blocks - 1 - step
            two = pl.ds(pl.multiple_of(block * 2 * SPAN, 2 * SPAN), 2 * SPAN)
            at = pl.ds(pl.multiple_of(block * SPAN, SPAN), SPAN)
            state = state_s[d]
            read = lax.dot_general(
                qe_s[d, two, :], state.astype(BF), NT, preferred_element_type=F32
            )
            x = cv_s[at, :] + read[:SPAN]
            exact = x + mm(t_s[d, at, :], spread(x, mask))
            a = exact.astype(BF)
            y_s[d, at, :] = read[SPAN:] + mm(b_s[d, at, :], spread(a, mask)) + diag_s[d, at, :] * exact
            decay = decay_s[d, pl.ds(pl.multiple_of(block * 8, 8), 8), :][:1]
            put = lax.dot_general(a, kend_s[d, at, :], TN, preferred_element_type=F32)
            state_s[d] = state * decay + put * mask.astype(F32)

    @pl.loop(0, length // rows)
    def _(step):
        at = pl.ds(pl.multiple_of(step * rows, rows), rows)
        ones = head_ones()
        total = own_s[at, :]
        for d in range(2):
            y = y_s[d, at, :]
            centred = y - head_sum(y, ones) * (1.0 / HEAD)
            variance = head_sum(centred * centred, ones) * (1.0 / HEAD)
            total = total + centred * lax.rsqrt(variance + 0.00064) * gain_ref[...]
        out_ref[at, :] = total.astype(BF)


MESH = pl.DeviceIdType.MESH


def whole_kernel(
    sp, dp, tok_ref, w_ref, up_ref, floor_ref, rate_ref, diag_ref, gain_ref, out_ref,
    tok_all, w_all, out_all, slots,
    ring_out, ring_in, far_out, far_in, pass_out, pass_in, back_out, back_in, *scratch,
):
    rows = tok_ref.shape[0]
    half_rows = rows // 2
    depth = w_ref.shape[0]
    chans = out_all.shape[1]
    chips = dp // 2
    z = lax.axis_index("sp")
    me = lax.axis_index("dp")
    chip = me // 2
    core = me % 2
    partner = chip * 2 + 1 - core

    def peer(k):
        return lax.rem(chip + k, chips) * 2 + core

    def z_peer(k):
        return lax.rem(z + k, sp)

    barrier = pltpu.get_barrier_semaphore()
    for target in [(z, partner)] + [(z, peer(k)) for k in range(1, chips)] + [
        (z_peer(k), me) for k in range(1, sp)
    ]:
        pl.semaphore_signal(barrier, inc=1, device_id=target, device_id_type=MESH)
    pl.semaphore_wait(barrier, chips + sp - 1)

    def remote(src, dst, out_sem, in_sem, target):
        copy = pltpu.make_async_remote_copy(
            src_ref=src, dst_ref=dst, send_sem=out_sem, recv_sem=in_sem,
            device_id=target, device_id_type=MESH,
        )
        copy.start()
        return copy

    def w_at(device):
        return pl.ds(pl.multiple_of(device * depth, depth), depth)

    def ring_step(s):
        copies = []
        for way in range(2):
            owner = z_peer(sp - s) if way == 0 else z_peer(s)
            at = pl.ds(
                pl.multiple_of(owner * rows + way * half_rows, half_rows), half_rows
            )
            first = tok_ref.at[pl.ds(way * half_rows, half_rows), :]
            copies.append(
                remote(
                    first if s == 0 else tok_all.at[at, :], tok_all.at[at, :],
                    ring_out.at[way, s], ring_in.at[way, s],
                    (z_peer(1) if way == 0 else z_peer(sp - 1), me),
                )
            )
        return copies

    ring = [ring_step(0)] if sp > 1 else []
    far = [
        remote(w_ref, w_all.at[w_at(me), :], far_out.at[k], far_in.at[k], (z, peer(k)))
        for k in range(1, chips)
    ]
    passed = [remote(w_ref, w_all.at[w_at(me), :], pass_out.at[0], pass_in.at[0], (z, partner))]
    w_all[w_at(me), :] = w_ref[...]
    tok_all[pl.ds(pl.multiple_of(z * rows, rows), rows), :] = tok_ref[...]
    for s in range(max(sp, chips) - 1):
        if s < sp - 2:
            for copy in ring[s]:
                copy.wait_recv()
            ring.append(ring_step(s + 1))
        if s < chips - 1:
            far[s].wait_recv()
            block = w_at(peer(chips - 1 - s))
            passed.append(
                remote(
                    w_all.at[block, :], w_all.at[block, :],
                    pass_out.at[s + 1], pass_in.at[s + 1], (z, partner),
                )
            )
    for copy in passed:
        copy.wait_recv()

    def last_ring():
        for copy in ring[-1]:
            copy.wait_recv()

    per = rows // SPAN
    arrivals = [(lambda: None, [z * per + b for b in range(per)])]
    for s in range(sp - 1):
        before, after = z_peer(sp - 1 - s), z_peer(s + 1)
        ready = [before * per + b for b in range(per // 2)]
        ready += [after * per + b for b in range(per // 2, per)]
        arrivals.append((last_ring if s == sp - 2 else lambda: None, ready))

    core_kernel(
        tok_all, w_all, up_ref, floor_ref, rate_ref, diag_ref, gain_ref, out_all, *scratch,
        arrivals=arrivals,
    )
    for copy in far + passed + [c for pair in ring for c in pair]:
        copy.wait_send()

    def out_at(owner):
        return pl.ds(pl.multiple_of(owner * rows, rows), rows)

    back = [
        remote(
            out_all.at[out_at(z_peer(k)), :], slots.at[z], back_out.at[k], back_in.at[k],
            (z_peer(k), me),
        )
        for k in range(1, sp)
    ]
    slots[z] = out_all[out_at(z), :]
    for copy in back:
        copy.wait()
    for s in range(sp):
        out_ref[:, s * chans : (s + 1) * chans] = slots[s]


def whole_call(sp, dp, rows, depth, chans, width):
    vm = pltpu.VMEM
    dma = pltpu.SemaphoreType.DMA
    length = rows * sp
    both = lambda n, dt: vm((2, n, chans), dt)
    return pl.pallas_call(
        functools.partial(whole_kernel, sp, dp),
        out_shape=jax.ShapeDtypeStruct((rows, chans * sp), BF),
        in_specs=[pl.BlockSpec(memory_space=vm)] * 7,
        out_specs=pl.BlockSpec(memory_space=vm),
        scratch_shapes=[
            vm((length, depth), BF), vm((depth, width), BF), vm((length, chans), BF),
            vm((sp, rows, chans), BF),
            dma((2, sp)), dma((2, sp)), dma((dp,)), dma((dp,)), dma((dp,)), dma((dp,)),
            dma((sp,)), dma((sp,)),
            both(2 * length, BF), both(length, BF), both(2 * length, BF), both(length, BF),
            vm((length, chans), F32), vm((length, chans), F32),
            both(length // SPAN * 8, F32), both(length, F32), both(length, BF), both(length, BF),
            vm((2, chans, chans), F32), both(length, F32),
        ],
        compiler_params=pltpu.CompilerParams(
            vmem_limit_bytes=58 * 1024 * 1024, collective_id=0, has_side_effects=True
        ),
        name="whole",
    )


def halves_kernel(
    sp, side, other, tok_ref, wr_ref, wk_ref, wv_ref, wd_ref, up_ref, floor_ref, rate_ref, diag_ref, gain_ref,
    out_ref, tok_all, wk_all, wv_all, wr_all, wd_all, up_s, floor_s, rate_s, diag_s, gain_s, out_all,
    w_in, w_out, relay_out, d_in, d_pass, t_in, t_pass, t_out, t_fwd, p_in, p_out, o_in, o_out, here, *scratch,
):
    rows = tok_ref.shape[0]
    depth = wk_ref.shape[0]
    chans = wk_all.shape[1]
    half = sp // 2
    part = rows // 4
    z = lax.axis_index("sp")
    me = lax.axis_index("dp")
    core = me % 2
    chip = me // 2
    cy, cx = chip // side, chip % side
    h = z // half
    j = z % half
    u = jnp.where(h == 1, j, half - 1 - j)
    slot = u * 2 + core
    partner = chip * 2 + 1 - core

    def layer(hh, uu):
        return half - 1 - uu + hh * (2 * uu + 1)

    def x_peer(k):
        return cy * side + lax.rem(cx + k, side)

    def y_peer(k):
        return lax.rem(cy + k, other) * side + cx

    x_peers = [x_peer(k) for k in range(1, side)]
    y_peers = [y_peer(k) for k in range(1, other)]

    def local(src, dst, n):
        copy = pltpu.make_async_copy(src, dst, here.at[n])
        copy.start()
        return copy

    def cols(who):
        return pl.ds(pl.multiple_of(who * chans, chans), chans)

    mine = at_row(me * depth, depth)
    own = [
        local(wd_ref, wd_all.at[mine, :], 0),
        local(wk_ref.at[:, cols(slot)], wk_all.at[mine, :], 1),
        local(up_ref.at[:, :, cols(slot)], up_s, 2),
        local(floor_ref.at[:, cols(slot)], floor_s, 3),
        local(wv_ref.at[:, cols(slot)], wv_all.at[mine, :], 4),
        local(wr_ref.at[:, cols(slot)], wr_all.at[mine, :], 5),
    ]

    @pl.when(core == h)
    def _():
        local(tok_ref, tok_all.at[at_row(z * rows, rows), :], 6)

    barrier = pltpu.get_barrier_semaphore()
    greet = [(z, p * 2 + k) for p in x_peers + y_peers for k in range(2)]
    greet += [(lax.rem(z + n, sp), chip * 2 + k) for n in range(1, sp) for k in range(2)]
    greet.append((z, partner))
    for target in greet:
        pl.semaphore_signal(barrier, inc=1, device_id=target, device_id_type=MESH)
    pl.semaphore_wait(barrier, len(greet))

    def remote(src, dst, out_sem, in_sem, target):
        return pltpu.make_async_remote_copy(
            src_ref=src, dst_ref=dst, send_sem=out_sem, recv_sem=in_sem,
            device_id=target, device_id_type=MESH,
        )

    def go(copy):
        copy.start()
        return copy

    sent = []
    wide = chans // WIDE
    pieces = [(wk_ref, wk_all, 0, chans), (wv_ref, wv_all, 0, chans)]
    pieces += [(wr_ref, wr_all, p * WIDE, WIDE) for p in range(wide)]
    decay = len(pieces)

    def take(n, who):
        src, _, low, size = pieces[n]
        return src.at[:, pl.ds(pl.multiple_of(who * chans + low, WIDE), size)]

    def landing(n, block):
        _, dst, low, size = pieces[n]
        return dst.at[block, low : low + size]

    def direct(n):
        for i, p in enumerate(x_peers + y_peers):
            for k in range(2):
                sent.append(go(remote(
                    take(n, u * 2 + k), landing(n, mine),
                    w_out.at[n, i * 2 + k], w_in.at[n, me], (z, p * 2 + k),
                )))
        last = 2 * len(x_peers + y_peers)
        sent.append(go(remote(
            take(n, u * 2 + 1 - core), landing(n, mine),
            w_out.at[n, last], w_in.at[n, me], (z, partner),
        )))

    def wait_for(sem, dst):
        remote(dst, dst, sem, sem, (z, partner)).wait_recv()

    def arrived(sem, dst, block):
        wait_for(sem, dst.at[block, :])

    def w_rows(p, c):
        return at_row((p * 2 + c) * depth, depth)

    def relay(n):
        count = 0
        for c, froms, tos in ((0, x_peers, y_peers), (1, y_peers, x_peers)):
            for p in froms:
                block = w_rows(p, c)
                wait_for(w_in.at[n, p * 2 + c], landing(n, block))
                for q in tos:
                    sent.append(go(remote(
                        landing(n, block), landing(n, block),
                        relay_out.at[n, count], w_in.at[n, p * 2 + c], (z, q * 2 + core),
                    )))
                    count += 1

    def finish(n):
        for c, others in ((1, x_peers), (0, y_peers)):
            for p in others:
                wait_for(w_in.at[n, p * 2 + c], landing(n, w_rows(p, c)))
        for ky in range(1, other):
            for kx in range(1, side):
                p = lax.rem(cy + ky, other) * side + lax.rem(cx + kx, side)
                for c in range(2):
                    wait_for(w_in.at[n, p * 2 + c], landing(n, w_rows(p, c)))
        wait_for(w_in.at[n, partner], landing(n, w_rows(chip, 1 - core)))

    def decay_direct():
        for i, p in enumerate(x_peers + y_peers):
            sent.append(go(remote(
                wd_ref, wd_all.at[mine, :], w_out.at[decay, i], d_in.at[me], (z, p * 2 + core))))
        sent.append(go(remote(
            wd_ref, wd_all.at[mine, :], w_out.at[decay, len(x_peers + y_peers)], d_in.at[me], (z, partner))))

    def decay_pass(p, n):
        block = w_rows(p, core)
        sent.append(go(remote(
            wd_all.at[block, :], wd_all.at[block, :], d_pass.at[n], d_in.at[p * 2 + core], (z, partner))))

    late = []

    def decay_relay():
        for c, froms, tos in ((0, x_peers, y_peers), (1, y_peers, x_peers)):
            @pl.when(core == c)
            def _():
                count = 0
                for p in froms:
                    block = w_rows(p, c)
                    arrived(d_in.at[p * 2 + c], wd_all, block)
                    for q in tos:
                        go(remote(
                            wd_all.at[block, :], wd_all.at[block, :],
                            relay_out.at[decay, count], d_in.at[p * 2 + c], (z, q * 2 + c)))
                        count += 1
                for p in tos:
                    arrived(d_in.at[p * 2 + c], wd_all, w_rows(p, c))

            def close(c=c, froms=froms, tos=tos):
                @pl.when(core == c)
                def _():
                    count = 0
                    for p in froms:
                        block = w_rows(p, c)
                        for q in tos:
                            remote(
                                wd_all.at[block, :], wd_all.at[block, :],
                                relay_out.at[decay, count], d_in.at[p * 2 + c], (z, q * 2 + c)).wait_send()
                            count += 1

            late.append(close)
        for n, p in enumerate(x_peers + y_peers):
            decay_pass(p, n)

    def decay_finish():
        n = len(x_peers + y_peers)
        corners = [
            lax.rem(cy + ky, other) * side + lax.rem(cx + kx, side)
            for ky in range(1, other) for kx in range(1, side)
        ]
        for p in corners:
            arrived(d_in.at[p * 2 + core], wd_all, w_rows(p, core))
            decay_pass(p, n)
            n += 1
        arrived(d_in.at[partner], wd_all, w_rows(chip, 1 - core))
        for p in x_peers + y_peers + corners:
            arrived(d_in.at[p * 2 + 1 - core], wd_all, w_rows(p, 1 - core))

    def t_rows(s, i):
        return at_row(s * rows + i * part, part)

    def block_sends(act):
        def all_parts(target_layer, first):
            for i in range(4):
                act(remote(
                    tok_ref.at[pl.ds(i * part, part), :], tok_all.at[t_rows(z, i), :],
                    t_out.at[first + i], t_in.at[z, i // 2], (target_layer, chip * 2 + i % 2)))

        @pl.when(core != h)
        def _():
            all_parts(layer(core, 0), 0)

        @pl.when(jnp.logical_and(core == h, u + 1 < half))
        def _():
            all_parts(layer(h, u + 1), 0)

        @pl.when(jnp.logical_and(core == h, u > 0))
        def _():
            all_parts(layer(h, u - 1), 4)

        @pl.when(core == h)
        def _():
            act(remote(
                tok_ref, tok_all.at[at_row(z * rows, rows), :], t_out.at[8], t_pass.at[z, 0], (z, partner)))

    def forward(s, outward, inward, n, q, act):
        block = t_rows(s, 2 * q + core)
        for cond, step in ((outward, 1), (inward, -1)):
            if cond is not None:
                @pl.when(cond)
                def _():
                    act(remote(
                        tok_all.at[block, :], tok_all.at[block, :], t_fwd.at[0, n, q], t_in.at[s, q],
                        (layer(h, u + step), me)))
        act(remote(
            tok_all.at[block, :], tok_all.at[block, :], t_fwd.at[1, n, q], t_pass.at[s, q], (z, partner)))

    near = [lax.rem(u + k, half) for k in range(1, half)]
    sources = [
        (layer(h, v), jnp.logical_and(u > v, u + 1 < half), jnp.logical_and(u < v, u > 0)) for v in near
    ]
    sources += [(layer(1 - h, v), u + 1 < half, None) for v in range(half)]

    def take_tokens(n, q):
        s, outward, inward = sources[n]
        arrived(t_in.at[s, q], tok_all, t_rows(s, 2 * q + core))
        forward(s, outward, inward, n, q, go)

    def take_far(now, q):
        @pl.when(now)
        def _():
            for n in range(half - 1, len(sources)):
                take_tokens(n, q)

    def own_tokens():
        block = at_row(z * rows, rows)

        @pl.when(core == h)
        def _():
            pltpu.make_async_copy(tok_ref, tok_all.at[block, :], here.at[6]).wait()

        @pl.when(core != h)
        def _():
            arrived(t_pass.at[z, 0], tok_all, block)

    def passed_tokens(n):
        s = sources[n][0]
        for q in range(2):
            arrived(t_pass.at[s, q], tok_all, t_rows(s, 2 * q + 1 - core))

    goal = (layer(core, z // 2), chip * 2 + z % 2)
    stay = jnp.logical_and(goal[0] == z, z % 2 == core)
    smalls = [(rate_ref, rate_s), (diag_ref, diag_s), (gain_ref, gain_s)]

    @pl.when(jnp.logical_not(stay))
    def _():
        for n, (src, dst) in enumerate(smalls):
            go(remote(src, dst, p_out.at[n], p_in.at[n], goal))

    @pl.when(stay)
    def _():
        for n, (src, dst) in enumerate(smalls):
            pltpu.make_async_copy(src, dst, p_in.at[n]).start()

    decay_direct()
    block_sends(go)
    direct(0)
    decay_relay()
    take_far(u + 1 < half, 0)
    relay(0)
    direct(1)
    direct(2)
    for n in range(half - 1):
        for q in range(2):
            take_tokens(n, q)
    take_far(u + 1 < half, 1)
    decay_finish()
    for n in (0, 2, 3):
        own[n].wait()
    own_tokens()
    for n in range(half - 1):
        passed_tokens(n)
    work = Core(
        tok_all, wk_all, wd_all, wv_all, wr_all, up_s, floor_s, rate_s, diag_s, gain_s, out_all, scratch)
    near_rows = h * half * rows
    far_rows = (1 - h) * half * rows
    work.decays(near_rows)
    take_far(u + 1 == half, 0)
    finish(0)
    own[1].wait()

    @pl.when(jnp.logical_not(stay))
    def _():
        for n, (src, dst) in enumerate(smalls):
            remote(src, dst, p_out.at[n], p_in.at[n], goal).wait_send()
    for n, (src, dst) in enumerate(smalls):
        remote(dst, dst, p_in.at[n], p_in.at[n], (z, partner)).wait_recv()

    units = work.keys(near_rows)
    work.invert(units)
    take_far(u + 1 == half, 1)
    for n in range(half - 1, len(sources)):
        passed_tokens(n)
    work.decays(far_rows)
    relay(1)
    for p in range(1, wide):
        direct(2 + p)
    units = work.keys(far_rows)
    work.invert(units)
    relay(2)
    finish(1)
    own[4].wait()
    work.values()
    for p in range(1, wide):
        relay(2 + p)
    work.scan()

    def give(s, p, n, act):
        block = at_row(s * rows, rows)
        low = p * WIDE
        act(remote(
            out_all.at[block, low : low + WIDE],
            out_ref.at[:, pl.ds(pl.multiple_of(slot * chans + low, WIDE), WIDE)],
            o_out.at[p, n], o_in.at[p, slot], (s, chip * 2 + h)))

    def give_far(p, act):
        for v in reversed(range(half)):
            give(layer(1 - h, v), p, v, act)

    def give_near(p, act):
        for n in range(half - 1):
            give(sources[n][0], p, half + n, act)

        @pl.when(core != h)
        def _():
            give(z, p, sp - 1, act)

    own[5].wait()
    for p in range(wide):
        finish(2 + p)
        work.outputs(far_rows, half * rows, p)
        give_far(p, go)
        work.outputs(near_rows, half * rows, p)
        give_near(p, go)

    @pl.when(core == h)
    def _():
        out_ref[:, cols(slot)] = out_all[at_row(z * rows, rows), :]

    def stop(copy):
        copy.wait_send()

    block_sends(stop)
    for n, (s, outward, inward) in enumerate(sources):
        for q in range(2):
            forward(s, outward, inward, n, q, stop)
    for copy in sent:
        copy.wait_send()
    for close in late:
        close()
    for p in range(wide):
        give_far(p, stop)
        give_near(p, stop)
        for g in range(sp):
            low = g * chans + p * WIDE

            @pl.when(jnp.logical_not(jnp.logical_and(core == h, slot == g)))
            def _():
                wait_for(o_in.at[p, g], out_ref.at[:, low : low + WIDE])


def halves_call(sp, dp, side, rows, width, depth, chans, rank):
    vm = pltpu.VMEM
    dma = pltpu.SemaphoreType.DMA
    chips = dp // 2
    other = chips // side
    peers = side + other - 2
    corners = (side - 1) * (other - 1)
    length = rows * sp
    wide = chans // WIDE
    return pl.pallas_call(
        functools.partial(halves_kernel, sp, side, other),
        out_shape=jax.ShapeDtypeStruct((rows, chans * sp), BF),
        in_specs=[pl.BlockSpec(memory_space=pl.ANY)] * 10,
        out_specs=pl.BlockSpec(memory_space=vm),
        scratch_shapes=[
            vm((length, width), BF), vm((width, chans), BF), vm((width, chans), BF), vm((width, chans), BF),
            vm((width, 2 * rank), BF), vm((2, rank, chans), BF), vm((2, chans), F32), vm((2, chans), F32),
            vm((2, chans), F32), vm((1, chans), F32), vm((length, chans), BF),
            dma((2 + wide, dp)), dma((3 + wide, 2 * peers + 1)), dma((3 + wide, 2 * corners)), dma((dp,)), dma((peers + corners,)),
            dma((sp, 2)), dma((sp, 2)), dma((9,)), dma((2, sp, 2)), dma((3,)), dma((3,)), dma((wide, sp)), dma((wide, sp)),
            dma((7,)),
        ] + core_scratch(length, chans),
        compiler_params=pltpu.CompilerParams(
            vmem_limit_bytes=32 * 1024 * 1024, collective_id=0, has_side_effects=True
        ),
        name="halves",
    )


def per_device(
    sp, dp,
    tokens, receptance_weight, key_projection_weight, value_projection_weight,
    decay_down_weight, decay_up_weight, decay_floor_level, correction_rate_logit,
    diagonal_address_factor, head_norm_gain,
):
    rows, width = tokens.shape[1:]
    depth, channels = receptance_weight.shape
    chans = channels // sp
    side = math.isqrt(dp // 2)
    gain = head_norm_gain[None, :]
    if chans % 128 == 0 and sp % 2 == 0 and dp == 2 * side * side and rows % SPAN == 0:
        given = [
            tokens[0], receptance_weight, key_projection_weight, value_projection_weight, decay_down_weight,
            decay_up_weight, decay_floor_level, correction_rate_logit, diagonal_address_factor, gain]
        given = [pltpu.with_memory_space_constraint(x, pltpu.HBM) for x in given]
        mixed = halves_call(sp, dp, side, rows, width, depth, chans, decay_up_weight.shape[1])(*given)
        return mixed[None]
    start = lax.axis_index("sp") * chans

    def mine(x):
        return lax.dynamic_slice_in_dim(x, start, chans, axis=x.ndim - 1)

    packed = jnp.concatenate(
        [mine(receptance_weight), mine(key_projection_weight), mine(value_projection_weight),
         decay_down_weight], axis=1)
    mixed = whole_call(sp, dp, rows, width, chans, packed.shape[1])(
        tokens[0], packed, mine(decay_up_weight), mine(decay_floor_level),
        correction_rate_logit, diagonal_address_factor, gain)
    return mixed[None]


def solution(mesh):
    in_specs = (
        P("dp", "sp", None), P("dp", None), P("dp", None), P("dp", None), P("dp", None),
        P(), P(), P(None, "sp"), P(None, "sp"), P("sp"),
    )
    return jax.shard_map(
        functools.partial(per_device, mesh.shape["sp"], mesh.shape["dp"]), mesh=mesh, in_specs=in_specs,
        out_specs=P("dp", "sp", None), check_vma=False,
    )
```
